256 devices in a mesh: sp: 16 (over y, x), tp: 16 (over z, core).
Axes of the slice: x: 4, y: 4, z: 8, core: 2. Of those that a mesh axis runs over, the one named last changes fastest.
Arguments:
- linear_part: bfloat16 [32768, 2048], P('sp', 'tp'), may hold values from -6 to 6
- gate_part: bfloat16 [32768, 2048], P('sp', 'tp'), may hold values from -8 to 8
- kernel_taps: bfloat16 [31, 2048], P(None, 'tp'), may hold values from -10 to 10
- channel_gain: float32 [2048], replicated, may hold values from 0.1 to 1.9
- output_weight: bfloat16 [2048, 2048], P('tp'), may hold values from -0.125 to 0.125
- residual: bfloat16 [32768, 2048], P(('sp', 'tp')), may hold values from -6 to 6
- mix_gain: float32 [2048], replicated, may hold values from 0.1 to 1.9
- documents: int32 [32768], P('sp'), may hold values from 0 to 3, never falling along the last dimension, each value on 1 to 16384 neighbouring positions
- expert_ids: int32 [32768, 2], P(('sp', 'tp')), may hold values from 0 to 15, all different within a row; in each aligned block of 128 rows (0 to 127, 128 to 255, ...) at most 64 rows name the same one
- route_weights: float32 [32768, 2], P(('sp', 'tp')), may hold values from 0.25 to 2.5
- expert_gate: bfloat16 [16, 2048, 512], P('sp'), may hold values from -0.125 to 0.125
- expert_up: bfloat16 [16, 2048, 512], P('sp'), may hold values from -0.125 to 0.125
- expert_down: bfloat16 [16, 512, 2048], P('sp'), may hold values from -0.25 to 0.25
- shared_gate: bfloat16 [2048, 256], replicated, may hold values from -0.125 to 0.125
- shared_up: bfloat16 [2048, 256], replicated, may hold values from -0.125 to 0.125
- shared_down: bfloat16 [256, 2048], replicated, may hold values from -0.375 to 0.375
- final_gain: float32 [2048], replicated, may hold values from 0.1 to 1.9
Outputs:
- layer_out: bfloat16 [32768, 2048], P(('sp', 'tp'))
The draws below stay inside these ranges and needn't reach their ends.
Inputs may be any that keep to these rules, and one draw needn't show every extreme that they name: `expert_ids`: each row names 2 different experts; among the rows of one device (aligned blocks of 128 rows) no expert is named by more than 64 rows, and exactly 64 in some block. `documents`: never falling along the sequence; each document 1 to 16384 positions.
All inputs are finite; a program needn't handle non-finite values.
Results may differ from the reference program's by a relative error of at most 0.0065.
Values may be sent and summed in bfloat16 or wider, within the bound.
A program may use at most 64 MiB of HBM per device.

```python
import math
import jax
import jax.numpy as jnp
import numpy as np
from jax import lax

D = 2048
KW = 31
FE = 512
FS = 256
TOP = 2
ROWS = 128
TOKENS = 32768
EXPERTS = 16
CAP = 64
DOCS = 4
DOC_MOST = 16384
N_SP = 16
N_TP = 16


def draw_kernel_taps(key, part):
    first = jax.random.fold_in(key, 11)
    second = jax.random.fold_in(key, 12)
    base = jnp.clip(jax.random.normal(first, (KW, D), jnp.float32), -4.0, 4.0) / math.sqrt(KW)
    spread = 10.0 ** jax.random.uniform(second, (D,), jnp.float32)
    return (base * spread[None, :]).astype(jnp.bfloat16)


def steps_of(stream_key, dims, pieces, least, high):
    level = 1.0
    for axis_at, parts in pieces:
        heights = jax.random.uniform(jax.random.fold_in(jax.random.fold_in(stream_key, 6), axis_at), (parts,), jnp.float32, least / len(pieces), high / len(pieces))
        level = level * jnp.repeat(jnp.exp(heights), dims[axis_at] // parts).reshape((-1,) + (1,) * (len(dims) - 1 - axis_at))
    return level


def profile(count, total, most, slope):
    loads = [(1 << 20) // math.isqrt(standing ** slope) + 1 for standing in range(2, count + 1)]
    spare, counts = total - most - (count - 1), [1] * (count - 1)
    while spare > 0:
        free = [i for i in range(count - 1) if counts[i] < most]
        whole, budget = sum([loads[i] for i in free]), spare
        for i in free:
            extra = min(most - counts[i], max(1, budget * loads[i] // whole), spare)
            counts[i] = counts[i] + extra
            spare = spare - extra
    return np.array([most] + counts)


def uneven_parts(own_key, count, total, most, slope):
    if count == 2:
        one = jax.random.randint(own_key, (), max(1, total - most), min(most, total - 1) + 1)
        return jnp.stack([one, total - one])
    sizes = jnp.asarray(profile(count, total, most, slope), jnp.int32)
    twos = (count - 1) // 2
    source_of, taker = sizes[1:1 + 2 * twos:2], sizes[2:2 + 2 * twos:2]
    slack = jnp.minimum(source_of - 1, most - taker)
    passed = jax.random.randint(jax.random.fold_in(own_key, 1), (twos,), 0, 1 << 20) % (slack + 1)
    sizes = sizes.at[1:1 + 2 * twos:2].set(source_of - passed).at[2:2 + 2 * twos:2].set(taker + passed)
    return sizes[jax.random.permutation(jax.random.fold_in(own_key, 2), count)]


def assign_block(stream_key, own, number, rows, amount, top, most, skew):
    ranking = jax.random.permutation(stream_key, amount)
    packed, usual = shares(amount, rows * top, most, skew, True), shares(amount, rows * top, most, skew, False)
    places = jnp.arange(amount)

    def named(tallies, offset_by):
        used = int((tallies > 0).sum())
        fixed = max(1, used // 4)
        shifted = fixed + (places - fixed + offset_by * (used - fixed)) % max(1, amount - fixed)
        return jnp.zeros((amount,), jnp.int32).at[ranking[jnp.where(places < fixed, places, shifted)]].set(jnp.asarray(tallies, jnp.int32))

    tallies = jnp.where(number % 4 == 0, named(packed, number // 4), named(usual, number - number // 4 - 1))
    mixed = jax.random.permutation(jax.random.fold_in(own, 3), amount)
    giver, sink = mixed[0:amount // 2 * 2:2], mixed[1:amount // 2 * 2:2]
    margin = jnp.minimum(tallies[giver] - 1, most - tallies[sink]) // 2
    margin = jnp.where((giver == ranking[0]) | (sink == ranking[0]) | (tallies[sink] == 0), 0, jnp.maximum(margin, 0))
    shifted = jax.random.randint(jax.random.fold_in(own, 4), (amount // 2,), 0, 1 << 20) % (margin + 1)
    tallies = tallies.at[giver].add(-shifted).at[sink].add(shifted)
    labels = jnp.searchsorted(jnp.cumsum(tallies), jnp.arange(rows * top), side="right").astype(jnp.int32)
    grid = labels.reshape(top, rows).T
    grid = grid[jax.random.permutation(jax.random.fold_in(own, 1), rows)]
    offset_by = jax.random.randint(jax.random.fold_in(own, 2), (rows, 1), 0, top)
    return jnp.take_along_axis(grid, (jnp.arange(top)[None, :] + offset_by) % top, axis=1)


def shares(count, total, bound, skew, full):
    weights = [(1 << 20) // math.isqrt(rank ** skew) + 1 for rank in range(1, count + 1)]
    largest = bound if full else min(bound, max(-(-total // count), total * weights[0] // sum(weights)))
    least = 1 if total - largest >= count - 1 else 0
    holding, surplus = [largest] + [least] * (count - 1), total - largest - least * (count - 1)
    while surplus > 0:
        free = [i for i in range(1, count) if holding[i] < largest] or [i for i in range(1, count) if holding[i] < bound]
        whole, remaining = sum([weights[i] for i in free]), surplus
        for i in free:
            extra = min(bound - holding[i], max(1, remaining * weights[i] // whole), surplus)
            holding[i] = holding[i] + extra
            surplus = surplus - extra
    return np.array(holding)


def scatter_about(key, shape, width, most, split=(), kind=jnp.bfloat16):
    drawn = width * jax.random.normal(key, shape, jnp.float32)
    if split:
        drawn = drawn * steps_of(key, shape, split, -0.22, 0.18)
    return jnp.clip(drawn, -most, most).astype(kind)


def setup_inputs(seed: int = 0) -> dict:
    key_list = jax.random.split(jax.random.key(seed), 18)
    linear_part = scatter_about(key_list[0], (TOKENS, D), 1.0, 6.0, ((0, 16), (1, 16)))
    gate_part = scatter_about(key_list[1], (TOKENS, D), 1.5, 8.0, ((0, 16), (1, 16)))
    kernel_taps = draw_kernel_taps(jax.random.fold_in(key_list[17], 71), 0)
    channel_gain = jnp.clip(1.0 + 0.18 * jax.random.normal(key_list[3], (D,), jnp.float32), 0.1, 1.9)
    output_weight = scatter_about(key_list[4], (D, D), D ** -0.5, 0.125, ((0, 16),))
    residual = scatter_about(key_list[5], (TOKENS, D), 1.0, 6.0, ((0, 256),))
    mix_gain = jnp.clip(1.0 + 0.18 * jax.random.normal(key_list[6], (D,), jnp.float32), 0.1, 1.9)
    documents = jnp.searchsorted(jnp.cumsum(uneven_parts(key_list[7], DOCS, TOKENS, DOC_MOST, 2)), jnp.arange(TOKENS), side="right").astype(jnp.int32)
    expert_ids_keys = jax.random.split(jax.random.fold_in(key_list[8], 1), TOKENS // ROWS)
    expert_ids_turns = jax.random.permutation(jax.random.fold_in(key_list[8], 3), TOKENS // ROWS)
    expert_ids = jax.vmap(lambda own, number: assign_block(jax.random.fold_in(key_list[8], 2), own, number, ROWS, EXPERTS, TOP, CAP, 2))(expert_ids_keys, expert_ids_turns).reshape((TOKENS, TOP))
    route_weights = jnp.clip(jnp.exp(math.log(2.5) - 2.3025851 * jax.random.uniform(key_list[9], (TOKENS, TOP), jnp.float32) ** steps_of(key_list[9], (TOKENS, TOP), ((0, 256),), -0.2, 0.2)), 0.25, 2.5)
    expert_gate = scatter_about(key_list[10], (EXPERTS, D, FE), D ** -0.5, 0.125, ((0, 16),))
    expert_up = scatter_about(key_list[11], (EXPERTS, D, FE), D ** -0.5, 0.125, ((0, 16),))
    expert_down = scatter_about(key_list[12], (EXPERTS, FE, D), FE ** -0.5, 0.25, ((0, 16),))
    shared_gate = scatter_about(key_list[13], (D, FS), D ** -0.5, 0.125)
    shared_up = scatter_about(key_list[14], (D, FS), D ** -0.5, 0.125)
    shared_down = scatter_about(key_list[15], (FS, D), FS ** -0.5, 0.375)
    final_gain = jnp.clip(1.0 + 0.18 * jax.random.normal(key_list[16], (D,), jnp.float32), 0.1, 1.9)
    return {"linear_part": linear_part, "gate_part": gate_part, "kernel_taps": kernel_taps, "channel_gain": channel_gain, "output_weight": output_weight, "residual": residual, "mix_gain": mix_gain, "documents": documents, "expert_ids": expert_ids, "route_weights": route_weights, "expert_gate": expert_gate, "expert_up": expert_up, "expert_down": expert_down, "shared_gate": shared_gate, "shared_up": shared_up, "shared_down": shared_down, "final_gain": final_gain}


EPSILON = 1e-05
RESIDUAL_SCALE = 8.0 ** 0.25

def normalize(values):
    mean = lax.optimization_barrier(jnp.mean(values, -1, keepdims=True))
    square = lax.optimization_barrier(jnp.mean(values * values, -1, keepdims=True))
    return (values - mean) * lax.rsqrt(square - mean * mean + EPSILON)

def reference(linear_part, gate_part, kernel_taps, channel_gain, output_weight, residual, mix_gain, documents, expert_ids, route_weights, expert_gate, expert_up, expert_down, shared_gate, shared_up, shared_down, final_gain):
    gated = (linear_part.astype(jnp.float32) * jax.nn.sigmoid(gate_part.astype(jnp.float32))).astype(jnp.bfloat16)
    reach = KW - 1
    padded = jnp.concatenate([jnp.zeros((reach, D), jnp.bfloat16), gated], 0)
    padded_docs = jnp.concatenate([jnp.full((reach,), -1, jnp.int32), documents.astype(jnp.int32)], 0)
    taps = kernel_taps.astype(jnp.float32)
    total = jnp.zeros((TOKENS, D), jnp.float32)
    for offset in range(KW):
        window = padded[reach - offset:reach - offset + TOKENS].astype(jnp.float32)
        same = padded_docs[reach - offset:reach - offset + TOKENS] == documents.astype(jnp.int32)
        total = total + jnp.where(same[:, None], window * taps[offset], 0.0)
    convolved = total.astype(jnp.bfloat16)
    activated = jax.nn.silu(normalize(convolved.astype(jnp.float32)) * channel_gain).astype(jnp.bfloat16)
    projected = jnp.dot(activated, output_weight, preferred_element_type=jnp.float32)
    normed = (normalize(RESIDUAL_SCALE * residual.astype(jnp.float32) + projected) * mix_gain).astype(jnp.bfloat16)
    limit = N_SP * N_TP * CAP

    def visit(routed, inputs):
        gate_w, up_w, down_w, expert = inputs
        hits = expert_ids == expert
        named = jnp.any(hits, 1)
        where_rows = jnp.nonzero(named, size=limit, fill_value=0)[0].astype(jnp.int32)
        count = jnp.sum(named.astype(jnp.int32))
        live = jnp.arange(limit, dtype=jnp.int32) < count
        weight = lax.optimization_barrier(jnp.sum(jnp.where(hits, route_weights, 0.0), 1))[where_rows]
        weight = jnp.where(live, weight, 0.0)
        rows = normed[where_rows]
        hidden = (jax.nn.silu(jnp.dot(rows, gate_w, preferred_element_type=jnp.float32)) * jnp.dot(rows, up_w, preferred_element_type=jnp.float32)).astype(jnp.bfloat16)
        answer = jnp.dot(hidden, down_w, preferred_element_type=jnp.float32).astype(jnp.bfloat16)
        return (routed.at[where_rows].add(weight[:, None] * answer.astype(jnp.float32)), None)
    routed, _ = lax.scan(visit, jnp.zeros((TOKENS, D), jnp.float32), (expert_gate, expert_up, expert_down, jnp.arange(EXPERTS, dtype=jnp.int32)))
    common = (jax.nn.silu(jnp.dot(normed, shared_gate, preferred_element_type=jnp.float32)) * jnp.dot(normed, shared_up, preferred_element_type=jnp.float32)).astype(jnp.bfloat16)
    shared_out = jnp.dot(common, shared_down, preferred_element_type=jnp.float32)
    return (normalize(RESIDUAL_SCALE * normed.astype(jnp.float32) + routed + shared_out) * final_gain).astype(jnp.bfloat16)
```

```python
import jax
import jax.numpy as jnp
from jax import lax
from jax.experimental import pallas as pl
from jax.experimental.pallas import tpu as pltpu
from jax.sharding import Mesh
from jax.sharding import PartitionSpec as P

TP = ("tp_0", "tp_1")
SP_TP = ("sp", "tp_0", "tp_1")


EPSILON = 1e-05
RESIDUAL_SCALE = 8.0**0.25


def passed_along(block, axis, distance):
    devices = range(lax.axis_size(axis))
    route = [(i - distance, i) for i in devices if i - distance in devices]
    return lax.ppermute(block, axis, route)


def cut_along(x, dim, length):
    before, after = (x.shape[:dim], x.shape[dim + 1 :])
    return jnp.moveaxis(x.reshape(*before, length, -1, *after), dim, 0)


def laid_out(tiles, dim):
    lengths = list(tiles.shape[1:])
    lengths[dim] *= tiles.shape[0]
    return jnp.moveaxis(tiles, 0, dim).reshape(lengths)


def exchange_in_order(tiles, axes, turns):
    inside = tiles.shape[1:]
    whole = tiles.reshape(*(lax.axis_size(a) for a in axes), *inside)
    for k in turns:
        whole = lax.all_to_all(whole, axes[k], k, k, tiled=True)
    return whole.reshape(-1, *inside)


def exchange_by_axis(x, axes, turns, split_dim, concat_dim):
    tiles = cut_along(x, split_dim, lax.axis_size(axes))
    return laid_out(exchange_in_order(tiles, axes, turns), concat_dim)


def normalize(values):
    mean = jnp.mean(values, -1, keepdims=True)
    square = jnp.mean(values * values, -1, keepdims=True)
    return (values - mean) * lax.rsqrt(square - mean * mean + EPSILON)


MESH_ID = pl.DeviceIdType.MESH
HALF = 1024
SIDE = 4
CAP = 64


def expert_kernel(
    normed, table, gain, w_gate, w_up, w_down, s_gate, s_up, s_down, out,
    wg, wu, wd, sg, su, sd,
    near, meta, packed, relay, arrived, acc_g, acc_u, answers, relay_back, back, partial, relay_part, part_in,
    kept, shared,
    w_sem, s1_s, s1_r, m_s, m_r, d_s, d_r, rl_s, rl_r, fw_s, fw_r,
    b_s, b_r, bl_s, bl_r, bf_s, bf_r, p_s, p_r,
):
    f32, bf16 = jnp.float32, jnp.bfloat16
    sp, tp = lax.axis_index("sp"), (lax.axis_index("tp_0"), lax.axis_index("tp_1"))
    y, x = sp // SIDE, sp % SIDE

    def at(dy, dx):
        return ((y + dy) % SIDE) * SIDE + (x + dx) % SIDE

    def first(o, k):
        return at(0, k) if o == 0 else at(k, 0)

    def second(o, k):
        return at(k, 0) if o == 0 else at(0, k)

    def send(src, dst, ss, rs, to):
        copy = pltpu.make_async_remote_copy(
            src_ref=src, dst_ref=dst, send_sem=ss, recv_sem=rs,
            device_id=(to, *tp), device_id_type=MESH_ID,
        )
        copy.start()
        sent.append(copy)

    def landed(dst, ss, rs):
        pltpu.make_async_remote_copy(
            src_ref=dst, dst_ref=dst, send_sem=ss, recv_sem=rs,
            device_id=(first(0, 1), *tp), device_id_type=MESH_ID,
        ).wait_recv()

    sent = []
    loads = [
        pltpu.make_async_copy(a, b, w_sem.at[i])
        for i, (a, b) in enumerate(
            [(s_gate, sg), (s_up, su), (s_down, sd), (w_gate, wg), (w_up, wu), (w_down, wd)]
        )
    ]
    for load in loads:
        load.start()

    barrier = pltpu.get_barrier_semaphore()
    for to in (at(0, 1), at(0, 3), at(1, 0), at(3, 0)):
        pl.semaphore_signal(barrier, inc=1, device_id=(to, *tp), device_id_type=MESH_ID)
    pl.semaphore_wait(barrier, 4)

    for o in (0, 1):
        mine = normed.at[:, o * HALF:(o + 1) * HALF]
        send(table, meta.at[o, 3], m_s.at[o, 0], m_r.at[o, 0], first(o, 1))
        send(table, meta.at[o, 1], m_s.at[o, 1], m_r.at[o, 1], first(o, 3))
        send(mine, near.at[o, 3], s1_s.at[o, 0], s1_r.at[o, 0], first(o, 1))
        send(mine, near.at[o, 1], s1_s.at[o, 1], s1_r.at[o, 1], first(o, 3))

    lanes = lax.broadcasted_iota(jnp.int32, (CAP, 128), 0).astype(f32)

    def expert_at(o, k):
        return second(o, k)

    def slot_row(o, k, e):
        return table[e] if k == 0 else meta[o, k, e]

    def weight_row(o, k, e):
        return table[e + 16] if k == 0 else meta[o, k, e + 16]

    def pack(o, k):
        rows = normed[:, o * HALF:(o + 1) * HALF] if k == 0 else near[o, k]
        for q in (2, 1, 3, 0):
            hit = jnp.where(lanes == slot_row(o, k, expert_at(o, q)), 1.0, 0.0).astype(bf16)
            block = jnp.dot(hit, rows, preferred_element_type=f32).astype(bf16)
            if q == 0:
                arrived[o, 0, k] = block
            else:
                packed[o, q - 1, k] = block
            if q == 2:
                way = 1 if k < 2 else 3
                send(packed.at[o, 1, k], relay.at[o, k], rl_s.at[o, k], rl_r.at[o, k], second(o, way))
            if q == 1:
                send(packed.at[o, 0, k], arrived.at[o, 3, k], d_s.at[o, 0, k], d_r.at[o, 0, k], second(o, 1))
            if q == 3:
                send(packed.at[o, 2, k], arrived.at[o, 1, k], d_s.at[o, 1, k], d_r.at[o, 1, k], second(o, 3))

    def pass_on(o, k):
        landed(relay.at[o, k], rl_s.at[o, k], rl_r.at[o, k])
        way = 1 if k < 2 else 3
        send(relay.at[o, k], arrived.at[o, 2, k], fw_s.at[o, k], fw_r.at[o, k], second(o, way))

    for o in (0, 1):
        pack(o, 0)
    for o in (0, 1):
        landed(meta.at[o, 3], m_s.at[o, 0], m_r.at[o, 0])
        send(meta.at[o, 3], meta.at[o, 2], m_s.at[o, 2], m_r.at[o, 2], first(o, 1))
        landed(near.at[o, 3], s1_s.at[o, 0], s1_r.at[o, 0])
        send(near.at[o, 3, 0:64], near.at[o, 2, 0:64], s1_s.at[o, 2], s1_r.at[o, 2], first(o, 1))
    for o in (0, 1):
        landed(meta.at[o, 1], m_s.at[o, 1], m_r.at[o, 1])
        landed(near.at[o, 1], s1_s.at[o, 1], s1_r.at[o, 1])
        send(near.at[o, 1, 64:128], near.at[o, 2, 64:128], s1_s.at[o, 3], s1_r.at[o, 3], first(o, 3))
    for k in (3, 1):
        for o in (0, 1):
            pack(o, k)
    for o in (0, 1):
        pass_on(o, 0)
    for o in (0, 1):
        landed(meta.at[o, 2], m_s.at[o, 2], m_r.at[o, 2])
        landed(near.at[o, 2, 0:64], s1_s.at[o, 2], s1_r.at[o, 2])
        landed(near.at[o, 2, 64:128], s1_s.at[o, 3], s1_r.at[o, 3])
        pack(o, 2)

    for load in loads[:3]:
        load.wait()
    act = jnp.dot(normed[...], sg[...], preferred_element_type=f32)
    lin = jnp.dot(normed[...], su[...], preferred_element_type=f32)
    common = (act / (1.0 + jnp.exp(-act)) * lin).astype(bf16)
    shared[...] = jnp.dot(common, sd[...], preferred_element_type=f32)
    for k in (3, 1, 2):
        for o in (0, 1):
            pass_on(o, k)
    for load in loads[3:]:
        load.wait()

    def product(o, q):
        rows = arrived[o, q].reshape(SIDE * CAP, HALF)
        for acc, w in ((acc_g, wg), (acc_u, wu)):
            got = jnp.dot(rows, w[o * HALF:(o + 1) * HALF, :], preferred_element_type=f32)
            got = got.reshape(SIDE, CAP, 512)
            if o == 0:
                acc[q] = got
            else:
                acc[:, q] = acc[:, q] + got

    def from_side(q, d):
        for k in range(SIDE):
            for o in (0, 1):
                landed(arrived.at[o, q, k], d_s.at[o, d, k], d_r.at[o, d, k])

    product(0, 0)
    from_side(3, 0)
    product(0, 3)
    from_side(1, 1)
    product(0, 1)
    for k in (0, 3, 1, 2):
        landed(arrived.at[0, 2, k], fw_s.at[0, k], fw_r.at[0, k])
    product(0, 2)
    product(1, 0)
    product(1, 3)
    product(1, 1)
    for k in (0, 3, 1, 2):
        landed(arrived.at[1, 2, k], fw_s.at[1, k], fw_r.at[1, k])
    product(1, 2)

    def give_back(o, q, k, block):
        if q == 0:
            back[o, k, 0] = block
            return
        answers[o, q - 1, k] = block
        mine = answers.at[o, q - 1, k]
        if q == 2:
            way = 1 if k < 2 else 3
            send(mine, relay_back.at[o, k], bl_s.at[o, k], bl_r.at[o, k], second(o, way))
        else:
            d = 0 if q == 1 else 1
            send(mine, back.at[o, k, SIDE - q], b_s.at[o, d, k], b_r.at[o, d, k], second(o, q))

    def pass_back(o, k):
        landed(relay_back.at[o, k], bl_s.at[o, k], bl_r.at[o, k])
        way = 1 if k < 2 else 3
        send(relay_back.at[o, k], back.at[o, k, 2], bf_s.at[o, k], bf_r.at[o, k], second(o, way))

    for dx in (2, 1, 3, 0):
        g = acc_g[:, dx].reshape(SIDE * CAP, 512)
        u = acc_u[:, dx].reshape(SIDE * CAP, 512)
        hidden = (g / (1.0 + jnp.exp(-g)) * u).astype(bf16)
        for o in (0, 1):
            ans = jnp.dot(
                hidden, wd[:, o * HALF:(o + 1) * HALF], preferred_element_type=f32
            ).astype(bf16)
            for dy in (2, 1, 3, 0):
                block = ans[dy * CAP:(dy + 1) * CAP]
                if o == 0:
                    give_back(0, dy, dx, block)
                else:
                    give_back(1, dx, dy, block)

    def choose(o, k, part):
        rows = []
        for j in range(SIDE):
            e = expert_at(o, j)
            w = weight_row(o, k, e)
            high = w.astype(bf16).astype(f32)
            value = high if part == 0 else w - high
            rows.append(jnp.where(lanes == slot_row(o, k, e), value, 0.0).astype(bf16))
        return jnp.concatenate(rows, 0)

    def combine(o, k):
        for j, d in ((3, 0), (1, 1)):
            landed(back.at[o, k, j], b_s.at[o, d, k], b_r.at[o, d, k])
        landed(back.at[o, k, 2], bf_s.at[o, k], bf_r.at[o, k])
        rows = back[o, k].reshape(SIDE * CAP, HALF)
        dims = (((0,), (0,)), ((), ()))
        total = lax.dot_general(choose(o, k, 0), rows, dims, preferred_element_type=f32)
        return total + lax.dot_general(choose(o, k, 1), rows, dims, preferred_element_type=f32)

    for k in (2, 1, 3, 0):
        for o in (0, 1):
            pass_back(o, k)
    for k in (2, 1, 3):
        for o in (0, 1):
            partial[o, k - 1] = combine(o, k).astype(bf16)
            mine = partial.at[o, k - 1]
            if k == 2:
                send(mine.at[0:64], relay_part.at[o, 0], p_s.at[o, 2], p_r.at[o, 2], first(o, 1))
                send(mine.at[64:128], relay_part.at[o, 1], p_s.at[o, 3], p_r.at[o, 3], first(o, 3))
            elif k == 1:
                send(mine, part_in.at[o, 2], p_s.at[o, 0], p_r.at[o, 0], first(o, 1))
            else:
                send(mine, part_in.at[o, 0], p_s.at[o, 1], p_r.at[o, 1], first(o, 3))
    for o in (0, 1):
        landed(relay_part.at[o, 0], p_s.at[o, 2], p_r.at[o, 2])
        send(relay_part.at[o, 0], part_in.at[o, 1, 0:64], p_s.at[o, 4], p_r.at[o, 4], first(o, 1))
        landed(relay_part.at[o, 1], p_s.at[o, 3], p_r.at[o, 3])
        send(relay_part.at[o, 1], part_in.at[o, 1, 64:128], p_s.at[o, 5], p_r.at[o, 5], first(o, 3))
    for o in (0, 1):
        kept[:, o * HALF:(o + 1) * HALF] = combine(o, 0)
    for o in (0, 1):
        landed(part_in.at[o, 2], p_s.at[o, 0], p_r.at[o, 0])
        landed(part_in.at[o, 0], p_s.at[o, 1], p_r.at[o, 1])
        landed(part_in.at[o, 1, 0:64], p_s.at[o, 4], p_r.at[o, 4])
        landed(part_in.at[o, 1, 64:128], p_s.at[o, 5], p_r.at[o, 5])
        here = slice(o * HALF, (o + 1) * HALF)
        kept[:, here] = (
            kept[:, here] + part_in[o, 0].astype(f32) + part_in[o, 1].astype(f32) + part_in[o, 2].astype(f32)
        )
    values = RESIDUAL_SCALE * normed[...].astype(f32) + kept[...] + shared[...]
    out[...] = (normalize(values) * gain[...]).astype(bf16)
    for copy in sent:
        copy.wait_send()


def experts(normed, table, gain, w_gate, w_up, w_down, s_gate, s_up, s_down):
    bf16, f32 = jnp.bfloat16, jnp.float32
    dma = pltpu.SemaphoreType.DMA
    vmem = pl.BlockSpec(memory_space=pltpu.VMEM)
    hbm = pl.BlockSpec(memory_space=pl.ANY)
    block = (CAP, HALF)
    return pl.pallas_call(
        expert_kernel,
        out_shape=jax.ShapeDtypeStruct(normed.shape, bf16),
        in_specs=[vmem, vmem, vmem, hbm, hbm, hbm, hbm, hbm, hbm],
        out_specs=vmem,
        scratch_shapes=[
            pltpu.VMEM(w_gate.shape, bf16),
            pltpu.VMEM(w_up.shape, bf16),
            pltpu.VMEM(w_down.shape, bf16),
            pltpu.VMEM(s_gate.shape, bf16),
            pltpu.VMEM(s_up.shape, bf16),
            pltpu.VMEM(s_down.shape, bf16),
            pltpu.VMEM((2, 4, 128, HALF), bf16),
            pltpu.VMEM((2, 4, 32, 1, 128), f32),
            pltpu.VMEM((2, 3, 4) + block, bf16),
            pltpu.VMEM((2, 4) + block, bf16),
            pltpu.VMEM((2, 4, 4) + block, bf16),
            pltpu.VMEM((4, 4, CAP, 512), f32),
            pltpu.VMEM((4, 4, CAP, 512), f32),
            pltpu.VMEM((2, 3, 4) + block, bf16),
            pltpu.VMEM((2, 4) + block, bf16),
            pltpu.VMEM((2, 4, 4) + block, bf16),
            pltpu.VMEM((2, 3, 128, HALF), bf16),
            pltpu.VMEM((2, 2) + block, bf16),
            pltpu.VMEM((2, 3, 128, HALF), bf16),
            pltpu.VMEM((128, 2048), f32),
            pltpu.VMEM((128, 2048), f32),
            dma((6,)),
            dma((2, 4)), dma((2, 4)), dma((2, 3)), dma((2, 3)),
            dma((2, 2, 4)), dma((2, 2, 4)), dma((2, 4)), dma((2, 4)), dma((2, 4)), dma((2, 4)),
            dma((2, 2, 4)), dma((2, 2, 4)), dma((2, 4)), dma((2, 4)), dma((2, 4)), dma((2, 4)),
            dma((2, 6)), dma((2, 6)),
        ],
        compiler_params=pltpu.CompilerParams(
            collective_id=0, has_side_effects=True, vmem_limit_bytes=60 * 1024 * 1024
        ),
    )(normed, table, gain, w_gate, w_up, w_down, s_gate, s_up, s_down)


def shards(
    linear_part,
    gate_part,
    kernel_taps,
    channel_gain,
    output_weight,
    residual,
    mix_gain,
    documents,
    expert_ids,
    route_weights,
    expert_gate,
    expert_up,
    expert_down,
    shared_gate,
    shared_up,
    shared_down,
    final_gain,
):
    reach = kernel_taps.shape[0] - 1
    length = linear_part.shape[0]
    gated = (
        linear_part.astype(jnp.float32) * jax.nn.sigmoid(gate_part.astype(jnp.float32))
    ).astype(jnp.bfloat16)
    before, before_docs = passed_along(
        (gated[length - reach :], documents[length - reach :]), "sp", 1
    )
    extended = jnp.concatenate([before, gated], 0)
    extended_docs = jnp.concatenate([before_docs, documents], 0)
    taps = kernel_taps.astype(jnp.float32)
    total = jnp.zeros(gated.shape, jnp.float32)
    for offset in range(reach + 1):
        window = lax.slice_in_dim(extended, reach - offset, reach - offset + length, axis=0).astype(
            jnp.float32
        )
        same = (
            lax.slice_in_dim(extended_docs, reach - offset, reach - offset + length, axis=0)
            == documents
        )
        total = total + jnp.where(same[:, None], window * taps[offset], 0.0)
    convolved = total.astype(jnp.bfloat16)
    position_rows = exchange_by_axis(convolved, TP, (1, 0), 0, 1)
    activated = jax.nn.silu(normalize(position_rows.astype(jnp.float32)) * channel_gain).astype(
        jnp.bfloat16
    )
    full_weight = lax.all_gather(output_weight, TP, axis=0, tiled=True)
    projected = jnp.dot(activated, full_weight, preferred_element_type=jnp.float32)
    normed = (
        normalize(RESIDUAL_SCALE * residual.astype(jnp.float32) + projected) * mix_gain
    ).astype(jnp.bfloat16)
    names = jnp.arange(16, dtype=jnp.int32)
    named = expert_ids[None, :, :] == names[:, None, None]
    hits = jnp.any(named, 2)
    ranks = jnp.cumsum(hits.astype(jnp.int32), 1) - 1
    slots = jnp.where(hits, ranks, -1).astype(jnp.float32)
    weights = jnp.sum(jnp.where(named, route_weights[None], 0.0), 2)
    table = jnp.concatenate([slots, weights], 0)[:, None, :]
    return experts(
        normed, table, final_gain[None, :], expert_gate[0], expert_up[0], expert_down[0],
        shared_gate, shared_up, shared_down,
    )


def solution(mesh):
    finer = Mesh(mesh.devices.reshape(mesh.shape["sp"], 8, 2), ("sp", "tp_0", "tp_1"))
    placed = (
        P("sp", TP),
        P("sp", TP),
        P(None, TP),
        P(),
        P(TP, None),
        P(SP_TP, None),
        P(),
        P("sp"),
        P(SP_TP, None),
        P(SP_TP, None),
        P("sp", None, None),
        P("sp", None, None),
        P("sp", None, None),
        P(),
        P(),
        P(),
        P(),
    )
    return jax.shard_map(
        shards, mesh=finer, in_specs=placed, out_specs=P(SP_TP, None), check_vma=False
    )
```

```python
import jax
import jax.numpy as jnp
from jax import lax
from jax.experimental import pallas as pl
from jax.experimental.pallas import tpu as pltpu
from jax.sharding import PartitionSpec as P

EPSILON = 1e-05
RESIDUAL_SCALE = 8.0**0.25
MESH_ID = pl.DeviceIdType.MESH
HALF = 1024
SIDE = 4
DEPTH = 8
CAP = 64
ROWS = 128
HALO = 32
TAPS = 31
PLACE = {0: 0, 1: 1, 7: 2, 2: 3, 6: 4, 3: 5, 5: 6, 4: 7}
GROUP = ((1, 5), (5, 8))


def normalize(values):
    mean = jnp.mean(values, -1, keepdims=True)
    square = jnp.mean(values * values, -1, keepdims=True)
    return (values - mean) * lax.rsqrt(square - mean * mean + EPSILON)


def layer_kernel(
    linear_h, gate_h, taps, channel_gain, w_h, residual_h, mix_gain, docs, ids, ways, gain,
    w_gate, w_up, w_down, s_gate, s_up, s_down, out,
    linear, gate, residual, weight, gated, tail, tail_docs, halo, halo_docs, tap32, conv, conv_in, act,
    sums, sums_in, part, part_in2, normed, table,
    wg, wu, wd, sg, su, sd,
    near, meta, packed, relay, arrived, acc_g, acc_u, answers, relay_back, back, partial, relay_part, part_in,
    kept, shared,
    l_sem, z_s, z_r, h_s, h_r, a_s, a_r, g_s, g_r, f_s, f_r, e_s, e_r, st_s, st_r, x_s, x_r,
    w_sem, s1_s, s1_r, m_s, m_r, d_s, d_r, rl_s, rl_r, fw_s, fw_r,
    b_s, b_r, bl_s, bl_r, bf_s, bf_r, p_s, p_r,
):
    f32, bf16 = jnp.float32, jnp.bfloat16
    sp, tp = lax.axis_index("sp"), lax.axis_index("tp")
    y, x = sp // SIDE, sp % SIDE
    z, core = tp // 2, tp % 2
    other = 1 - core

    def at(dy, dx):
        return ((y + dy) % SIDE) * SIDE + (x + dx) % SIDE

    def first(o, k):
        return at(0, k) if o == 0 else at(k, 0)

    def second(o, k):
        return at(k, 0) if o == 0 else at(0, k)

    def along(dz):
        return ((z + dz) % DEPTH) * 2 + core

    def push(src, dst, ss, rs, to_sp, to_tp):
        copy = pltpu.make_async_remote_copy(
            src_ref=src, dst_ref=dst, send_sem=ss, recv_sem=rs,
            device_id=(to_sp, to_tp), device_id_type=MESH_ID,
        )
        copy.start()
        sent.append(copy)

    def send(src, dst, ss, rs, to):
        push(src, dst, ss, rs, to, tp)

    def landed(dst, ss, rs):
        pltpu.make_async_remote_copy(
            src_ref=dst, dst_ref=dst, send_sem=ss, recv_sem=rs,
            device_id=(first(0, 1), tp), device_id_type=MESH_ID,
        ).wait_recv()

    sent = []
    own_loads = [
        pltpu.make_async_copy(a, b, l_sem.at[i])
        for i, (a, b) in enumerate(
            [(w_h, weight.at[0]), (linear_h, linear), (gate_h, gate), (residual_h, residual)]
        )
    ]
    for load in own_loads:
        load.start()
    loads = [
        pltpu.make_async_copy(a, b, w_sem.at[i])
        for i, (a, b) in enumerate(
            [(s_gate, sg), (s_up, su), (s_down, sd), (w_gate, wg), (w_up, wu), (w_down, wd)]
        )
    ]

    after, ahead = (sp + 1) % 16, (sp + 15) % 16
    barrier = pltpu.get_barrier_semaphore()

    def greet(to_sp, to_tp):
        pl.semaphore_signal(barrier, inc=1, device_id=(to_sp, to_tp), device_id_type=MESH_ID)

    for dz in range(1, DEPTH):
        greet(sp, along(dz))
    for to in (at(0, 1), at(0, 3), at(1, 0), at(3, 0), after, ahead):
        greet(to, tp)
    greet(sp, z * 2 + other)
    pl.semaphore_wait(barrier, 14)

    def columns(o, k, width=1):
        fast, slow = (x, y) if o == 0 else (y, x)
        return pl.ds(pl.multiple_of((slow * SIDE + (fast + k) % SIDE) * 128, 128), 128)

    def side_columns(o, ks, kf):
        fast, slow = (x, y) if o == 0 else (y, x)
        block = ((slow + ks) % SIDE) * SIDE + (fast + kf) % SIDE
        return pl.ds(pl.multiple_of(block * 128, 128), 128)

    own_loads[0].wait()
    for dz in (7, 1, 6, 2, 5, 3, 4):
        there = PLACE[(DEPTH - dz) % DEPTH]
        o = 0 if there < GROUP[0][1] else 1
        cols = columns(o, 0)
        push(weight.at[0, :, cols], weight.at[there, :, cols], z_s.at[there], z_r.at[there], sp, along(dz))

    own_loads[1].wait()
    own_loads[2].wait()

    def gate_rows(a, b):
        a, b = a.astype(f32), b.astype(f32)
        return (a * (1.0 / (1.0 + jnp.exp(-b)))).astype(bf16)

    tail[...] = gate_rows(linear[2048 - HALO:, :], gate[2048 - HALO:, :])
    doc = docs[...]
    spot = lax.broadcasted_iota(jnp.int32, (16, 128), 0) * 128 + lax.broadcasted_iota(jnp.int32, (16, 128), 1)
    local, last = [], []
    for d in (1, 2, 3):
        below = jnp.where(doc < d, 1.0, 0.0)
        local.append(jnp.sum(jnp.sum(below, 1, keepdims=True), 0, keepdims=True))
        below = jnp.where(spot >= 2048 - (TAPS - 1), below, 0.0)
        last.append(jnp.sum(jnp.sum(below, 1, keepdims=True), 0, keepdims=True))
    for i in range(3):
        tail_docs[i:i + 1, :] = jnp.broadcast_to(last[i], (1, 128))
    tail_docs[3:8, :] = jnp.zeros((5, 128), f32)
    push(tail, halo, h_s.at[0], h_r.at[0], after, tp)
    push(tail_docs, halo_docs, h_s.at[1], h_r.at[1], after, tp)
    for load in loads:
        load.start()

    def gate_block(i, _):
        rows = pl.ds(pl.multiple_of(i * 128, 128), 128)
        there = pl.ds(pl.multiple_of(i * 128 + HALO, 32), 128)
        gated[there, :] = gate_rows(linear[rows, :], gate[rows, :]).astype(f32)
        return 0

    lax.fori_loop(0, 16, gate_block, 0)
    tap32[0:TAPS, :] = taps[...].astype(f32)

    def spread(o, k, rows, i):
        lo, hi = GROUP[o]
        mine = weight.at[lo:hi, rows, side_columns(o, 0, k)]
        send(mine, mine, e_s.at[o, k, i], e_r.at[o, k, i], second(o, 1 if i % 2 == 0 else 3))

    whole, upper, lower = slice(0, 128), slice(0, 64), slice(64, 128)

    def gather_start(o):
        lo, hi = GROUP[o]
        mine = weight.at[lo:hi, :, columns(o, 0)]
        for there in range(lo, hi):
            landed(weight.at[there, :, columns(o, 0)], z_s.at[there], z_r.at[there])
        send(mine, mine, g_s.at[o, 0], g_r.at[o, 0], first(o, 1))
        send(mine, mine, g_s.at[o, 1], g_r.at[o, 1], first(o, 3))
        spread(o, 0, whole, 0)
        spread(o, 0, whole, 1)

    def gather_near(o):
        lo, hi = GROUP[o]
        landed(weight.at[lo:hi, :, columns(o, 3)], g_s.at[o, 0], g_r.at[o, 0])
        half = weight.at[lo:hi, upper, columns(o, 3)]
        send(half, half, g_s.at[o, 2], g_r.at[o, 2], first(o, 1))
        spread(o, 3, whole, 0)
        spread(o, 3, whole, 1)
        landed(weight.at[lo:hi, :, columns(o, 1)], g_s.at[o, 1], g_r.at[o, 1])
        half = weight.at[lo:hi, lower, columns(o, 1)]
        send(half, half, g_s.at[o, 3], g_r.at[o, 3], first(o, 3))
        spread(o, 1, whole, 0)
        spread(o, 1, whole, 1)

    def gather_far(o):
        lo, hi = GROUP[o]
        landed(weight.at[lo:hi, upper, columns(o, 2)], g_s.at[o, 2], g_r.at[o, 2])
        landed(weight.at[lo:hi, lower, columns(o, 2)], g_s.at[o, 3], g_r.at[o, 3])
        spread(o, 2, whole, 0)
        spread(o, 2, whole, 1)

    def gather_pass(o):
        lo, hi = GROUP[o]
        for k in (0, 3, 1, 2):
            landed(weight.at[lo:hi, :, side_columns(o, 3, k)], e_s.at[o, k, 0], e_r.at[o, k, 0])
            half = weight.at[lo:hi, upper, side_columns(o, 3, k)]
            send(half, half, e_s.at[o, k, 2], e_r.at[o, k, 2], second(o, 1))
            landed(weight.at[lo:hi, :, side_columns(o, 1, k)], e_s.at[o, k, 1], e_r.at[o, k, 1])
            half = weight.at[lo:hi, lower, side_columns(o, 1, k)]
            send(half, half, e_s.at[o, k, 3], e_r.at[o, k, 3], second(o, 3))

    def gather_end(o):
        lo, hi = GROUP[o]
        for k in (0, 3, 1, 2):
            landed(weight.at[lo:hi, upper, side_columns(o, 2, k)], e_s.at[o, k, 2], e_r.at[o, k, 2])
            landed(weight.at[lo:hi, lower, side_columns(o, 2, k)], e_s.at[o, k, 3], e_r.at[o, k, 3])

    names = lax.broadcasted_iota(jnp.int32, (16, ROWS), 0)
    hit_0, hit_1 = names == ids[0:1, :], names == ids[1:2, :]
    hits = jnp.where(hit_0 | hit_1, 1.0, 0.0)
    before = lax.broadcasted_iota(jnp.int32, (ROWS, ROWS), 0) < lax.broadcasted_iota(jnp.int32, (ROWS, ROWS), 1)
    ranks = jnp.dot(hits.astype(bf16), jnp.where(before, 1.0, 0.0).astype(bf16), preferred_element_type=f32)
    slots = jnp.where(hits > 0.5, ranks, -1.0)
    values = jnp.where(hit_0, ways[0:1, :], 0.0) + jnp.where(hit_1, ways[1:2, :], 0.0)
    for e in range(16):
        table[e] = slots[e:e + 1, :]
        table[e + 16] = values[e:e + 1, :]

    gather_start(0)
    landed(halo, h_s.at[0], h_r.at[0])
    landed(halo_docs, h_s.at[1], h_r.at[1])
    inside = sp > 0
    gated[0:HALO, :] = jnp.where(inside, halo[...].astype(f32), 0.0)
    starts = []
    for i in range(3):
        extra = jnp.where(inside, halo_docs[i:i + 1, :], float(TAPS - 1)) - float(TAPS - 1)
        starts.append(local[i] + extra)

    CHUNK = 64

    def conv_block(dz):
        base = ((z + dz) % DEPTH) * 256

        def piece(i, _):
            row = pl.multiple_of(base + i * CHUNK, CHUNK)
            spot = lax.broadcasted_iota(jnp.int32, (CHUNK, 128), 0).astype(f32) + row.astype(f32)
            begun = jnp.full((CHUNK, 128), -1000.0, f32)
            for s in starts:
                begun = jnp.maximum(begun, jnp.where(s <= spot, s, -1000.0))
            age = spot - begun
            total = jnp.zeros((CHUNK, 128), f32)
            for j in range(TAPS):
                window = gated[pl.ds(row + (HALO - j), CHUNK), :]
                total = total + jnp.where(age >= float(j), window * tap32[j:j + 1, :], 0.0)
            conv[pl.ds(row, CHUNK), :] = total.astype(bf16)
            return 0

        lax.fori_loop(0, 256 // CHUNK, piece, 0)
        rows = pl.ds(pl.multiple_of(base, 256), 256)
        if dz == 0:
            conv_in[:, 0:128] = conv[rows, :]
        else:
            there = PLACE[(DEPTH - dz) % DEPTH]
            push(
                conv.at[rows, :], conv_in.at[:, there * 128:(there + 1) * 128],
                a_s.at[there], a_r.at[there], sp, along(dz),
            )

    for dz in (4, 3, 5):
        conv_block(dz)
    gather_near(0)
    for dz in (2, 6):
        conv_block(dz)
    gather_start(1)
    for dz in (1, 7):
        conv_block(dz)
    gather_far(0)
    conv_block(0)
    gather_near(1)
    gather_far(1)
    gather_pass(0)

    for there in range(1, DEPTH):
        landed(conv_in.at[:, there * 128:(there + 1) * 128], a_s.at[there], a_r.at[there])
    mean_part = jnp.zeros((256, 128), f32)
    square_part = jnp.zeros((256, 128), f32)
    for s in range(DEPTH):
        v = conv_in[:, s * 128:(s + 1) * 128].astype(f32)
        mean_part = mean_part + v
        square_part = square_part + v * v
    sums[0] = mean_part
    sums[1] = square_part
    push(sums, sums_in, st_s, st_r, sp, z * 2 + other)
    gather_pass(1)
    landed(sums_in, st_s, st_r)
    mean = jnp.sum(sums[0] + sums_in[0], 1, keepdims=True) * (1.0 / 2048.0)
    square = jnp.sum(sums[1] + sums_in[1], 1, keepdims=True) * (1.0 / 2048.0)
    scale = lax.rsqrt(square - mean * mean + EPSILON)
    for dz, s in PLACE.items():
        v = conv_in[:, s * 128:(s + 1) * 128].astype(f32)
        v = (v - mean) * scale * channel_gain[along(dz)]
        act[:, s * 128:(s + 1) * 128] = (v / (1.0 + jnp.exp(-v))).astype(bf16)

    gather_end(0)
    for n in range(4):
        w = weight[0:4, :, n * 512:(n + 1) * 512].reshape(512, 512)
        part[n] = jnp.dot(act[:, 0:512], w, preferred_element_type=f32).reshape(2, ROWS, 512)
    gather_end(1)
    for n in range(4):
        w = weight[4:8, :, n * 512:(n + 1) * 512].reshape(512, 512)
        got = jnp.dot(act[:, 512:1024], w, preferred_element_type=f32).reshape(2, ROWS, 512)
        part[n] = part[n] + got
        push(part.at[n, other], part_in2.at[n], x_s.at[n], x_r.at[n], sp, z * 2 + other)
    own_loads[3].wait()
    for n in range(4):
        cols = slice(n * 512, (n + 1) * 512)
        landed(part_in2.at[n], x_s.at[n], x_r.at[n])
        kept[:, cols] = RESIDUAL_SCALE * residual[:, cols].astype(f32) + part[n, core] + part_in2[n]
    normed[...] = (normalize(kept[...]) * mix_gain[...]).astype(bf16)

    for o in (0, 1):
        mine = normed.at[:, o * HALF:(o + 1) * HALF]
        send(table, meta.at[o, 3], m_s.at[o, 0], m_r.at[o, 0], first(o, 1))
        send(table, meta.at[o, 1], m_s.at[o, 1], m_r.at[o, 1], first(o, 3))
        send(mine, near.at[o, 3], s1_s.at[o, 0], s1_r.at[o, 0], first(o, 1))
        send(mine, near.at[o, 1], s1_s.at[o, 1], s1_r.at[o, 1], first(o, 3))

    lanes = lax.broadcasted_iota(jnp.int32, (CAP, 128), 0).astype(f32)

    def expert_at(o, k):
        return second(o, k)

    def slot_row(o, k, e):
        return table[e] if k == 0 else meta[o, k, e]

    def weight_row(o, k, e):
        return table[e + 16] if k == 0 else meta[o, k, e + 16]

    def pack(o, k):
        rows = normed[:, o * HALF:(o + 1) * HALF] if k == 0 else near[o, k]
        for q in (2, 1, 3, 0):
            hit = jnp.where(lanes == slot_row(o, k, expert_at(o, q)), 1.0, 0.0).astype(bf16)
            block = jnp.dot(hit, rows, preferred_element_type=f32).astype(bf16)
            if q == 0:
                arrived[o, 0, k] = block
            else:
                packed[o, q - 1, k] = block
            if q == 2:
                way = 1 if k < 2 else 3
                send(packed.at[o, 1, k], relay.at[o, k], rl_s.at[o, k], rl_r.at[o, k], second(o, way))
            if q == 1:
                send(packed.at[o, 0, k], arrived.at[o, 3, k], d_s.at[o, 0, k], d_r.at[o, 0, k], second(o, 1))
            if q == 3:
                send(packed.at[o, 2, k], arrived.at[o, 1, k], d_s.at[o, 1, k], d_r.at[o, 1, k], second(o, 3))

    def pass_on(o, k):
        landed(relay.at[o, k], rl_s.at[o, k], rl_r.at[o, k])
        way = 1 if k < 2 else 3
        send(relay.at[o, k], arrived.at[o, 2, k], fw_s.at[o, k], fw_r.at[o, k], second(o, way))

    for o in (0, 1):
        pack(o, 0)
    for o in (0, 1):
        landed(meta.at[o, 3], m_s.at[o, 0], m_r.at[o, 0])
        send(meta.at[o, 3], meta.at[o, 2], m_s.at[o, 2], m_r.at[o, 2], first(o, 1))
        landed(near.at[o, 3], s1_s.at[o, 0], s1_r.at[o, 0])
        send(near.at[o, 3, 0:64], near.at[o, 2, 0:64], s1_s.at[o, 2], s1_r.at[o, 2], first(o, 1))
    for o in (0, 1):
        landed(meta.at[o, 1], m_s.at[o, 1], m_r.at[o, 1])
        landed(near.at[o, 1], s1_s.at[o, 1], s1_r.at[o, 1])
        send(near.at[o, 1, 64:128], near.at[o, 2, 64:128], s1_s.at[o, 3], s1_r.at[o, 3], first(o, 3))
    for k in (3, 1):
        for o in (0, 1):
            pack(o, k)
    for o in (0, 1):
        pass_on(o, 0)
    for o in (0, 1):
        landed(meta.at[o, 2], m_s.at[o, 2], m_r.at[o, 2])
        landed(near.at[o, 2, 0:64], s1_s.at[o, 2], s1_r.at[o, 2])
        landed(near.at[o, 2, 64:128], s1_s.at[o, 3], s1_r.at[o, 3])
        pack(o, 2)

    for load in loads[:3]:
        load.wait()
    act = jnp.dot(normed[...], sg[...], preferred_element_type=f32)
    lin = jnp.dot(normed[...], su[...], preferred_element_type=f32)
    common = (act / (1.0 + jnp.exp(-act)) * lin).astype(bf16)
    shared[...] = jnp.dot(common, sd[...], preferred_element_type=f32)
    for k in (3, 1, 2):
        for o in (0, 1):
            pass_on(o, k)
    for load in loads[3:]:
        load.wait()

    def product(o, q):
        rows = arrived[o, q].reshape(SIDE * CAP, HALF)
        for acc, w in ((acc_g, wg), (acc_u, wu)):
            got = jnp.dot(rows, w[o * HALF:(o + 1) * HALF, :], preferred_element_type=f32)
            got = got.reshape(SIDE, CAP, 512)
            if o == 0:
                acc[q] = got
            else:
                acc[:, q] = acc[:, q] + got

    def from_side(q, d):
        for k in range(SIDE):
            for o in (0, 1):
                landed(arrived.at[o, q, k], d_s.at[o, d, k], d_r.at[o, d, k])

    product(0, 0)
    from_side(3, 0)
    product(0, 3)
    from_side(1, 1)
    product(0, 1)
    for k in (0, 3, 1, 2):
        landed(arrived.at[0, 2, k], fw_s.at[0, k], fw_r.at[0, k])
    product(0, 2)
    product(1, 0)
    product(1, 3)
    product(1, 1)
    for k in (0, 3, 1, 2):
        landed(arrived.at[1, 2, k], fw_s.at[1, k], fw_r.at[1, k])
    product(1, 2)

    def give_back(o, q, k, block):
        if q == 0:
            back[o, k, 0] = block
            return
        answers[o, q - 1, k] = block
        mine = answers.at[o, q - 1, k]
        if q == 2:
            way = 1 if k < 2 else 3
            send(mine, relay_back.at[o, k], bl_s.at[o, k], bl_r.at[o, k], second(o, way))
        else:
            d = 0 if q == 1 else 1
            send(mine, back.at[o, k, SIDE - q], b_s.at[o, d, k], b_r.at[o, d, k], second(o, q))

    def pass_back(o, k):
        landed(relay_back.at[o, k], bl_s.at[o, k], bl_r.at[o, k])
        way = 1 if k < 2 else 3
        send(relay_back.at[o, k], back.at[o, k, 2], bf_s.at[o, k], bf_r.at[o, k], second(o, way))

    for dx in (2, 1, 3, 0):
        g = acc_g[:, dx].reshape(SIDE * CAP, 512)
        u = acc_u[:, dx].reshape(SIDE * CAP, 512)
        hidden = (g / (1.0 + jnp.exp(-g)) * u).astype(bf16)
        for o in (0, 1):
            ans = jnp.dot(
                hidden, wd[:, o * HALF:(o + 1) * HALF], preferred_element_type=f32
            ).astype(bf16)
            for dy in (2, 1, 3, 0):
                block = ans[dy * CAP:(dy + 1) * CAP]
                if o == 0:
                    give_back(0, dy, dx, block)
                else:
                    give_back(1, dx, dy, block)

    def choose(o, k, part):
        rows = []
        for j in range(SIDE):
            e = expert_at(o, j)
            w = weight_row(o, k, e)
            high = w.astype(bf16).astype(f32)
            value = high if part == 0 else w - high
            rows.append(jnp.where(lanes == slot_row(o, k, e), value, 0.0).astype(bf16))
        return jnp.concatenate(rows, 0)

    def combine(o, k):
        for j, d in ((3, 0), (1, 1)):
            landed(back.at[o, k, j], b_s.at[o, d, k], b_r.at[o, d, k])
        landed(back.at[o, k, 2], bf_s.at[o, k], bf_r.at[o, k])
        rows = back[o, k].reshape(SIDE * CAP, HALF)
        dims = (((0,), (0,)), ((), ()))
        total = lax.dot_general(choose(o, k, 0), rows, dims, preferred_element_type=f32)
        return total + lax.dot_general(choose(o, k, 1), rows, dims, preferred_element_type=f32)

    for k in (2, 1, 3, 0):
        for o in (0, 1):
            pass_back(o, k)
    for k in (2, 1, 3):
        for o in (0, 1):
            partial[o, k - 1] = combine(o, k).astype(bf16)
            mine = partial.at[o, k - 1]
            if k == 2:
                send(mine.at[0:64], relay_part.at[o, 0], p_s.at[o, 2], p_r.at[o, 2], first(o, 1))
                send(mine.at[64:128], relay_part.at[o, 1], p_s.at[o, 3], p_r.at[o, 3], first(o, 3))
            elif k == 1:
                send(mine, part_in.at[o, 2], p_s.at[o, 0], p_r.at[o, 0], first(o, 1))
            else:
                send(mine, part_in.at[o, 0], p_s.at[o, 1], p_r.at[o, 1], first(o, 3))
    for o in (0, 1):
        landed(relay_part.at[o, 0], p_s.at[o, 2], p_r.at[o, 2])
        send(relay_part.at[o, 0], part_in.at[o, 1, 0:64], p_s.at[o, 4], p_r.at[o, 4], first(o, 1))
        landed(relay_part.at[o, 1], p_s.at[o, 3], p_r.at[o, 3])
        send(relay_part.at[o, 1], part_in.at[o, 1, 64:128], p_s.at[o, 5], p_r.at[o, 5], first(o, 3))
    for o in (0, 1):
        kept[:, o * HALF:(o + 1) * HALF] = combine(o, 0)
    for o in (0, 1):
        landed(part_in.at[o, 2], p_s.at[o, 0], p_r.at[o, 0])
        landed(part_in.at[o, 0], p_s.at[o, 1], p_r.at[o, 1])
        landed(part_in.at[o, 1, 0:64], p_s.at[o, 4], p_r.at[o, 4])
        landed(part_in.at[o, 1, 64:128], p_s.at[o, 5], p_r.at[o, 5])
        here = slice(o * HALF, (o + 1) * HALF)
        kept[:, here] = (
            kept[:, here] + part_in[o, 0].astype(f32) + part_in[o, 1].astype(f32) + part_in[o, 2].astype(f32)
        )
    values = RESIDUAL_SCALE * normed[...].astype(f32) + kept[...] + shared[...]
    out[...] = (normalize(values) * gain[...]).astype(bf16)
    for copy in sent:
        copy.wait_send()


def shards(
    linear_part, gate_part, kernel_taps, channel_gain, output_weight, residual, mix_gain, documents,
    expert_ids, route_weights, expert_gate, expert_up, expert_down, shared_gate, shared_up, shared_down,
    final_gain,
):
    bf16, f32 = jnp.bfloat16, jnp.float32
    dma = pltpu.SemaphoreType.DMA
    vmem = pl.BlockSpec(memory_space=pltpu.VMEM)
    hbm = pl.BlockSpec(memory_space=pl.ANY)
    block = (CAP, HALF)
    w_gate, w_up, w_down = expert_gate[0], expert_up[0], expert_down[0]
    args = (
        (linear_part, hbm), (gate_part, hbm), (kernel_taps, vmem), (channel_gain.reshape(16, 1, 128), vmem),
        (output_weight, hbm), (residual, hbm), (mix_gain[None, :], vmem), (documents.reshape(16, 128), vmem),
        (expert_ids.T, vmem), (route_weights.T, vmem), (final_gain[None, :], vmem),
        (w_gate, hbm), (w_up, hbm), (w_down, hbm), (shared_gate, hbm), (shared_up, hbm), (shared_down, hbm),
    )
    return pl.pallas_call(
        layer_kernel,
        out_shape=jax.ShapeDtypeStruct(residual.shape, bf16),
        in_specs=[spec for _, spec in args],
        out_specs=vmem,
        scratch_shapes=[
            pltpu.VMEM((2048, 128), bf16),
            pltpu.VMEM((2048, 128), bf16),
            pltpu.VMEM((ROWS, 2048), bf16),
            pltpu.VMEM((DEPTH, 128, 2048), bf16),
            pltpu.VMEM((2048 + HALO, 128), f32),
            pltpu.VMEM((HALO, 128), bf16),
            pltpu.VMEM((8, 128), f32),
            pltpu.VMEM((HALO, 128), bf16),
            pltpu.VMEM((8, 128), f32),
            pltpu.VMEM((32, 128), f32),
            pltpu.VMEM((2048, 128), bf16),
            pltpu.VMEM((256, HALF), bf16),
            pltpu.VMEM((256, HALF), bf16),
            pltpu.VMEM((2, 256, 128), f32),
            pltpu.VMEM((2, 256, 128), f32),
            pltpu.VMEM((4, 2, ROWS, 512), f32),
            pltpu.VMEM((4, ROWS, 512), f32),
            pltpu.VMEM((ROWS, 2048), bf16),
            pltpu.VMEM((32, 1, 128), f32),
            pltpu.VMEM(w_gate.shape, bf16),
            pltpu.VMEM(w_up.shape, bf16),
            pltpu.VMEM(w_down.shape, bf16),
            pltpu.VMEM(shared_gate.shape, bf16),
            pltpu.VMEM(shared_up.shape, bf16),
            pltpu.VMEM(shared_down.shape, bf16),
            pltpu.VMEM((2, 4, ROWS, HALF), bf16),
            pltpu.VMEM((2, 4, 32, 1, 128), f32),
            pltpu.VMEM((2, 3, 4) + block, bf16),
            pltpu.VMEM((2, 4) + block, bf16),
            pltpu.VMEM((2, 4, 4) + block, bf16),
            pltpu.VMEM((4, 4, CAP, 512), f32),
            pltpu.VMEM((4, 4, CAP, 512), f32),
            pltpu.VMEM((2, 3, 4) + block, bf16),
            pltpu.VMEM((2, 4) + block, bf16),
            pltpu.VMEM((2, 4, 4) + block, bf16),
            pltpu.VMEM((2, 3, ROWS, HALF), bf16),
            pltpu.VMEM((2, 2) + block, bf16),
            pltpu.VMEM((2, 3, ROWS, HALF), bf16),
            pltpu.VMEM((ROWS, 2048), f32),
            pltpu.VMEM((ROWS, 2048), f32),
            dma((4,)), dma((8,)), dma((8,)), dma((2,)), dma((2,)), dma((8,)), dma((8,)),
            dma((2, 4)), dma((2, 4)), dma((1,)), dma((1,)), dma((2, 4, 4)), dma((2, 4, 4)),
            dma, dma, dma((4,)), dma((4,)),
            dma((6,)),
            dma((2, 4)), dma((2, 4)), dma((2, 3)), dma((2, 3)),
            dma((2, 2, 4)), dma((2, 2, 4)), dma((2, 4)), dma((2, 4)), dma((2, 4)), dma((2, 4)),
            dma((2, 2, 4)), dma((2, 2, 4)), dma((2, 4)), dma((2, 4)), dma((2, 4)), dma((2, 4)),
            dma((2, 6)), dma((2, 6)),
        ],
        compiler_params=pltpu.CompilerParams(
            collective_id=0, has_side_effects=True, vmem_limit_bytes=63 * 1024 * 1024
        ),
    )(*[a for a, _ in args])


def solution(mesh):
    both = P(("sp", "tp"), None)
    placed = (
        P("sp", "tp"), P("sp", "tp"), P(None, "tp"), P(), P("tp", None), both, P(), P("sp"), both, both,
        P("sp", None, None), P("sp", None, None), P("sp", None, None), P(), P(), P(), P(),
    )
    return jax.shard_map(shards, mesh=mesh, in_specs=placed, out_specs=both, check_vma=False)
```

```python
import jax
import jax.numpy as jnp
from jax import lax
from jax.experimental import pallas as pl
from jax.experimental.pallas import tpu as pltpu
from jax.sharding import PartitionSpec as P

EPSILON = 1e-05
RESIDUAL_SCALE = 8.0**0.25
MESH_ID = pl.DeviceIdType.MESH
HALF = 1024
SIDE = 4
DEPTH = 8
CAP = 64
ROWS = 128
HALO = 32
TAPS = 31
PLACE = {0: 0, 1: 1, 7: 2, 2: 3, 6: 4, 3: 5, 5: 6, 4: 7}
GROUP = ((1, 5), (5, 8))


def normalize(values):
    mean = jnp.mean(values, -1, keepdims=True)
    square = jnp.mean(values * values, -1, keepdims=True)
    return (values - mean) * lax.rsqrt(square - mean * mean + EPSILON)


def layer_kernel(
    linear_h, gate_h, taps, channel_gain, w_h, residual_h, mix_gain, docs, ids, ways, gain,
    w_gate, w_up, w_down, s_gate, s_up, s_down, out,
    linear, gate, residual, weight, gated, tail, tail_docs, halo, halo_docs, tap32, conv, conv_in, act,
    sums, sums_in, part, part_in2, normed, table,
    wg, wu, wd, sg, su, sd,
    near, meta, packed, relay, arrived, acc_g, acc_u, hidden, answers, relay_back, back, partial, relay_part, part_in,
    kept, shared,
    l_sem, z_s, z_r, h_s, h_r, a_s, a_r, g_s, g_r, f_s, f_r, e_s, e_r, st_s, st_r, x_s, x_r,
    w_sem, s1_s, s1_r, m_s, m_r, d_s, d_r, rl_s, rl_r, fw_s, fw_r,
    b_s, b_r, bl_s, bl_r, bf_s, bf_r, p_s, p_r,
):
    f32, bf16 = jnp.float32, jnp.bfloat16
    sp, tp = lax.axis_index("sp"), lax.axis_index("tp")
    y, x = sp // SIDE, sp % SIDE
    z, core = tp // 2, tp % 2
    other = 1 - core

    def at(dy, dx):
        return ((y + dy) % SIDE) * SIDE + (x + dx) % SIDE

    def first(o, k):
        return at(0, k) if o == 0 else at(k, 0)

    def second(o, k):
        return at(k, 0) if o == 0 else at(0, k)

    def along(dz):
        return ((z + dz) % DEPTH) * 2 + core

    def push(src, dst, ss, rs, to_sp, to_tp):
        copy = pltpu.make_async_remote_copy(
            src_ref=src, dst_ref=dst, send_sem=ss, recv_sem=rs,
            device_id=(to_sp, to_tp), device_id_type=MESH_ID,
        )
        copy.start()
        sent.append(copy)

    def send(src, dst, ss, rs, to):
        push(src, dst, ss, rs, to, tp)

    def landed(dst, ss, rs):
        pltpu.make_async_remote_copy(
            src_ref=dst, dst_ref=dst, send_sem=ss, recv_sem=rs,
            device_id=(first(0, 1), tp), device_id_type=MESH_ID,
        ).wait_recv()

    sent = []
    own_loads = [
        pltpu.make_async_copy(a, b, l_sem.at[i])
        for i, (a, b) in enumerate(
            [(w_h, weight.at[0]), (linear_h, linear), (gate_h, gate), (residual_h, residual)]
        )
    ]
    for load in own_loads:
        load.start()
    loads = [
        pltpu.make_async_copy(a, b, w_sem.at[i])
        for i, (a, b) in enumerate(
            [(s_gate, sg), (s_up, su), (s_down, sd), (w_gate, wg), (w_up, wu), (w_down, wd)]
        )
    ]

    after, ahead = (sp + 1) % 16, (sp + 15) % 16
    barrier = pltpu.get_barrier_semaphore()

    def greet(to_sp, to_tp):
        pl.semaphore_signal(barrier, inc=1, device_id=(to_sp, to_tp), device_id_type=MESH_ID)

    for dz in range(1, DEPTH):
        greet(sp, along(dz))
    for to in (at(0, 1), at(0, 3), at(1, 0), at(3, 0), after, ahead):
        greet(to, tp)
    greet(sp, z * 2 + other)
    pl.semaphore_wait(barrier, 14)

    def columns(o, k, width=1):
        fast, slow = (x, y) if o == 0 else (y, x)
        return pl.ds(pl.multiple_of((slow * SIDE + (fast + k) % SIDE) * 128, 128), 128)

    def side_columns(o, ks, kf):
        fast, slow = (x, y) if o == 0 else (y, x)
        block = ((slow + ks) % SIDE) * SIDE + (fast + kf) % SIDE
        return pl.ds(pl.multiple_of(block * 128, 128), 128)

    own_loads[0].wait()
    for dz in (7, 1, 6, 2, 5, 3, 4):
        there = PLACE[(DEPTH - dz) % DEPTH]
        o = 0 if there < GROUP[0][1] else 1
        cols = columns(o, 0)
        push(weight.at[0, :, cols], weight.at[there, :, cols], z_s.at[there], z_r.at[there], sp, along(dz))

    own_loads[1].wait()
    own_loads[2].wait()

    def gate_rows(a, b):
        a, b = a.astype(f32), b.astype(f32)
        return (a * (1.0 / (1.0 + jnp.exp(-b)))).astype(bf16)

    tail[...] = gate_rows(linear[2048 - HALO:, :], gate[2048 - HALO:, :])
    doc = docs[...]
    spot = lax.broadcasted_iota(jnp.int32, (16, 128), 0) * 128 + lax.broadcasted_iota(jnp.int32, (16, 128), 1)
    local, last = [], []
    for d in (1, 2, 3):
        below = jnp.where(doc < d, 1.0, 0.0)
        local.append(jnp.sum(jnp.sum(below, 1, keepdims=True), 0, keepdims=True))
        below = jnp.where(spot >= 2048 - (TAPS - 1), below, 0.0)
        last.append(jnp.sum(jnp.sum(below, 1, keepdims=True), 0, keepdims=True))
    for i in range(3):
        tail_docs[i:i + 1, :] = jnp.broadcast_to(last[i], (1, 128))
    tail_docs[3:8, :] = jnp.zeros((5, 128), f32)
    push(tail, halo, h_s.at[0], h_r.at[0], after, tp)
    push(tail_docs, halo_docs, h_s.at[1], h_r.at[1], after, tp)
    for load in loads:
        load.start()

    def gate_block(i, _):
        rows = pl.ds(pl.multiple_of(i * 128, 128), 128)
        there = pl.ds(pl.multiple_of(i * 128 + HALO, 32), 128)
        gated[there, :] = gate_rows(linear[rows, :], gate[rows, :]).astype(f32)
        return 0

    lax.fori_loop(0, 16, gate_block, 0)
    tap32[0:TAPS, :] = taps[...].astype(f32)

    def spread(o, k, rows, i):
        lo, hi = GROUP[o]
        mine = weight.at[lo:hi, rows, side_columns(o, 0, k)]
        send(mine, mine, e_s.at[o, k, i], e_r.at[o, k, i], second(o, 1 if i % 2 == 0 else 3))

    whole, upper, lower = slice(0, 128), slice(0, 64), slice(64, 128)

    def gather_start(o):
        lo, hi = GROUP[o]
        mine = weight.at[lo:hi, :, columns(o, 0)]
        for there in range(lo, hi):
            landed(weight.at[there, :, columns(o, 0)], z_s.at[there], z_r.at[there])
        send(mine, mine, g_s.at[o, 0], g_r.at[o, 0], first(o, 1))
        send(mine, mine, g_s.at[o, 1], g_r.at[o, 1], first(o, 3))
        spread(o, 0, whole, 0)
        spread(o, 0, whole, 1)

    def gather_near(o):
        lo, hi = GROUP[o]
        landed(weight.at[lo:hi, :, columns(o, 3)], g_s.at[o, 0], g_r.at[o, 0])
        half = weight.at[lo:hi, upper, columns(o, 3)]
        send(half, half, g_s.at[o, 2], g_r.at[o, 2], first(o, 1))
        spread(o, 3, whole, 0)
        spread(o, 3, whole, 1)
        landed(weight.at[lo:hi, :, columns(o, 1)], g_s.at[o, 1], g_r.at[o, 1])
        half = weight.at[lo:hi, lower, columns(o, 1)]
        send(half, half, g_s.at[o, 3], g_r.at[o, 3], first(o, 3))
        spread(o, 1, whole, 0)
        spread(o, 1, whole, 1)

    def gather_far(o):
        lo, hi = GROUP[o]
        landed(weight.at[lo:hi, upper, columns(o, 2)], g_s.at[o, 2], g_r.at[o, 2])
        landed(weight.at[lo:hi, lower, columns(o, 2)], g_s.at[o, 3], g_r.at[o, 3])
        spread(o, 2, whole, 0)
        spread(o, 2, whole, 1)

    def gather_pass(o):
        lo, hi = GROUP[o]
        for k in (0, 3, 1, 2):
            landed(weight.at[lo:hi, :, side_columns(o, 3, k)], e_s.at[o, k, 0], e_r.at[o, k, 0])
            half = weight.at[lo:hi, upper, side_columns(o, 3, k)]
            send(half, half, e_s.at[o, k, 2], e_r.at[o, k, 2], second(o, 1))
            landed(weight.at[lo:hi, :, side_columns(o, 1, k)], e_s.at[o, k, 1], e_r.at[o, k, 1])
            half = weight.at[lo:hi, lower, side_columns(o, 1, k)]
            send(half, half, e_s.at[o, k, 3], e_r.at[o, k, 3], second(o, 3))

    def gather_end(o):
        lo, hi = GROUP[o]
        for k in (0, 3, 1, 2):
            landed(weight.at[lo:hi, upper, side_columns(o, 2, k)], e_s.at[o, k, 2], e_r.at[o, k, 2])
            landed(weight.at[lo:hi, lower, side_columns(o, 2, k)], e_s.at[o, k, 3], e_r.at[o, k, 3])

    names = lax.broadcasted_iota(jnp.int32, (16, ROWS), 0)
    hit_0, hit_1 = names == ids[0:1, :], names == ids[1:2, :]
    hits = jnp.where(hit_0 | hit_1, 1.0, 0.0)
    before = lax.broadcasted_iota(jnp.int32, (ROWS, ROWS), 0) < lax.broadcasted_iota(jnp.int32, (ROWS, ROWS), 1)
    ranks = jnp.dot(hits.astype(bf16), jnp.where(before, 1.0, 0.0).astype(bf16), preferred_element_type=f32)
    slots = jnp.where(hits > 0.5, ranks, -1.0)
    values = jnp.where(hit_0, ways[0:1, :], 0.0) + jnp.where(hit_1, ways[1:2, :], 0.0)
    for e in range(16):
        table[e] = slots[e:e + 1, :]
        table[e + 16] = values[e:e + 1, :]

    gather_start(0)
    landed(halo, h_s.at[0], h_r.at[0])
    landed(halo_docs, h_s.at[1], h_r.at[1])
    inside = sp > 0
    gated[0:HALO, :] = jnp.where(inside, halo[...].astype(f32), 0.0)
    starts = []
    for i in range(3):
        extra = jnp.where(inside, halo_docs[i:i + 1, :], float(TAPS - 1)) - float(TAPS - 1)
        starts.append(local[i] + extra)

    CHUNK = 64

    def conv_block(dz):
        base = ((z + dz) % DEPTH) * 256

        def piece(i, _):
            row = pl.multiple_of(base + i * CHUNK, CHUNK)
            spot = lax.broadcasted_iota(jnp.int32, (CHUNK, 128), 0).astype(f32) + row.astype(f32)
            begun = jnp.full((CHUNK, 128), -1000.0, f32)
            for s in starts:
                begun = jnp.maximum(begun, jnp.where(s <= spot, s, -1000.0))
            age = spot - begun
            total = jnp.zeros((CHUNK, 128), f32)
            for j in range(TAPS):
                window = gated[pl.ds(row + (HALO - j), CHUNK), :]
                total = total + jnp.where(age >= float(j), window * tap32[j:j + 1, :], 0.0)
            conv[pl.ds(row, CHUNK), :] = total.astype(bf16)
            return 0

        lax.fori_loop(0, 256 // CHUNK, piece, 0)
        rows = pl.ds(pl.multiple_of(base, 256), 256)
        if dz == 0:
            conv_in[:, 0:128] = conv[rows, :]
        else:
            there = PLACE[(DEPTH - dz) % DEPTH]
            push(
                conv.at[rows, :], conv_in.at[:, there * 128:(there + 1) * 128],
                a_s.at[there], a_r.at[there], sp, along(dz),
            )

    for dz in (4, 3, 5):
        conv_block(dz)
    gather_near(0)
    for dz in (2, 6):
        conv_block(dz)
    gather_start(1)
    for dz in (1, 7):
        conv_block(dz)
    gather_far(0)
    conv_block(0)
    gather_near(1)
    gather_far(1)
    gather_pass(0)

    for there in range(1, DEPTH):
        landed(conv_in.at[:, there * 128:(there + 1) * 128], a_s.at[there], a_r.at[there])
    mean_part = jnp.zeros((256, 128), f32)
    square_part = jnp.zeros((256, 128), f32)
    for s in range(DEPTH):
        v = conv_in[:, s * 128:(s + 1) * 128].astype(f32)
        mean_part = mean_part + v
        square_part = square_part + v * v
    sums[0] = mean_part
    sums[1] = square_part
    push(sums, sums_in, st_s, st_r, sp, z * 2 + other)
    gather_pass(1)
    landed(sums_in, st_s, st_r)
    mean = jnp.sum(sums[0] + sums_in[0], 1, keepdims=True) * (1.0 / 2048.0)
    square = jnp.sum(sums[1] + sums_in[1], 1, keepdims=True) * (1.0 / 2048.0)
    scale = lax.rsqrt(square - mean * mean + EPSILON)
    for dz, s in PLACE.items():
        v = conv_in[:, s * 128:(s + 1) * 128].astype(f32)
        v = (v - mean) * scale * channel_gain[along(dz)]
        act[:, s * 128:(s + 1) * 128] = (v / (1.0 + jnp.exp(-v))).astype(bf16)

    gather_end(0)
    for n in range(4):
        w = weight[0:4, :, n * 512:(n + 1) * 512].reshape(512, 512)
        part[n] = jnp.dot(act[:, 0:512], w, preferred_element_type=f32).reshape(2, ROWS, 512)
    gather_end(1)
    for n in range(4):
        w = weight[4:8, :, n * 512:(n + 1) * 512].reshape(512, 512)
        got = jnp.dot(act[:, 512:1024], w, preferred_element_type=f32).reshape(2, ROWS, 512)
        part[n] = part[n] + got
        push(part.at[n, other], part_in2.at[n], x_s.at[n], x_r.at[n], sp, z * 2 + other)
    own_loads[3].wait()
    for n in range(4):
        cols = slice(n * 512, (n + 1) * 512)
        landed(part_in2.at[n], x_s.at[n], x_r.at[n])
        kept[:, cols] = RESIDUAL_SCALE * residual[:, cols].astype(f32) + part[n, core] + part_in2[n]
    normed[...] = (normalize(kept[...]) * mix_gain[...]).astype(bf16)

    for o in (0, 1):
        mine = normed.at[:, o * HALF:(o + 1) * HALF]
        send(table, meta.at[o, 3], m_s.at[o, 0], m_r.at[o, 0], first(o, 1))
        send(table, meta.at[o, 1], m_s.at[o, 1], m_r.at[o, 1], first(o, 3))
        send(mine, near.at[o, 3], s1_s.at[o, 0], s1_r.at[o, 0], first(o, 1))
        send(mine, near.at[o, 1], s1_s.at[o, 1], s1_r.at[o, 1], first(o, 3))

    lanes = lax.broadcasted_iota(jnp.int32, (CAP, 128), 0).astype(f32)

    def expert_at(o, k):
        return second(o, k)

    def slot_row(o, k, e):
        return table[e] if k == 0 else meta[o, k, e]

    def weight_row(o, k, e):
        return table[e + 16] if k == 0 else meta[o, k, e + 16]

    def pack(o, k):
        rows = normed[:, o * HALF:(o + 1) * HALF] if k == 0 else near[o, k]
        for q in (2, 1, 3, 0):
            hit = jnp.where(lanes == slot_row(o, k, expert_at(o, q)), 1.0, 0.0).astype(bf16)
            block = jnp.dot(hit, rows, preferred_element_type=f32).astype(bf16)
            if q == 0:
                arrived[o, 0, k] = block
            else:
                packed[o, q - 1, k] = block
            if q == 2:
                way = 1 if k < 2 else 3
                send(packed.at[o, 1, k], relay.at[o, k], rl_s.at[o, k], rl_r.at[o, k], second(o, way))
            if q == 1:
                send(packed.at[o, 0, k], arrived.at[o, 3, k], d_s.at[o, 0, k], d_r.at[o, 0, k], second(o, 1))
            if q == 3:
                send(packed.at[o, 2, k], arrived.at[o, 1, k], d_s.at[o, 1, k], d_r.at[o, 1, k], second(o, 3))

    def pass_on(o, k):
        landed(relay.at[o, k], rl_s.at[o, k], rl_r.at[o, k])
        way = 1 if k < 2 else 3
        send(relay.at[o, k], arrived.at[o, 2, k], fw_s.at[o, k], fw_r.at[o, k], second(o, way))

    for o in (0, 1):
        pack(o, 0)
    for o in (0, 1):
        landed(meta.at[o, 3], m_s.at[o, 0], m_r.at[o, 0])
        send(meta.at[o, 3], meta.at[o, 2], m_s.at[o, 2], m_r.at[o, 2], first(o, 1))
        landed(near.at[o, 3], s1_s.at[o, 0], s1_r.at[o, 0])
        send(near.at[o, 3, 0:64], near.at[o, 2, 0:64], s1_s.at[o, 2], s1_r.at[o, 2], first(o, 1))
    for o in (0, 1):
        landed(meta.at[o, 1], m_s.at[o, 1], m_r.at[o, 1])
        landed(near.at[o, 1], s1_s.at[o, 1], s1_r.at[o, 1])
        send(near.at[o, 1, 64:128], near.at[o, 2, 64:128], s1_s.at[o, 3], s1_r.at[o, 3], first(o, 3))
    for k in (3, 1):
        for o in (0, 1):
            pack(o, k)
    for o in (0, 1):
        pass_on(o, 0)
    for o in (0, 1):
        landed(meta.at[o, 2], m_s.at[o, 2], m_r.at[o, 2])
        landed(near.at[o, 2, 0:64], s1_s.at[o, 2], s1_r.at[o, 2])
        landed(near.at[o, 2, 64:128], s1_s.at[o, 3], s1_r.at[o, 3])
        pack(o, 2)

    acc_g[...] = jnp.zeros_like(acc_g)
    acc_u[...] = jnp.zeros_like(acc_u)
    for load in loads[:3]:
        load.wait()
    act = jnp.dot(normed[...], sg[...], preferred_element_type=f32)
    lin = jnp.dot(normed[...], su[...], preferred_element_type=f32)
    common = (act / (1.0 + jnp.exp(-act)) * lin).astype(bf16)
    shared[...] = jnp.dot(common, sd[...], preferred_element_type=f32)
    for k in (3, 1):
        for o in (0, 1):
            pass_on(o, k)
    for load in loads[3:]:
        load.wait()

    def product(o, k):
        landed(arrived.at[o, 3, k], d_s.at[o, 0, k], d_r.at[o, 0, k])
        landed(arrived.at[o, 1, k], d_s.at[o, 1, k], d_r.at[o, 1, k])
        landed(arrived.at[o, 2, k], fw_s.at[o, k], fw_r.at[o, k])
        rows = arrived[o, :, k].reshape(SIDE * CAP, HALF)
        for acc, w in ((acc_g, wg), (acc_u, wu)):
            got = jnp.dot(rows, w[o * HALF:(o + 1) * HALF, :], preferred_element_type=f32)
            got = got.reshape(SIDE, CAP, 512)
            if o == 0:
                acc[:, k] = acc[:, k] + got
            else:
                acc[k] = acc[k] + got

    for o in (0, 1):
        product(o, 0)
    for o in (0, 1):
        pass_on(o, 2)
    for k in (3, 1, 2):
        for o in (0, 1):
            product(o, k)

    def give_back(o, q, k, block):
        if q == 0:
            back[o, k, 0] = block
            return
        answers[o, q - 1, k] = block
        mine = answers.at[o, q - 1, k]
        if q == 2:
            way = 1 if k < 2 else 3
            send(mine, relay_back.at[o, k], bl_s.at[o, k], bl_r.at[o, k], second(o, way))
        else:
            d = 0 if q == 1 else 1
            send(mine, back.at[o, k, SIDE - q], b_s.at[o, d, k], b_r.at[o, d, k], second(o, q))

    def pass_back(o, k):
        landed(relay_back.at[o, k], bl_s.at[o, k], bl_r.at[o, k])
        way = 1 if k < 2 else 3
        send(relay_back.at[o, k], back.at[o, k, 2], bf_s.at[o, k], bf_r.at[o, k], second(o, way))

    ready = set()

    def hide(dy, dx):
        if (dy, dx) not in ready:
            ready.add((dy, dx))
            g = acc_g[dy, dx]
            hidden[dy, dx] = (g / (1.0 + jnp.exp(-g)) * acc_u[dy, dx]).astype(bf16)

    for k in (2, 1, 3, 0):
        for o in (0, 1):
            for q in range(SIDE):
                hide(*((q, k) if o == 0 else (k, q)))
            rows = (hidden[:, k] if o == 0 else hidden[k]).reshape(SIDE * CAP, 512)
            ans = jnp.dot(rows, wd[:, o * HALF:(o + 1) * HALF], preferred_element_type=f32).astype(bf16)
            for q in (2, 1, 3, 0):
                give_back(o, q, k, ans[q * CAP:(q + 1) * CAP])

    def choose(o, k, part):
        rows = []
        for j in range(SIDE):
            e = expert_at(o, j)
            w = weight_row(o, k, e)
            high = w.astype(bf16).astype(f32)
            value = high if part == 0 else w - high
            rows.append(jnp.where(lanes == slot_row(o, k, e), value, 0.0).astype(bf16))
        return jnp.concatenate(rows, 0)

    def combine(o, k):
        for j, d in ((3, 0), (1, 1)):
            landed(back.at[o, k, j], b_s.at[o, d, k], b_r.at[o, d, k])
        landed(back.at[o, k, 2], bf_s.at[o, k], bf_r.at[o, k])
        rows = back[o, k].reshape(SIDE * CAP, HALF)
        dims = (((0,), (0,)), ((), ()))
        total = lax.dot_general(choose(o, k, 0), rows, dims, preferred_element_type=f32)
        return total + lax.dot_general(choose(o, k, 1), rows, dims, preferred_element_type=f32)

    def pass_sum(o, k):
        total = combine(o, k)
        mine = partial.at[o, k - 1]
        if k == 2:
            partial[o, k - 1] = total.astype(bf16)
            send(mine.at[0:64], relay_part.at[o, 0], p_s.at[o, 2], p_r.at[o, 2], first(o, 1))
            send(mine.at[64:128], relay_part.at[o, 1], p_s.at[o, 3], p_r.at[o, 3], first(o, 3))
        elif k == 1:
            landed(relay_part.at[o, 0], p_s.at[o, 2], p_r.at[o, 2])
            partial[o, k - 1, 0:64] = (total[0:64] + relay_part[o, 0].astype(f32)).astype(bf16)
            partial[o, k - 1, 64:128] = total[64:128].astype(bf16)
            send(mine, part_in.at[o, 0], p_s.at[o, 0], p_r.at[o, 0], first(o, 1))
        else:
            landed(relay_part.at[o, 1], p_s.at[o, 3], p_r.at[o, 3])
            partial[o, k - 1, 0:64] = total[0:64].astype(bf16)
            partial[o, k - 1, 64:128] = (total[64:128] + relay_part[o, 1].astype(f32)).astype(bf16)
            send(mine, part_in.at[o, 1], p_s.at[o, 1], p_r.at[o, 1], first(o, 3))

    for step, k in (
        (pass_back, 2), (pass_back, 1), (pass_sum, 2), (pass_back, 3), (pass_sum, 1), (pass_back, 0), (pass_sum, 3)
    ):
        for o in (0, 1):
            step(o, k)
    for o in (0, 1):
        kept[:, o * HALF:(o + 1) * HALF] = combine(o, 0)
    for o in (0, 1):
        landed(part_in.at[o, 0], p_s.at[o, 0], p_r.at[o, 0])
        landed(part_in.at[o, 1], p_s.at[o, 1], p_r.at[o, 1])
        here = slice(o * HALF, (o + 1) * HALF)
        kept[:, here] = kept[:, here] + part_in[o, 0].astype(f32) + part_in[o, 1].astype(f32)
    values = RESIDUAL_SCALE * normed[...].astype(f32) + kept[...] + shared[...]
    out[...] = normalize(values) * gain[...]
    for copy in sent:
        copy.wait_send()


def shards(
    linear_part, gate_part, kernel_taps, channel_gain, output_weight, residual, mix_gain, documents,
    expert_ids, route_weights, expert_gate, expert_up, expert_down, shared_gate, shared_up, shared_down,
    final_gain,
):
    bf16, f32 = jnp.bfloat16, jnp.float32
    dma = pltpu.SemaphoreType.DMA
    vmem = pl.BlockSpec(memory_space=pltpu.VMEM)
    hbm = pl.BlockSpec(memory_space=pl.ANY)
    block = (CAP, HALF)
    w_gate, w_up, w_down = expert_gate[0], expert_up[0], expert_down[0]
    args = (
        (linear_part, hbm), (gate_part, hbm), (kernel_taps, vmem), (channel_gain.reshape(16, 1, 128), vmem),
        (output_weight, hbm), (residual, hbm), (mix_gain[None, :], vmem), (documents.reshape(16, 128), vmem),
        (expert_ids.T, vmem), (route_weights.T, vmem), (final_gain[None, :], vmem),
        (w_gate, hbm), (w_up, hbm), (w_down, hbm), (shared_gate, hbm), (shared_up, hbm), (shared_down, hbm),
    )
    return pl.pallas_call(
        layer_kernel,
        out_shape=jax.ShapeDtypeStruct(residual.shape, f32),
        in_specs=[spec for _, spec in args],
        out_specs=vmem,
        scratch_shapes=[
            pltpu.VMEM((2048, 128), bf16),
            pltpu.VMEM((2048, 128), bf16),
            pltpu.VMEM((ROWS, 2048), bf16),
            pltpu.VMEM((DEPTH, 128, 2048), bf16),
            pltpu.VMEM((2048 + HALO, 128), f32),
            pltpu.VMEM((HALO, 128), bf16),
            pltpu.VMEM((8, 128), f32),
            pltpu.VMEM((HALO, 128), bf16),
            pltpu.VMEM((8, 128), f32),
            pltpu.VMEM((32, 128), f32),
            pltpu.VMEM((2048, 128), bf16),
            pltpu.VMEM((256, HALF), bf16),
            pltpu.VMEM((256, HALF), bf16),
            pltpu.VMEM((2, 256, 128), f32),
            pltpu.VMEM((2, 256, 128), f32),
            pltpu.VMEM((4, 2, ROWS, 512), f32),
            pltpu.VMEM((4, ROWS, 512), f32),
            pltpu.VMEM((ROWS, 2048), bf16),
            pltpu.VMEM((32, 1, 128), f32),
            pltpu.VMEM(w_gate.shape, bf16),
            pltpu.VMEM(w_up.shape, bf16),
            pltpu.VMEM(w_down.shape, bf16),
            pltpu.VMEM(shared_gate.shape, bf16),
            pltpu.VMEM(shared_up.shape, bf16),
            pltpu.VMEM(shared_down.shape, bf16),
            pltpu.VMEM((2, 4, ROWS, HALF), bf16),
            pltpu.VMEM((2, 4, 32, 1, 128), f32),
            pltpu.VMEM((2, 3, 4) + block, bf16),
            pltpu.VMEM((2, 4) + block, bf16),
            pltpu.VMEM((2, 4, 4) + block, bf16),
            pltpu.VMEM((4, 4, CAP, 512), f32),
            pltpu.VMEM((4, 4, CAP, 512), f32),
            pltpu.VMEM((4, 4, CAP, 512), bf16),
            pltpu.VMEM((2, 3, 4) + block, bf16),
            pltpu.VMEM((2, 4) + block, bf16),
            pltpu.VMEM((2, 4, 4) + block, bf16),
            pltpu.VMEM((2, 3, ROWS, HALF), bf16),
            pltpu.VMEM((2, 2) + block, bf16),
            pltpu.VMEM((2, 2, ROWS, HALF), bf16),
            pltpu.VMEM((ROWS, 2048), f32),
            pltpu.VMEM((ROWS, 2048), f32),
            dma((4,)), dma((8,)), dma((8,)), dma((2,)), dma((2,)), dma((8,)), dma((8,)),
            dma((2, 4)), dma((2, 4)), dma((1,)), dma((1,)), dma((2, 4, 4)), dma((2, 4, 4)),
            dma, dma, dma((4,)), dma((4,)),
            dma((6,)),
            dma((2, 4)), dma((2, 4)), dma((2, 3)), dma((2, 3)),
            dma((2, 2, 4)), dma((2, 2, 4)), dma((2, 4)), dma((2, 4)), dma((2, 4)), dma((2, 4)),
            dma((2, 2, 4)), dma((2, 2, 4)), dma((2, 4)), dma((2, 4)), dma((2, 4)), dma((2, 4)),
            dma((2, 4)), dma((2, 4)),
        ],
        compiler_params=pltpu.CompilerParams(
            collective_id=0, has_side_effects=True, vmem_limit_bytes=63 * 1024 * 1024
        ),
    )(*[a for a, _ in args]).astype(bf16)


def solution(mesh):
    both = P(("sp", "tp"), None)
    placed = (
        P("sp", "tp"), P("sp", "tp"), P(None, "tp"), P(), P("tp", None), both, P(), P("sp"), both, both,
        P("sp", None, None), P("sp", None, None), P("sp", None, None), P(), P(), P(), P(),
    )
    return jax.shard_map(shards, mesh=mesh, in_specs=placed, out_specs=both, check_vma=False)
```

```python
import jax
import jax.numpy as jnp
from jax import lax
from jax.experimental import pallas as pl
from jax.experimental.pallas import tpu as pltpu
from jax.sharding import PartitionSpec as P

EPSILON = 1e-05
RESIDUAL_SCALE = 8.0**0.25
MESH_ID = pl.DeviceIdType.MESH
HALF = 1024
SIDE = 4
DEPTH = 8
CAP = 64
ROWS = 128
HALO = 32
TAPS = 31
PLACE = {0: 0, 1: 1, 7: 2, 2: 3, 6: 4, 3: 5, 5: 6, 4: 7}
GROUP = ((1, 5), (5, 8))


def normalize(values):
    mean = jnp.mean(values, -1, keepdims=True)
    square = jnp.mean(values * values, -1, keepdims=True)
    return (values - mean) * lax.rsqrt(square - mean * mean + EPSILON)


def layer_kernel(
    linear_h, gate_h, taps, channel_gain, w_h, residual_h, mix_gain, docs, ids, ways, gain,
    w_gate, w_up, w_down, s_gate, s_up, s_down, out,
    linear, gate, residual, weight, gated, tail, tail_docs, halo, halo_docs, tap32, conv, conv_in, act,
    sums, sums_in, part, part_in2, normed, table,
    wg, wu, wd, sg, su, sd,
    near, meta, packed, relay, arrived, acc_g, acc_u, hidden, answers, relay_back, back, partial, relay_part, part_in,
    kept, shared,
    l_sem, z_s, z_r, h_s, h_r, a_s, a_r, g_s, g_r, f_s, f_r, e_s, e_r, st_s, st_r, x_s, x_r,
    w_sem, s1_s, s1_r, m_s, m_r, d_s, d_r, rl_s, rl_r, fw_s, fw_r,
    b_s, b_r, bl_s, bl_r, bf_s, bf_r, p_s, p_r,
):
    f32, bf16 = jnp.float32, jnp.bfloat16
    sp, tp = lax.axis_index("sp"), lax.axis_index("tp")
    y, x = sp // SIDE, sp % SIDE
    z, core = tp // 2, tp % 2
    other = 1 - core

    def at(dy, dx):
        return ((y + dy) % SIDE) * SIDE + (x + dx) % SIDE

    def first(o, k):
        return at(0, k) if o == 0 else at(k, 0)

    def second(o, k):
        return at(k, 0) if o == 0 else at(0, k)

    def along(dz):
        return ((z + dz) % DEPTH) * 2 + core

    def push(src, dst, ss, rs, to_sp, to_tp):
        copy = pltpu.make_async_remote_copy(
            src_ref=src, dst_ref=dst, send_sem=ss, recv_sem=rs,
            device_id=(to_sp, to_tp), device_id_type=MESH_ID,
        )
        copy.start()
        sent.append(copy)

    def send(src, dst, ss, rs, to):
        push(src, dst, ss, rs, to, tp)

    def landed(dst, ss, rs):
        pltpu.make_async_remote_copy(
            src_ref=dst, dst_ref=dst, send_sem=ss, recv_sem=rs,
            device_id=(first(0, 1), tp), device_id_type=MESH_ID,
        ).wait_recv()

    sent = []

    def drain(keep=0):
        while len(sent) > keep:
            sent.pop(0).wait_send()

    own_loads = [
        pltpu.make_async_copy(a, b, l_sem.at[i])
        for i, (a, b) in enumerate(
            [(w_h, weight.at[0]), (linear_h, linear), (gate_h, gate), (residual_h, residual)]
        )
    ]
    for load in own_loads:
        load.start()
    loads = [
        pltpu.make_async_copy(a, b, w_sem.at[i])
        for i, (a, b) in enumerate(
            [(s_gate, sg), (s_up, su), (s_down, sd), (w_gate, wg), (w_up, wu), (w_down, wd)]
        )
    ]

    after, ahead = (sp + 1) % 16, (sp + 15) % 16
    barrier = pltpu.get_barrier_semaphore()

    def greet(to_sp, to_tp):
        pl.semaphore_signal(barrier, inc=1, device_id=(to_sp, to_tp), device_id_type=MESH_ID)

    for dz in range(1, DEPTH):
        greet(sp, along(dz))
    for to in (at(0, 1), at(0, 3), at(1, 0), at(3, 0), after, ahead):
        greet(to, tp)
    greet(sp, z * 2 + other)
    pl.semaphore_wait(barrier, 14)

    def columns(o, k, width=1):
        fast, slow = (x, y) if o == 0 else (y, x)
        return pl.ds(pl.multiple_of((slow * SIDE + (fast + k) % SIDE) * 128, 128), 128)

    def side_columns(o, ks, kf):
        fast, slow = (x, y) if o == 0 else (y, x)
        block = ((slow + ks) % SIDE) * SIDE + (fast + kf) % SIDE
        return pl.ds(pl.multiple_of(block * 128, 128), 128)

    own_loads[0].wait()
    for dz in (7, 1, 6, 2, 5, 3, 4):
        there = PLACE[(DEPTH - dz) % DEPTH]
        o = 0 if there < GROUP[0][1] else 1
        cols = columns(o, 0)
        push(weight.at[0, :, cols], weight.at[there, :, cols], z_s.at[there], z_r.at[there], sp, along(dz))

    own_loads[1].wait()
    own_loads[2].wait()

    def gate_rows(a, b):
        a, b = a.astype(f32), b.astype(f32)
        return (a * (1.0 / (1.0 + jnp.exp(-b)))).astype(bf16)

    tail[...] = gate_rows(linear[2048 - HALO:, :], gate[2048 - HALO:, :])
    doc = docs[...]
    spot = lax.broadcasted_iota(jnp.int32, (16, 128), 0) * 128 + lax.broadcasted_iota(jnp.int32, (16, 128), 1)
    local, last = [], []
    for d in (1, 2, 3):
        below = jnp.where(doc < d, 1.0, 0.0)
        local.append(jnp.sum(jnp.sum(below, 1, keepdims=True), 0, keepdims=True))
        below = jnp.where(spot >= 2048 - (TAPS - 1), below, 0.0)
        last.append(jnp.sum(jnp.sum(below, 1, keepdims=True), 0, keepdims=True))
    for i in range(3):
        tail_docs[i:i + 1, :] = jnp.broadcast_to(last[i], (1, 128))
    tail_docs[3:8, :] = jnp.zeros((5, 128), f32)
    push(tail, halo, h_s.at[0], h_r.at[0], after, tp)
    push(tail_docs, halo_docs, h_s.at[1], h_r.at[1], after, tp)
    for load in loads:
        load.start()

    def gate_block(i, _):
        rows = pl.ds(pl.multiple_of(i * 128, 128), 128)
        there = pl.ds(pl.multiple_of(i * 128 + HALO, 32), 128)
        gated[there, :] = gate_rows(linear[rows, :], gate[rows, :]).astype(f32)
        return 0

    lax.fori_loop(0, 16, gate_block, 0)
    tap32[0:TAPS, :] = taps[...].astype(f32)

    def spread(o, k, rows, i):
        lo, hi = GROUP[o]
        mine = weight.at[lo:hi, rows, side_columns(o, 0, k)]
        send(mine, mine, e_s.at[o, k, i], e_r.at[o, k, i], second(o, 1 if i % 2 == 0 else 3))

    whole, upper, lower = slice(0, 128), slice(0, 64), slice(64, 128)

    def gather_start(o):
        lo, hi = GROUP[o]
        mine = weight.at[lo:hi, :, columns(o, 0)]
        for there in range(lo, hi):
            landed(weight.at[there, :, columns(o, 0)], z_s.at[there], z_r.at[there])
        send(mine, mine, g_s.at[o, 0], g_r.at[o, 0], first(o, 1))
        send(mine, mine, g_s.at[o, 1], g_r.at[o, 1], first(o, 3))
        spread(o, 0, whole, 0)
        spread(o, 0, whole, 1)

    def gather_near(o):
        lo, hi = GROUP[o]
        landed(weight.at[lo:hi, :, columns(o, 3)], g_s.at[o, 0], g_r.at[o, 0])
        half = weight.at[lo:hi, upper, columns(o, 3)]
        send(half, half, g_s.at[o, 2], g_r.at[o, 2], first(o, 1))
        spread(o, 3, whole, 0)
        spread(o, 3, whole, 1)
        landed(weight.at[lo:hi, :, columns(o, 1)], g_s.at[o, 1], g_r.at[o, 1])
        half = weight.at[lo:hi, lower, columns(o, 1)]
        send(half, half, g_s.at[o, 3], g_r.at[o, 3], first(o, 3))
        spread(o, 1, whole, 0)
        spread(o, 1, whole, 1)

    def gather_far(o):
        lo, hi = GROUP[o]
        landed(weight.at[lo:hi, upper, columns(o, 2)], g_s.at[o, 2], g_r.at[o, 2])
        landed(weight.at[lo:hi, lower, columns(o, 2)], g_s.at[o, 3], g_r.at[o, 3])
        spread(o, 2, whole, 0)
        spread(o, 2, whole, 1)

    def gather_pass(o):
        lo, hi = GROUP[o]
        for k in (0, 3, 1, 2):
            landed(weight.at[lo:hi, :, side_columns(o, 3, k)], e_s.at[o, k, 0], e_r.at[o, k, 0])
            half = weight.at[lo:hi, upper, side_columns(o, 3, k)]
            send(half, half, e_s.at[o, k, 2], e_r.at[o, k, 2], second(o, 1))
            landed(weight.at[lo:hi, :, side_columns(o, 1, k)], e_s.at[o, k, 1], e_r.at[o, k, 1])
            half = weight.at[lo:hi, lower, side_columns(o, 1, k)]
            send(half, half, e_s.at[o, k, 3], e_r.at[o, k, 3], second(o, 3))

    def gather_end(o):
        lo, hi = GROUP[o]
        for k in (0, 3, 1, 2):
            landed(weight.at[lo:hi, upper, side_columns(o, 2, k)], e_s.at[o, k, 2], e_r.at[o, k, 2])
            landed(weight.at[lo:hi, lower, side_columns(o, 2, k)], e_s.at[o, k, 3], e_r.at[o, k, 3])

    names = lax.broadcasted_iota(jnp.int32, (16, ROWS), 0)
    hit_0, hit_1 = names == ids[0:1, :], names == ids[1:2, :]
    hits = jnp.where(hit_0 | hit_1, 1.0, 0.0)
    before = lax.broadcasted_iota(jnp.int32, (ROWS, ROWS), 0) < lax.broadcasted_iota(jnp.int32, (ROWS, ROWS), 1)
    ranks = jnp.dot(hits.astype(bf16), jnp.where(before, 1.0, 0.0).astype(bf16), preferred_element_type=f32)
    slots = jnp.where(hits > 0.5, ranks, -1.0)
    values = jnp.where(hit_0, ways[0:1, :], 0.0) + jnp.where(hit_1, ways[1:2, :], 0.0)
    for e in range(16):
        table[e] = slots[e:e + 1, :]
        table[e + 16] = values[e:e + 1, :]

    gather_start(0)
    landed(halo, h_s.at[0], h_r.at[0])
    landed(halo_docs, h_s.at[1], h_r.at[1])
    inside = sp > 0
    gated[0:HALO, :] = jnp.where(inside, halo[...].astype(f32), 0.0)
    starts = []
    for i in range(3):
        extra = jnp.where(inside, halo_docs[i:i + 1, :], float(TAPS - 1)) - float(TAPS - 1)
        starts.append(local[i] + extra)

    CHUNK = 64

    def conv_block(dz):
        base = ((z + dz) % DEPTH) * 256

        def piece(i, _):
            row = pl.multiple_of(base + i * CHUNK, CHUNK)
            spot = lax.broadcasted_iota(jnp.int32, (CHUNK, 128), 0).astype(f32) + row.astype(f32)
            begun = jnp.full((CHUNK, 128), -1000.0, f32)
            for s in starts:
                begun = jnp.maximum(begun, jnp.where(s <= spot, s, -1000.0))
            age = spot - begun
            total = jnp.zeros((CHUNK, 128), f32)
            for j in range(TAPS):
                window = gated[pl.ds(row + (HALO - j), CHUNK), :]
                total = total + jnp.where(age >= float(j), window * tap32[j:j + 1, :], 0.0)
            conv[pl.ds(row, CHUNK), :] = total.astype(bf16)
            return 0

        lax.fori_loop(0, 256 // CHUNK, piece, 0)
        rows = pl.ds(pl.multiple_of(base, 256), 256)
        if dz == 0:
            conv_in[:, 0:128] = conv[rows, :]
        else:
            there = PLACE[(DEPTH - dz) % DEPTH]
            push(
                conv.at[rows, :], conv_in.at[:, there * 128:(there + 1) * 128],
                a_s.at[there], a_r.at[there], sp, along(dz),
            )

    for dz in (4, 3, 5):
        conv_block(dz)
    gather_near(0)
    for dz in (2, 6):
        conv_block(dz)
    gather_start(1)
    for dz in (1, 7):
        conv_block(dz)
    gather_far(0)
    conv_block(0)
    gather_near(1)
    gather_far(1)
    gather_pass(0)

    for there in range(1, DEPTH):
        landed(conv_in.at[:, there * 128:(there + 1) * 128], a_s.at[there], a_r.at[there])
    mean_part = jnp.zeros((256, 128), f32)
    square_part = jnp.zeros((256, 128), f32)
    for s in range(DEPTH):
        v = conv_in[:, s * 128:(s + 1) * 128].astype(f32)
        mean_part = mean_part + v
        square_part = square_part + v * v
    sums[0] = mean_part
    sums[1] = square_part
    push(sums, sums_in, st_s, st_r, sp, z * 2 + other)
    gather_pass(1)
    landed(sums_in, st_s, st_r)
    mean = jnp.sum(sums[0] + sums_in[0], 1, keepdims=True) * (1.0 / 2048.0)
    square = jnp.sum(sums[1] + sums_in[1], 1, keepdims=True) * (1.0 / 2048.0)
    scale = lax.rsqrt(square - mean * mean + EPSILON)
    for dz, s in PLACE.items():
        v = conv_in[:, s * 128:(s + 1) * 128].astype(f32)
        v = (v - mean) * scale * channel_gain[along(dz)]
        act[:, s * 128:(s + 1) * 128] = (v / (1.0 + jnp.exp(-v))).astype(bf16)

    gather_end(0)
    for n in range(4):
        w = weight[0:4, :, n * 512:(n + 1) * 512].reshape(512, 512)
        part[n] = jnp.dot(act[:, 0:512], w, preferred_element_type=f32).reshape(2, ROWS, 512)
    gather_end(1)
    for n in range(4):
        w = weight[4:8, :, n * 512:(n + 1) * 512].reshape(512, 512)
        got = jnp.dot(act[:, 512:1024], w, preferred_element_type=f32).reshape(2, ROWS, 512)
        part[n] = part[n] + got
        push(part.at[n, other], part_in2.at[n], x_s.at[n], x_r.at[n], sp, z * 2 + other)
    own_loads[3].wait()
    for n in range(4):
        cols = slice(n * 512, (n + 1) * 512)
        landed(part_in2.at[n], x_s.at[n], x_r.at[n])
        kept[:, cols] = RESIDUAL_SCALE * residual[:, cols].astype(f32) + part[n, core] + part_in2[n]
    normed[...] = (normalize(kept[...]) * mix_gain[...]).astype(bf16)

    before_rows = len(sent)
    for o in (0, 1):
        mine = normed.at[:, o * HALF:(o + 1) * HALF]
        send(table, meta.at[o, 3], m_s.at[o, 0], m_r.at[o, 0], first(o, 1))
        send(table, meta.at[o, 1], m_s.at[o, 1], m_r.at[o, 1], first(o, 3))
        send(mine, near.at[o, 3], s1_s.at[o, 0], s1_r.at[o, 0], first(o, 1))
        send(mine, near.at[o, 1], s1_s.at[o, 1], s1_r.at[o, 1], first(o, 3))

    lanes = lax.broadcasted_iota(jnp.int32, (CAP, 128), 0).astype(f32)

    def expert_at(o, k):
        return second(o, k)

    def slot_row(o, k, e):
        return table[e] if k == 0 else meta[o, k, e]

    def weight_row(o, k, e):
        return table[e + 16] if k == 0 else meta[o, k, e + 16]

    def pack(o, k):
        rows = normed[:, o * HALF:(o + 1) * HALF] if k == 0 else near[o, k]
        for q in (2, 1, 3, 0):
            hit = jnp.where(lanes == slot_row(o, k, expert_at(o, q)), 1.0, 0.0).astype(bf16)
            block = jnp.dot(hit, rows, preferred_element_type=f32).astype(bf16)
            if q == 0:
                arrived[o, 0, k] = block
            else:
                packed[o, q - 1, k] = block
            if q == 2:
                way = 1 if k < 2 else 3
                send(packed.at[o, 1, k], relay.at[o, k], rl_s.at[o, k], rl_r.at[o, k], second(o, way))
            if q == 1:
                send(packed.at[o, 0, k], arrived.at[o, 3, k], d_s.at[o, 0, k], d_r.at[o, 0, k], second(o, 1))
            if q == 3:
                send(packed.at[o, 2, k], arrived.at[o, 1, k], d_s.at[o, 1, k], d_r.at[o, 1, k], second(o, 3))

    def pass_on(o, k):
        landed(relay.at[o, k], rl_s.at[o, k], rl_r.at[o, k])
        way = 1 if k < 2 else 3
        send(relay.at[o, k], arrived.at[o, 2, k], fw_s.at[o, k], fw_r.at[o, k], second(o, way))

    for o in (0, 1):
        pack(o, 0)
    drain(len(sent) - before_rows)
    for o in (0, 1):
        landed(meta.at[o, 3], m_s.at[o, 0], m_r.at[o, 0])
        send(meta.at[o, 3], meta.at[o, 2], m_s.at[o, 2], m_r.at[o, 2], first(o, 1))
        landed(near.at[o, 3], s1_s.at[o, 0], s1_r.at[o, 0])
        send(near.at[o, 3, 0:64], near.at[o, 2, 0:64], s1_s.at[o, 2], s1_r.at[o, 2], first(o, 1))
    for o in (0, 1):
        landed(meta.at[o, 1], m_s.at[o, 1], m_r.at[o, 1])
        landed(near.at[o, 1], s1_s.at[o, 1], s1_r.at[o, 1])
        send(near.at[o, 1, 64:128], near.at[o, 2, 64:128], s1_s.at[o, 3], s1_r.at[o, 3], first(o, 3))
    for k in (3, 1):
        for o in (0, 1):
            pack(o, k)
    for o in (0, 1):
        pass_on(o, 0)
    for o in (0, 1):
        landed(meta.at[o, 2], m_s.at[o, 2], m_r.at[o, 2])
        landed(near.at[o, 2, 0:64], s1_s.at[o, 2], s1_r.at[o, 2])
        landed(near.at[o, 2, 64:128], s1_s.at[o, 3], s1_r.at[o, 3])
        pack(o, 2)

    acc_g[...] = jnp.zeros_like(acc_g)
    acc_u[...] = jnp.zeros_like(acc_u)
    for load in loads[:3]:
        load.wait()
    act = jnp.dot(normed[...], sg[...], preferred_element_type=f32)
    lin = jnp.dot(normed[...], su[...], preferred_element_type=f32)
    common = (act / (1.0 + jnp.exp(-act)) * lin).astype(bf16)
    shared[...] = jnp.dot(common, sd[...], preferred_element_type=f32)
    for k in (3, 1):
        for o in (0, 1):
            pass_on(o, k)
    for load in loads[3:]:
        load.wait()

    def product(o, k):
        landed(arrived.at[o, 3, k], d_s.at[o, 0, k], d_r.at[o, 0, k])
        landed(arrived.at[o, 1, k], d_s.at[o, 1, k], d_r.at[o, 1, k])
        landed(arrived.at[o, 2, k], fw_s.at[o, k], fw_r.at[o, k])
        rows = arrived[o, :, k].reshape(SIDE * CAP, HALF)
        for acc, w in ((acc_g, wg), (acc_u, wu)):
            got = jnp.dot(rows, w[o * HALF:(o + 1) * HALF, :], preferred_element_type=f32)
            got = got.reshape(SIDE, CAP, 512)
            if o == 0:
                acc[:, k] = acc[:, k] + got
            else:
                acc[k] = acc[k] + got

    for o in (0, 1):
        product(o, 0)
    for o in (0, 1):
        pass_on(o, 2)
    for k in (3, 1, 2):
        for o in (0, 1):
            product(o, k)

    before_answers = len(sent)
    def relayed(k):
        for o in (0, 1):
            way = 1 if k < 2 else 3
            send(answers.at[o, 1, k], relay_back.at[o, k], bl_s.at[o, k], bl_r.at[o, k], second(o, way))

    def direct(k):
        for o in (0, 1):
            for q, d in ((1, 0), (3, 1)):
                send(
                    answers.at[o, q - 1, k], back.at[o, k, SIDE - q], b_s.at[o, d, k], b_r.at[o, d, k],
                    second(o, q),
                )

    def pass_back(o, k):
        landed(relay_back.at[o, k], bl_s.at[o, k], bl_r.at[o, k])
        way = 1 if k < 2 else 3
        send(relay_back.at[o, k], back.at[o, k, 2], bf_s.at[o, k], bf_r.at[o, k], second(o, way))

    ready = set()

    def hide(dy, dx):
        if (dy, dx) not in ready:
            ready.add((dy, dx))
            g = acc_g[dy, dx]
            hidden[dy, dx] = (g / (1.0 + jnp.exp(-g)) * acc_u[dy, dx]).astype(bf16)

    def answer(k):
        for o in (0, 1):
            for q in range(SIDE):
                hide(*((q, k) if o == 0 else (k, q)))
            rows = (hidden[:, k] if o == 0 else hidden[k]).reshape(SIDE * CAP, 512)
            ans = jnp.dot(rows, wd[:, o * HALF:(o + 1) * HALF], preferred_element_type=f32).astype(bf16)
            back[o, k, 0] = ans[0:CAP]
            for q in (1, 2, 3):
                answers[o, q - 1, k] = ans[q * CAP:(q + 1) * CAP]

    answer(2)
    relayed(2)
    direct(2)
    answer(1)
    relayed(1)
    answer(3)
    relayed(3)
    answer(0)

    def choose(o, k, part):
        rows = []
        for j in range(SIDE):
            e = expert_at(o, j)
            w = weight_row(o, k, e)
            high = w.astype(bf16).astype(f32)
            value = high if part == 0 else w - high
            rows.append(jnp.where(lanes == slot_row(o, k, e), value, 0.0).astype(bf16))
        return jnp.concatenate(rows, 0)

    def combine(o, k):
        for j, d in ((3, 0), (1, 1)):
            landed(back.at[o, k, j], b_s.at[o, d, k], b_r.at[o, d, k])
        landed(back.at[o, k, 2], bf_s.at[o, k], bf_r.at[o, k])
        rows = back[o, k].reshape(SIDE * CAP, HALF)
        dims = (((0,), (0,)), ((), ()))
        total = lax.dot_general(choose(o, k, 0), rows, dims, preferred_element_type=f32)
        return total + lax.dot_general(choose(o, k, 1), rows, dims, preferred_element_type=f32)

    def pass_sum(o, k):
        total = combine(o, k)
        mine = partial.at[o, k - 1]
        if k == 2:
            partial[o, k - 1] = total.astype(bf16)
            send(mine.at[0:64], relay_part.at[o, 0], p_s.at[o, 2], p_r.at[o, 2], first(o, 1))
            send(mine.at[64:128], relay_part.at[o, 1], p_s.at[o, 3], p_r.at[o, 3], first(o, 3))
        elif k == 1:
            landed(relay_part.at[o, 0], p_s.at[o, 2], p_r.at[o, 2])
            partial[o, k - 1, 0:64] = (total[0:64] + relay_part[o, 0].astype(f32)).astype(bf16)
            partial[o, k - 1, 64:128] = total[64:128].astype(bf16)
            send(mine, part_in.at[o, 0], p_s.at[o, 0], p_r.at[o, 0], first(o, 1))
        else:
            landed(relay_part.at[o, 1], p_s.at[o, 3], p_r.at[o, 3])
            partial[o, k - 1, 0:64] = total[0:64].astype(bf16)
            partial[o, k - 1, 64:128] = (total[64:128] + relay_part[o, 1].astype(f32)).astype(bf16)
            send(mine, part_in.at[o, 1], p_s.at[o, 1], p_r.at[o, 1], first(o, 3))

    def both(step, k):
        for o in (0, 1):
            step(o, k)

    both(pass_back, 2)
    direct(1)
    both(pass_back, 1)
    direct(3)
    both(pass_back, 3)
    relayed(0)
    drain(len(sent) - before_answers)
    both(pass_sum, 2)
    direct(0)
    both(pass_back, 0)
    both(pass_sum, 1)
    both(pass_sum, 3)
    for o in (0, 1):
        kept[:, o * HALF:(o + 1) * HALF] = combine(o, 0)
    drain(4)
    for o in (0, 1):
        landed(part_in.at[o, 0], p_s.at[o, 0], p_r.at[o, 0])
        landed(part_in.at[o, 1], p_s.at[o, 1], p_r.at[o, 1])
        here = slice(o * HALF, (o + 1) * HALF)
        kept[:, here] = kept[:, here] + part_in[o, 0].astype(f32) + part_in[o, 1].astype(f32)
    values = RESIDUAL_SCALE * normed[...].astype(f32) + kept[...] + shared[...]
    out[...] = (normalize(values) * gain[...]).astype(bf16)
    drain()


def shards(
    linear_part, gate_part, kernel_taps, channel_gain, output_weight, residual, mix_gain, documents,
    expert_ids, route_weights, expert_gate, expert_up, expert_down, shared_gate, shared_up, shared_down,
    final_gain,
):
    bf16, f32 = jnp.bfloat16, jnp.float32
    dma = pltpu.SemaphoreType.DMA
    vmem = pl.BlockSpec(memory_space=pltpu.VMEM)
    hbm = pl.BlockSpec(memory_space=pltpu.MemorySpace.HBM)
    block = (CAP, HALF)
    w_gate, w_up, w_down = expert_gate[0], expert_up[0], expert_down[0]
    args = (
        (linear_part, hbm), (gate_part, hbm), (kernel_taps, vmem), (channel_gain.reshape(16, 1, 128), vmem),
        (output_weight, hbm), (residual, hbm), (mix_gain[None, :], vmem), (documents.reshape(16, 128), vmem),
        (expert_ids.T, vmem), (route_weights.T, vmem), (final_gain[None, :], vmem),
        (w_gate, hbm), (w_up, hbm), (w_down, hbm), (shared_gate, hbm), (shared_up, hbm), (shared_down, hbm),
    )
    return pl.pallas_call(
        layer_kernel,
        out_shape=jax.ShapeDtypeStruct(residual.shape, bf16),
        in_specs=[spec for _, spec in args],
        out_specs=vmem,
        scratch_shapes=[
            pltpu.VMEM((2048, 128), bf16),
            pltpu.VMEM((2048, 128), bf16),
            pltpu.VMEM((ROWS, 2048), bf16),
            pltpu.VMEM((DEPTH, 128, 2048), bf16),
            pltpu.VMEM((2048 + HALO, 128), f32),
            pltpu.VMEM((HALO, 128), bf16),
            pltpu.VMEM((8, 128), f32),
            pltpu.VMEM((HALO, 128), bf16),
            pltpu.VMEM((8, 128), f32),
            pltpu.VMEM((32, 128), f32),
            pltpu.VMEM((2048, 128), bf16),
            pltpu.VMEM((256, HALF), bf16),
            pltpu.VMEM((256, HALF), bf16),
            pltpu.VMEM((2, 256, 128), f32),
            pltpu.VMEM((2, 256, 128), f32),
            pltpu.VMEM((4, 2, ROWS, 512), f32),
            pltpu.VMEM((4, ROWS, 512), f32),
            pltpu.VMEM((ROWS, 2048), bf16),
            pltpu.VMEM((32, 1, 128), f32),
            pltpu.VMEM(w_gate.shape, bf16),
            pltpu.VMEM(w_up.shape, bf16),
            pltpu.VMEM(w_down.shape, bf16),
            pltpu.VMEM(shared_gate.shape, bf16),
            pltpu.VMEM(shared_up.shape, bf16),
            pltpu.VMEM(shared_down.shape, bf16),
            pltpu.VMEM((2, 4, ROWS, HALF), bf16),
            pltpu.VMEM((2, 4, 32, 1, 128), f32),
            pltpu.VMEM((2, 3, 4) + block, bf16),
            pltpu.VMEM((2, 4) + block, bf16),
            pltpu.VMEM((2, 4, 4) + block, bf16),
            pltpu.VMEM((4, 4, CAP, 512), f32),
            pltpu.VMEM((4, 4, CAP, 512), f32),
            pltpu.VMEM((4, 4, CAP, 512), bf16),
            pltpu.VMEM((2, 3, 4) + block, bf16),
            pltpu.VMEM((2, 4) + block, bf16),
            pltpu.VMEM((2, 4, 4) + block, bf16),
            pltpu.VMEM((2, 3, ROWS, HALF), bf16),
            pltpu.VMEM((2, 2) + block, bf16),
            pltpu.VMEM((2, 2, ROWS, HALF), bf16),
            pltpu.VMEM((ROWS, 2048), f32),
            pltpu.VMEM((ROWS, 2048), f32),
            dma((4,)), dma((8,)), dma((8,)), dma((2,)), dma((2,)), dma((8,)), dma((8,)),
            dma((2, 4)), dma((2, 4)), dma((1,)), dma((1,)), dma((2, 4, 4)), dma((2, 4, 4)),
            dma, dma, dma((4,)), dma((4,)),
            dma((6,)),
            dma((2, 4)), dma((2, 4)), dma((2, 3)), dma((2, 3)),
            dma((2, 2, 4)), dma((2, 2, 4)), dma((2, 4)), dma((2, 4)), dma((2, 4)), dma((2, 4)),
            dma((2, 2, 4)), dma((2, 2, 4)), dma((2, 4)), dma((2, 4)), dma((2, 4)), dma((2, 4)),
            dma((2, 4)), dma((2, 4)),
        ],
        compiler_params=pltpu.CompilerParams(
            collective_id=0, has_side_effects=True, vmem_limit_bytes=54 * 1024 * 1024
        ),
    )(*[a for a, _ in args])


def solution(mesh):
    both = P(("sp", "tp"), None)
    placed = (
        P("sp", "tp"), P("sp", "tp"), P(None, "tp"), P(), P("tp", None), both, P(), P("sp"), both, both,
        P("sp", None, None), P("sp", None, None), P("sp", None, None), P(), P(), P(), P(),
    )
    return jax.shard_map(shards, mesh=mesh, in_specs=placed, out_specs=both, check_vma=False)
```

```python
import jax
import jax.numpy as jnp
from jax import lax
from jax.experimental import pallas as pl
from jax.experimental.pallas import tpu as pltpu
from jax.sharding import PartitionSpec as P

EPSILON = 1e-05
RESIDUAL_SCALE = 8.0**0.25
MESH_ID = pl.DeviceIdType.MESH
HALF = 1024
SIDE = 4
DEPTH = 8
CAP = 64
ROWS = 128
HALO = 32
TAPS = 31
PLACE = {1: 0, 7: 1, 2: 2, 6: 3, 3: 4, 5: 5, 4: 6, 0: 7}
GROUP = ((0, 2), (2, 4), (4, 7))


def normalize(values):
    mean = jnp.mean(values, -1, keepdims=True)
    square = jnp.mean(values * values, -1, keepdims=True)
    return (values - mean) * lax.rsqrt(square - mean * mean + EPSILON)


def layer_kernel(
    linear_h, gate_h, taps_h, channel_gain_h, w_h, residual_h, mix_gain_h, docs_h, ids_h, ways_h, gain_h,
    w_gate, w_up, w_down, s_gate, s_up, s_down, out,
    taps, channel_gain, mix_gain, docs, ids, ways, gain,
    linear, gate, residual, weight, gated, tail, tail_docs, halo, halo_docs, tap32, conv, conv_in, act,
    sums, sums_in, part, part_in2, normed, table,
    wg, wu, wd, sg, su, sd,
    near, meta, packed, relay, arrived, acc_g, acc_u, hidden, answers, relay_back, back, partial, relay_part,
    part_in, kept, shared,
    l_sem, w_sem, z_r, h_r, a_r, g_r, e_r, end_r, st_r, x_r, s1_r, m_r, d_r, rl_r, b_r, bl_r, p_r,
    z_s, h_s, a_s, g_s, e_s, st_s, x_s, s1_s, m_s, d_s, rl_s, fw_s, b_s, bl_s, bf_s, p_s,
):
    f32, bf16 = jnp.float32, jnp.bfloat16
    sp, tp = lax.axis_index("sp"), lax.axis_index("tp")
    y, x = sp // SIDE, sp % SIDE
    z, core = tp // 2, tp % 2
    other = 1 - core

    def at(dy, dx):
        return ((y + dy) % SIDE) * SIDE + (x + dx) % SIDE

    def first(o, k):
        return at(0, k) if o == 0 else at(k, 0)

    def second(o, k):
        return at(k, 0) if o == 0 else at(0, k)

    def along(dz):
        return ((z + dz) % DEPTH) * 2 + core

    def push(src, dst, ss, rs, to_sp, to_tp):
        pltpu.make_async_remote_copy(
            src_ref=src, dst_ref=dst, send_sem=ss, recv_sem=rs,
            device_id=(to_sp, to_tp), device_id_type=MESH_ID,
        ).start()

    def send(src, dst, ss, rs, to):
        push(src, dst, ss, rs, to, tp)

    def landed(dst, rs):
        pltpu.make_async_remote_copy(
            src_ref=dst, dst_ref=dst, send_sem=rs, recv_sem=rs,
            device_id=(first(0, 1), tp), device_id_type=MESH_ID,
        ).wait_recv()

    def gone(src, ss):
        pltpu.make_async_remote_copy(
            src_ref=src, dst_ref=src, send_sem=ss, recv_sem=ss,
            device_id=(first(0, 1), tp), device_id_type=MESH_ID,
        ).wait_send()

    own_loads = [
        pltpu.make_async_copy(a, b, l_sem.at[i])
        for i, (a, b) in enumerate(
            [
                (w_h, weight.at[7]), (linear_h, linear), (gate_h, gate), (docs_h, docs), (ids_h, ids),
                (ways_h, ways), (taps_h, taps), (channel_gain_h, channel_gain), (mix_gain_h, mix_gain),
                (gain_h, gain), (residual_h, residual),
            ]
        )
    ]
    for load in own_loads:
        load.start()
    loads = [
        pltpu.make_async_copy(a, b, w_sem.at[i])
        for i, (a, b) in enumerate(
            [(s_gate, sg), (s_up, su), (s_down, sd), (w_gate, wg), (w_up, wu), (w_down, wd)]
        )
    ]

    after, ahead = (sp + 1) % 16, (sp + 15) % 16
    barrier = pltpu.get_barrier_semaphore()

    def greet(to_sp, to_tp):
        pl.semaphore_signal(barrier, inc=1, device_id=(to_sp, to_tp), device_id_type=MESH_ID)

    for dz in (1, 7):
        greet(sp, along(dz))
    for to in (at(0, 1), at(0, 3), at(1, 0), at(3, 0), after, ahead):
        greet(to, tp)
    greet(sp, z * 2 + other)
    pl.semaphore_wait(barrier, 9)

    def columns(o, k, ks=0):
        fast, slow = (x, y) if o == 0 else (y, x)
        block = ((slow + ks) % SIDE) * SIDE + (fast + k) % SIDE
        return pl.ds(pl.multiple_of(block * 128, 128), 128)

    def strip(o):
        return slice(o * 64, o * 64 + 64)

    def upper(o):
        return slice(o * 64, o * 64 + 32)

    def lower(o):
        return slice(o * 64 + 32, o * 64 + 64)

    def hop(here, there, dz):
        for o in (0, 1):
            push(
                weight.at[here, strip(o), columns(o, 0)], weight.at[there, strip(o), columns(o, 0)],
                z_s, z_r.at[there], sp, along(dz),
            )

    def hopped(there):
        landed(weight.at[there, :, 0:128], z_r.at[there])

    own_loads[0].wait()
    hop(7, PLACE[7], 1)
    hop(7, PLACE[1], 7)

    for load in own_loads[1:4]:
        load.wait()

    def gate_rows(a, b):
        a, b = a.astype(f32), b.astype(f32)
        return (a * (1.0 / (1.0 + jnp.exp(-b)))).astype(bf16)

    tail[...] = gate_rows(linear[2048 - HALO:, :], gate[2048 - HALO:, :])
    doc = docs[...]
    spot = lax.broadcasted_iota(jnp.int32, (16, 128), 0) * 128 + lax.broadcasted_iota(jnp.int32, (16, 128), 1)
    local, last = [], []
    for d in (1, 2, 3):
        below = jnp.where(doc < d, 1.0, 0.0)
        local.append(jnp.sum(jnp.sum(below, 1, keepdims=True), 0, keepdims=True))
        below = jnp.where(spot >= 2048 - (TAPS - 1), below, 0.0)
        last.append(jnp.sum(jnp.sum(below, 1, keepdims=True), 0, keepdims=True))
    for i in range(3):
        tail_docs[i:i + 1, :] = jnp.broadcast_to(last[i], (1, 128))
    tail_docs[3:8, :] = jnp.zeros((5, 128), f32)
    push(tail, halo, h_s.at[0], h_r.at[0], after, tp)
    push(tail_docs, halo_docs, h_s.at[1], h_r.at[1], after, tp)
    for load in loads:
        load.start()

    def gate_block(i, _):
        rows = pl.ds(pl.multiple_of(i * 128, 128), 128)
        there = pl.ds(pl.multiple_of(i * 128 + HALO, 32), 128)
        gated[there, :] = gate_rows(linear[rows, :], gate[rows, :]).astype(f32)
        return 0

    lax.fori_loop(0, 16, gate_block, 0)
    for load in own_loads[4:10]:
        load.wait()
    tap32[0:TAPS, :] = taps[...].astype(f32)

    def spread(o, g, k):
        lo, hi = GROUP[g]
        mine = weight.at[lo:hi, strip(o), columns(o, k)]
        late = 1 if k == 2 else 0
        send(mine, mine, e_s, e_r.at[o, g, late, 0], second(o, 1))
        send(mine, mine, e_s, e_r.at[o, g, late, 1], second(o, 3))

    def gather_start(g):
        lo, hi = GROUP[g]
        for o in (0, 1):
            mine = weight.at[lo:hi, strip(o), columns(o, 0)]
            send(mine, mine, g_s, g_r.at[o, g, 0], first(o, 1))
            send(mine, mine, g_s, g_r.at[o, g, 1], first(o, 3))
        for o in (0, 1):
            spread(o, g, 0)

    def gather_near(g):
        lo, hi = GROUP[g]
        for o in (0, 1):
            landed(weight.at[lo:hi, strip(o), columns(o, 3)], g_r.at[o, g, 0])
            half = weight.at[lo:hi, upper(o), columns(o, 3)]
            send(half, half, g_s, g_r.at[o, g, 2], first(o, 1))
            landed(weight.at[lo:hi, strip(o), columns(o, 1)], g_r.at[o, g, 1])
            half = weight.at[lo:hi, lower(o), columns(o, 1)]
            send(half, half, g_s, g_r.at[o, g, 2], first(o, 3))
        for o in (0, 1):
            spread(o, g, 3)
            spread(o, g, 1)

    def gather_far(g):
        lo, hi = GROUP[g]
        for o in (0, 1):
            landed(weight.at[lo:hi, strip(o), columns(o, 2)], g_r.at[o, g, 2])
            spread(o, g, 2)

    def gather_pass(g, ks):
        lo, hi = GROUP[g]
        late = 1 if ks == (2,) else 0
        for o in (0, 1):
            landed(weight.at[lo:hi, strip(o), 0:128 * len(ks)], e_r.at[o, g, late, 0])
            for k in ks:
                half = weight.at[lo:hi, upper(o), columns(o, k, 3)]
                send(half, half, e_s, end_r.at[o, g], second(o, 1))
            landed(weight.at[lo:hi, strip(o), 0:128 * len(ks)], e_r.at[o, g, late, 1])
            for k in ks:
                half = weight.at[lo:hi, lower(o), columns(o, k, 1)]
                send(half, half, e_s, end_r.at[o, g], second(o, 3))

    def gather_end(g):
        lo, hi = GROUP[g]
        for o in (0, 1):
            landed(weight.at[lo:hi, strip(o), 0:512], end_r.at[o, g])

    SOON = (0, 3, 1)

    names = lax.broadcasted_iota(jnp.int32, (16, ROWS), 0)
    hit_0, hit_1 = names == ids[0:1, :], names == ids[1:2, :]
    hits = jnp.where(hit_0 | hit_1, 1.0, 0.0)
    before = lax.broadcasted_iota(jnp.int32, (ROWS, ROWS), 0) < lax.broadcasted_iota(jnp.int32, (ROWS, ROWS), 1)
    ranks = jnp.dot(hits.astype(bf16), jnp.where(before, 1.0, 0.0).astype(bf16), preferred_element_type=f32)
    slots = jnp.where(hits > 0.5, ranks, -1.0)
    values = jnp.where(hit_0, ways[0:1, :], 0.0) + jnp.where(hit_1, ways[1:2, :], 0.0)
    for e in range(16):
        table[e] = slots[e:e + 1, :]
        table[e + 16] = values[e:e + 1, :]

    hopped(PLACE[7])
    hop(PLACE[7], PLACE[6], 1)
    hopped(PLACE[1])
    hop(PLACE[1], PLACE[2], 7)
    gather_start(0)
    landed(halo, h_r.at[0])
    landed(halo_docs, h_r.at[1])
    inside = sp > 0
    gated[0:HALO, :] = jnp.where(inside, halo[...].astype(f32), 0.0)
    starts = []
    for i in range(3):
        extra = jnp.where(inside, halo_docs[i:i + 1, :], float(TAPS - 1)) - float(TAPS - 1)
        starts.append(local[i] + extra)

    CHUNK = 64

    def conv_block(dz):
        base = ((z + dz) % DEPTH) * 256

        def piece(i, _):
            row = pl.multiple_of(base + i * CHUNK, CHUNK)
            spot = lax.broadcasted_iota(jnp.int32, (CHUNK, 128), 0).astype(f32) + row.astype(f32)
            begun = jnp.full((CHUNK, 128), -1000.0, f32)
            for s in starts:
                begun = jnp.maximum(begun, jnp.where(s <= spot, s, -1000.0))
            age = spot - begun
            total = jnp.zeros((CHUNK, 128), f32)
            for j in range(TAPS):
                window = gated[pl.ds(row + (HALO - j), CHUNK), :]
                total = total + jnp.where(age >= float(j), window * tap32[j:j + 1, :], 0.0)
            conv[pl.ds(row, CHUNK), :] = total.astype(bf16)
            return 0

        lax.fori_loop(0, 256 // CHUNK, piece, 0)
        rows = pl.ds(pl.multiple_of(base, 256), 256)
        if dz == 0:
            conv_in[:, 7 * 128:] = conv[rows, :]
        else:
            there = PLACE[(DEPTH - dz) % DEPTH]
            push(
                conv.at[rows, :], conv_in.at[:, there * 128:(there + 1) * 128],
                a_s, a_r, sp, along(dz),
            )

    conv_block(1)
    conv_block(7)
    hopped(PLACE[6])
    hop(PLACE[6], PLACE[5], 1)
    hopped(PLACE[2])
    hop(PLACE[2], PLACE[3], 7)
    gather_start(1)
    conv_block(2)
    gather_near(0)
    conv_block(6)
    hopped(PLACE[5])
    hop(PLACE[5], PLACE[4], 1)
    hopped(PLACE[3])
    conv_block(3)
    conv_block(5)
    gather_far(0)
    gather_near(1)
    hopped(PLACE[4])
    gather_start(2)
    conv_block(4)
    conv_block(0)
    gather_far(1)
    gather_pass(0, SOON)
    gather_near(2)
    gather_pass(0, (2,))
    gather_far(2)
    gather_pass(1, SOON)
    gather_pass(1, (2,))

    landed(conv_in.at[:, 0:7 * 128], a_r)
    mean_part = jnp.zeros((256, 128), f32)
    square_part = jnp.zeros((256, 128), f32)
    for s in range(DEPTH):
        v = conv_in[:, s * 128:(s + 1) * 128].astype(f32)
        mean_part = mean_part + v
        square_part = square_part + v * v
    sums[0] = mean_part
    sums[1] = square_part
    push(sums, sums_in, st_s, st_r, sp, z * 2 + other)
    gather_pass(2, SOON)
    gather_pass(2, (2,))
    landed(sums_in, st_r)
    mean = jnp.sum(sums[0] + sums_in[0], 1, keepdims=True) * (1.0 / 2048.0)
    square = jnp.sum(sums[1] + sums_in[1], 1, keepdims=True) * (1.0 / 2048.0)
    scale = lax.rsqrt(square - mean * mean + EPSILON)
    for dz, s in PLACE.items():
        v = conv_in[:, s * 128:(s + 1) * 128].astype(f32)
        v = (v - mean) * scale * channel_gain[along(dz)]
        act[:, s * 128:(s + 1) * 128] = (v / (1.0 + jnp.exp(-v))).astype(bf16)

    for g, (lo, hi) in enumerate(((0, 2), (2, 4), (4, 8))):
        gather_end(g)
        for n in range(4):
            w = weight[lo:hi, :, n * 512:(n + 1) * 512].reshape((hi - lo) * 128, 512)
            got = jnp.dot(act[:, lo * 128:hi * 128], w, preferred_element_type=f32).reshape(2, ROWS, 512)
            part[n] = got if g == 0 else part[n] + got
            if g == 2:
                push(part.at[n, other], part_in2.at[n], x_s, x_r.at[n], sp, z * 2 + other)
    own_loads[10].wait()
    for n in range(4):
        cols = slice(n * 512, (n + 1) * 512)
        landed(part_in2.at[n], x_r.at[n])
        kept[:, cols] = RESIDUAL_SCALE * residual[:, cols].astype(f32) + part[n, core] + part_in2[n]
    normed[...] = (normalize(kept[...]) * mix_gain[...]).astype(bf16)

    for o in (0, 1):
        mine = normed.at[:, o * HALF:(o + 1) * HALF]
        send(table, meta.at[o, 3], m_s, m_r.at[o, 0], first(o, 1))
        send(table, meta.at[o, 1], m_s, m_r.at[o, 1], first(o, 3))
        send(mine, near.at[o, 3], s1_s, s1_r.at[o, 0], first(o, 1))
        send(mine, near.at[o, 1], s1_s, s1_r.at[o, 1], first(o, 3))

    lanes = lax.broadcasted_iota(jnp.int32, (CAP, 128), 0).astype(f32)

    def expert_at(o, k):
        return second(o, k)

    def slot_row(o, k, e):
        return table[e] if k == 0 else meta[o, k, e]

    def weight_row(o, k, e):
        return table[e + 16] if k == 0 else meta[o, k, e + 16]

    def pack(o, k):
        rows = normed[:, o * HALF:(o + 1) * HALF] if k == 0 else near[o, k]
        for q in (2, 1, 3, 0):
            hit = jnp.where(lanes == slot_row(o, k, expert_at(o, q)), 1.0, 0.0).astype(bf16)
            block = jnp.dot(hit, rows, preferred_element_type=f32).astype(bf16)
            if q == 0:
                arrived[o, 0, k] = block
            else:
                packed[o, q - 1, k] = block
            if q == 2:
                way = 1 if k < 2 else 3
                send(packed.at[o, 1, k], relay.at[o, k], rl_s, rl_r.at[o, k], second(o, way))
            if q == 1:
                send(packed.at[o, 0, k], arrived.at[o, 3, k], d_s, d_r.at[o, k], second(o, 1))
            if q == 3:
                send(packed.at[o, 2, k], arrived.at[o, 1, k], d_s, d_r.at[o, k], second(o, 3))

    def pass_on(o, k):
        landed(relay.at[o, k], rl_r.at[o, k])
        way = 1 if k < 2 else 3
        send(relay.at[o, k], arrived.at[o, 2, k], fw_s, d_r.at[o, k], second(o, way))

    for o in (0, 1):
        pack(o, 0)
    gone(weight.at[0:7, :, 0:128], z_s)
    gone(tail, h_s.at[0])
    gone(tail_docs, h_s.at[1])
    gone(conv_in.at[:, 0:7 * 128], a_s)
    gone(weight.at[0:7, :, 0:384], g_s)
    gone(weight.at[0:7, :, 0:1536], e_s)
    gone(sums, st_s)
    gone(part_in2, x_s)
    for o in (0, 1):
        landed(meta.at[o, 3], m_r.at[o, 0])
        send(meta.at[o, 3], meta.at[o, 2], m_s, m_r.at[o, 2], first(o, 1))
        landed(near.at[o, 3], s1_r.at[o, 0])
        send(near.at[o, 3, 0:64], near.at[o, 2, 0:64], s1_s, s1_r.at[o, 2], first(o, 1))
    for o in (0, 1):
        landed(meta.at[o, 1], m_r.at[o, 1])
        landed(near.at[o, 1], s1_r.at[o, 1])
        send(near.at[o, 1, 64:128], near.at[o, 2, 64:128], s1_s, s1_r.at[o, 2], first(o, 3))
    for k in (3, 1):
        for o in (0, 1):
            pack(o, k)
    for o in (0, 1):
        pass_on(o, 0)
    for o in (0, 1):
        landed(meta.at[o, 2], m_r.at[o, 2])
        landed(near.at[o, 2], s1_r.at[o, 2])
        pack(o, 2)

    acc_g[...] = jnp.zeros_like(acc_g)
    acc_u[...] = jnp.zeros_like(acc_u)
    for load in loads[:3]:
        load.wait()
    act = jnp.dot(normed[...], sg[...], preferred_element_type=f32)
    lin = jnp.dot(normed[...], su[...], preferred_element_type=f32)
    common = (act / (1.0 + jnp.exp(-act)) * lin).astype(bf16)
    shared[...] = jnp.dot(common, sd[...], preferred_element_type=f32)
    for k in (3, 1):
        for o in (0, 1):
            pass_on(o, k)
    for load in loads[3:]:
        load.wait()

    def product(o, k):
        landed(arrived.at[o, 1:4, k], d_r.at[o, k])
        rows = arrived[o, :, k].reshape(SIDE * CAP, HALF)
        for acc, w in ((acc_g, wg), (acc_u, wu)):
            got = jnp.dot(rows, w[o * HALF:(o + 1) * HALF, :], preferred_element_type=f32)
            got = got.reshape(SIDE, CAP, 512)
            if o == 0:
                acc[:, k] = acc[:, k] + got
            else:
                acc[k] = acc[k] + got

    for o in (0, 1):
        product(o, 0)
    for o in (0, 1):
        pass_on(o, 2)
    for k in (3, 1, 2):
        for o in (0, 1):
            product(o, k)

    def relayed(k):
        for o in (0, 1):
            way = 1 if k < 2 else 3
            send(answers.at[o, 1, k], relay_back.at[o, k], bl_s, bl_r.at[o, k], second(o, way))

    def direct(k):
        for o in (0, 1):
            for q in (1, 3):
                send(answers.at[o, q - 1, k], back.at[o, k, SIDE - q], b_s, b_r.at[o, k], second(o, q))

    def pass_back(o, k):
        landed(relay_back.at[o, k], bl_r.at[o, k])
        way = 1 if k < 2 else 3
        send(relay_back.at[o, k], back.at[o, k, 2], bf_s, b_r.at[o, k], second(o, way))

    ready = set()

    def hide(dy, dx):
        if (dy, dx) not in ready:
            ready.add((dy, dx))
            g = acc_g[dy, dx]
            hidden[dy, dx] = (g / (1.0 + jnp.exp(-g)) * acc_u[dy, dx]).astype(bf16)

    def answer(k):
        for o in (0, 1):
            for q in range(SIDE):
                hide(*((q, k) if o == 0 else (k, q)))
            rows = (hidden[:, k] if o == 0 else hidden[k]).reshape(SIDE * CAP, 512)
            ans = jnp.dot(rows, wd[:, o * HALF:(o + 1) * HALF], preferred_element_type=f32).astype(bf16)
            back[o, k, 0] = ans[0:CAP]
            for q in (1, 2, 3):
                answers[o, q - 1, k] = ans[q * CAP:(q + 1) * CAP]

    answer(2)
    relayed(2)
    direct(2)
    answer(1)
    relayed(1)
    answer(3)
    relayed(3)
    answer(0)

    def choose(o, k, part):
        rows = []
        for j in range(SIDE):
            e = expert_at(o, j)
            w = weight_row(o, k, e)
            high = w.astype(bf16).astype(f32)
            value = high if part == 0 else w - high
            rows.append(jnp.where(lanes == slot_row(o, k, e), value, 0.0).astype(bf16))
        return jnp.concatenate(rows, 0)

    def combine(o, k):
        landed(back.at[o, k, 1:4], b_r.at[o, k])
        rows = back[o, k].reshape(SIDE * CAP, HALF)
        dims = (((0,), (0,)), ((), ()))
        total = lax.dot_general(choose(o, k, 0), rows, dims, preferred_element_type=f32)
        return total + lax.dot_general(choose(o, k, 1), rows, dims, preferred_element_type=f32)

    def pass_sum(o, k):
        total = combine(o, k)
        mine = partial.at[o, k - 1]
        if k == 2:
            partial[o, k - 1] = total.astype(bf16)
            send(mine.at[0:64], relay_part.at[o, 0], p_s, p_r.at[o, 0], first(o, 1))
            send(mine.at[64:128], relay_part.at[o, 1], p_s, p_r.at[o, 1], first(o, 3))
        elif k == 1:
            landed(relay_part.at[o, 0], p_r.at[o, 0])
            partial[o, k - 1, 0:64] = (total[0:64] + relay_part[o, 0].astype(f32)).astype(bf16)
            partial[o, k - 1, 64:128] = total[64:128].astype(bf16)
            send(mine, part_in.at[o, 0], p_s, p_r.at[o, 2], first(o, 1))
        else:
            landed(relay_part.at[o, 1], p_r.at[o, 1])
            partial[o, k - 1, 0:64] = total[0:64].astype(bf16)
            partial[o, k - 1, 64:128] = (total[64:128] + relay_part[o, 1].astype(f32)).astype(bf16)
            send(mine, part_in.at[o, 1], p_s, p_r.at[o, 2], first(o, 3))

    def both(step, k):
        for o in (0, 1):
            step(o, k)

    both(pass_back, 2)
    direct(1)
    both(pass_back, 1)
    direct(3)
    both(pass_back, 3)
    relayed(0)
    gone(meta.at[:, 0:3], m_s)
    gone(near.at[:, 0:3], s1_s)
    gone(arrived.at[0], d_s)
    gone(relay, rl_s)
    gone(relay, fw_s)
    both(pass_sum, 2)
    direct(0)
    both(pass_back, 0)
    both(pass_sum, 1)
    both(pass_sum, 3)
    for o in (0, 1):
        kept[:, o * HALF:(o + 1) * HALF] = combine(o, 0)
    gone(back.at[0], b_s)
    gone(relay_back, bl_s)
    gone(relay_back, bf_s)
    for o in (0, 1):
        landed(part_in.at[o], p_r.at[o, 2])
        here = slice(o * HALF, (o + 1) * HALF)
        kept[:, here] = kept[:, here] + part_in[o, 0].astype(f32) + part_in[o, 1].astype(f32)
    values = RESIDUAL_SCALE * normed[...].astype(f32) + kept[...] + shared[...]
    out[...] = (normalize(values) * gain[...]).astype(bf16)
    gone(near.at[:, 0:3], p_s)


def shards(
    linear_part, gate_part, kernel_taps, channel_gain, output_weight, residual, mix_gain, documents,
    expert_ids, route_weights, expert_gate, expert_up, expert_down, shared_gate, shared_up, shared_down,
    final_gain,
):
    bf16, f32 = jnp.bfloat16, jnp.float32
    dma = pltpu.SemaphoreType.DMA
    vmem = pl.BlockSpec(memory_space=pltpu.VMEM)
    hbm = pl.BlockSpec(memory_space=pltpu.MemorySpace.HBM)
    block = (CAP, HALF)
    w_gate, w_up, w_down = expert_gate[0], expert_up[0], expert_down[0]
    args = (
        (linear_part, hbm), (gate_part, hbm), (kernel_taps, hbm), (channel_gain.reshape(16, 1, 128), hbm),
        (output_weight, hbm), (residual, hbm), (mix_gain[None, :], hbm), (documents.reshape(16, 128), hbm),
        (expert_ids.T, hbm), (route_weights.T, hbm), (final_gain[None, :], hbm),
        (w_gate, hbm), (w_up, hbm), (w_down, hbm), (shared_gate, hbm), (shared_up, hbm), (shared_down, hbm),
    )
    return pl.pallas_call(
        layer_kernel,
        out_shape=jax.ShapeDtypeStruct(residual.shape, bf16),
        in_specs=[spec for _, spec in args],
        out_specs=vmem,
        scratch_shapes=[
            pltpu.VMEM((TAPS, 128), bf16),
            pltpu.VMEM((16, 1, 128), f32),
            pltpu.VMEM((1, 2048), f32),
            pltpu.VMEM((16, 128), jnp.int32),
            pltpu.VMEM((2, ROWS), jnp.int32),
            pltpu.VMEM((2, ROWS), f32),
            pltpu.VMEM((1, 2048), f32),
            pltpu.VMEM((2048, 128), bf16),
            pltpu.VMEM((2048, 128), bf16),
            pltpu.VMEM((ROWS, 2048), bf16),
            pltpu.VMEM((DEPTH, 128, 2048), bf16),
            pltpu.VMEM((2048 + HALO, 128), f32),
            pltpu.VMEM((HALO, 128), bf16),
            pltpu.VMEM((8, 128), f32),
            pltpu.VMEM((HALO, 128), bf16),
            pltpu.VMEM((8, 128), f32),
            pltpu.VMEM((32, 128), f32),
            pltpu.VMEM((2048, 128), bf16),
            pltpu.VMEM((256, HALF), bf16),
            pltpu.VMEM((256, HALF), bf16),
            pltpu.VMEM((2, 256, 128), f32),
            pltpu.VMEM((2, 256, 128), f32),
            pltpu.VMEM((4, 2, ROWS, 512), f32),
            pltpu.VMEM((4, ROWS, 512), f32),
            pltpu.VMEM((ROWS, 2048), bf16),
            pltpu.VMEM((32, 1, 128), f32),
            pltpu.VMEM(w_gate.shape, bf16),
            pltpu.VMEM(w_up.shape, bf16),
            pltpu.VMEM(w_down.shape, bf16),
            pltpu.VMEM(shared_gate.shape, bf16),
            pltpu.VMEM(shared_up.shape, bf16),
            pltpu.VMEM(shared_down.shape, bf16),
            pltpu.VMEM((2, 4, ROWS, HALF), bf16),
            pltpu.VMEM((2, 4, 32, 1, 128), f32),
            pltpu.VMEM((2, 3, 4) + block, bf16),
            pltpu.VMEM((2, 4) + block, bf16),
            pltpu.VMEM((2, 4, 4) + block, bf16),
            pltpu.VMEM((4, 4, CAP, 512), f32),
            pltpu.VMEM((4, 4, CAP, 512), f32),
            pltpu.VMEM((4, 4, CAP, 512), bf16),
            pltpu.VMEM((2, 3, 4) + block, bf16),
            pltpu.VMEM((2, 4) + block, bf16),
            pltpu.VMEM((2, 4, 4) + block, bf16),
            pltpu.VMEM((2, 3, ROWS, HALF), bf16),
            pltpu.VMEM((2, 2) + block, bf16),
            pltpu.VMEM((2, 2, ROWS, HALF), bf16),
            pltpu.VMEM((ROWS, 2048), f32),
            pltpu.VMEM((ROWS, 2048), f32),
            dma((11,)), dma((6,)), dma((7,)), dma((2,)), dma, dma((2, 3, 3)), dma((2, 3, 2, 2)), dma((2, 3)),
            dma, dma((4,)), dma((2, 3)), dma((2, 3)), dma((2, 4)), dma((2, 4)), dma((2, 4)), dma((2, 4)),
            dma((2, 3)),
            dma, dma((2,)), dma, dma, dma, dma, dma, dma, dma, dma, dma, dma, dma, dma, dma, dma,
        ],
        compiler_params=pltpu.CompilerParams(
            collective_id=0, has_side_effects=True, vmem_limit_bytes=54 * 1024 * 1024
        ),
    )(*[a for a, _ in args])


def solution(mesh):
    both = P(("sp", "tp"), None)
    placed = (
        P("sp", "tp"), P("sp", "tp"), P(None, "tp"), P(), P("tp", None), both, P(), P("sp"), both, both,
        P("sp", None, None), P("sp", None, None), P("sp", None, None), P(), P(), P(), P(),
    )
    return jax.shard_map(shards, mesh=mesh, in_specs=placed, out_specs=both, check_vma=False)
```

```python
import jax
import jax.numpy as jnp
from jax import lax
from jax.experimental import pallas as pl
from jax.experimental.pallas import tpu as pltpu
from jax.sharding import PartitionSpec as P

EPSILON = 1e-05
RESIDUAL_SCALE = 8.0**0.25
MESH_ID = pl.DeviceIdType.MESH
HALF = 1024
SIDE = 4
DEPTH = 8
CAP = 64
ROWS = 128
HALO = 32
TAPS = 31
PLACE = {1: 0, 7: 1, 2: 2, 6: 3, 3: 4, 5: 5, 4: 6, 0: 7}
GROUP = ((0, 2), (2, 4), (4, 7))


def normalize(values):
    mean = jnp.mean(values, -1, keepdims=True)
    square = jnp.mean(values * values, -1, keepdims=True)
    return (values - mean) * lax.rsqrt(square - mean * mean + EPSILON)


def layer_kernel(
    linear_h, gate_h, taps_h, channel_gain_h, w_h, residual_h, mix_gain_h, docs_h, ids_h, ways_h, gain_h,
    w_gate, w_up, w_down, s_gate, s_up, s_down, out,
    taps, channel_gain, mix_gain, docs, ids, ways, gain,
    linear, gate, residual, weight, gated, tail, tail_docs, halo, halo_docs, tap32, conv, conv_in, act,
    sums, sums_in, part, part_in2, normed, table,
    wg, wu, wd, sg, su, sd,
    near, meta, packed, relay, arrived, acc_g, acc_u, hidden, answers, relay_back, back, partial, relay_part,
    part_in, kept, shared,
    l_sem, w_sem, z_r, h_r, a_r, g_r, e_r, end_r, st_r, x_r, s1_r, m_r, d_r, rl_r, b_r, bl_r, p_r,
    z_s, h_s, a_s, g_s, e_s, st_s, x_s, s1_s, m_s, d_s, rl_s, fw_s, b_s, bl_s, bf_s, p_s,
):
    f32, bf16 = jnp.float32, jnp.bfloat16
    sp, tp = lax.axis_index("sp"), lax.axis_index("tp")
    y, x = sp // SIDE, sp % SIDE
    z, core = tp // 2, tp % 2
    other = 1 - core

    def at(dy, dx):
        return ((y + dy) % SIDE) * SIDE + (x + dx) % SIDE

    def first(o, k):
        return at(0, k) if o == 0 else at(k, 0)

    def second(o, k):
        return at(k, 0) if o == 0 else at(0, k)

    def along(dz):
        return ((z + dz) % DEPTH) * 2 + core

    def push(src, dst, ss, rs, to_sp, to_tp):
        pltpu.make_async_remote_copy(
            src_ref=src, dst_ref=dst, send_sem=ss, recv_sem=rs,
            device_id=(to_sp, to_tp), device_id_type=MESH_ID,
        ).start()

    def send(src, dst, ss, rs, to):
        push(src, dst, ss, rs, to, tp)

    def landed(dst, rs):
        pltpu.make_async_remote_copy(
            src_ref=dst, dst_ref=dst, send_sem=rs, recv_sem=rs,
            device_id=(first(0, 1), tp), device_id_type=MESH_ID,
        ).wait_recv()

    def gone(src, ss):
        pltpu.make_async_remote_copy(
            src_ref=src, dst_ref=src, send_sem=ss, recv_sem=ss,
            device_id=(first(0, 1), tp), device_id_type=MESH_ID,
        ).wait_send()

    own_loads = [
        pltpu.make_async_copy(a, b, l_sem.at[i])
        for i, (a, b) in enumerate(
            [
                (w_h, weight.at[7]), (linear_h, linear), (gate_h, gate), (docs_h, docs), (ids_h, ids),
                (ways_h, ways), (taps_h, taps), (channel_gain_h, channel_gain), (mix_gain_h, mix_gain),
                (gain_h, gain), (residual_h, residual),
            ]
        )
    ]
    for load in own_loads:
        load.start()
    loads = [
        pltpu.make_async_copy(a, b, w_sem.at[i])
        for i, (a, b) in enumerate(
            [(s_gate, sg), (s_up, su), (s_down, sd), (w_gate, wg), (w_up, wu), (w_down, wd)]
        )
    ]

    after, ahead = (sp + 1) % 16, (sp + 15) % 16
    barrier = pltpu.get_barrier_semaphore()

    def greet(to_sp, to_tp):
        pl.semaphore_signal(barrier, inc=1, device_id=(to_sp, to_tp), device_id_type=MESH_ID)

    for dz in (1, 7, 2, 6):
        greet(sp, along(dz))
    for to in (at(0, 1), at(0, 3), at(1, 0), at(3, 0), after, ahead):
        greet(to, tp)
    greet(sp, z * 2 + other)
    pl.semaphore_wait(barrier, 11)

    def columns(o, k, ks=0):
        fast, slow = (x, y) if o == 0 else (y, x)
        block = ((slow + ks) % SIDE) * SIDE + (fast + k) % SIDE
        return pl.ds(pl.multiple_of(block * 128, 128), 128)

    def strip(o):
        return slice(o * 64, o * 64 + 64)

    def upper(o):
        return slice(o * 64, o * 64 + 32)

    def lower(o):
        return slice(o * 64 + 32, o * 64 + 64)

    def hop(here, there, dz):
        for o in (0, 1):
            push(
                weight.at[here, strip(o), columns(o, 0)], weight.at[there, strip(o), columns(o, 0)],
                z_s, z_r.at[there], sp, along(dz),
            )

    def hopped(there):
        landed(weight.at[there, :, 0:128], z_r.at[there])

    own_loads[0].wait()
    hop(7, PLACE[7], 1)
    hop(7, PLACE[1], 7)
    hop(7, PLACE[6], 2)
    hop(7, PLACE[2], 6)

    for load in own_loads[1:4]:
        load.wait()

    def gate_rows(a, b):
        a, b = a.astype(f32), b.astype(f32)
        return (a * (1.0 / (1.0 + jnp.exp(-b)))).astype(bf16)

    tail[...] = gate_rows(linear[2048 - HALO:, :], gate[2048 - HALO:, :])
    doc = docs[...]
    spot = lax.broadcasted_iota(jnp.int32, (16, 128), 0) * 128 + lax.broadcasted_iota(jnp.int32, (16, 128), 1)
    local, last = [], []
    for d in (1, 2, 3):
        below = jnp.where(doc < d, 1.0, 0.0)
        local.append(jnp.sum(jnp.sum(below, 1, keepdims=True), 0, keepdims=True))
        below = jnp.where(spot >= 2048 - (TAPS - 1), below, 0.0)
        last.append(jnp.sum(jnp.sum(below, 1, keepdims=True), 0, keepdims=True))
    for i in range(3):
        tail_docs[i:i + 1, :] = jnp.broadcast_to(last[i], (1, 128))
    tail_docs[3:8, :] = jnp.zeros((5, 128), f32)
    push(tail, halo, h_s.at[0], h_r.at[0], after, tp)
    push(tail_docs, halo_docs, h_s.at[1], h_r.at[1], after, tp)
    for load in loads:
        load.start()

    def gate_block(i, _):
        rows = pl.ds(pl.multiple_of(i * 128, 128), 128)
        there = pl.ds(pl.multiple_of(i * 128 + HALO, 32), 128)
        gated[there, :] = gate_rows(linear[rows, :], gate[rows, :]).astype(f32)
        return 0

    lax.fori_loop(0, 16, gate_block, 0)
    for load in own_loads[4:10]:
        load.wait()
    tap32[0:TAPS, :] = taps[...].astype(f32)

    def spread(o, g, k):
        lo, hi = GROUP[g]
        mine = weight.at[lo:hi, strip(o), columns(o, k)]
        late = (0, 1, 2, 1)[k]
        send(mine, mine, e_s, e_r.at[o, g, late, 0], second(o, 1))
        send(mine, mine, e_s, e_r.at[o, g, late, 1], second(o, 3))

    def gather_start(g):
        lo, hi = GROUP[g]
        for o in (0, 1):
            mine = weight.at[lo:hi, strip(o), columns(o, 0)]
            send(mine, mine, g_s, g_r.at[o, g, 0], first(o, 1))
            send(mine, mine, g_s, g_r.at[o, g, 1], first(o, 3))
        for o in (0, 1):
            spread(o, g, 0)

    def gather_near(g):
        lo, hi = GROUP[g]
        for o in (0, 1):
            landed(weight.at[lo:hi, strip(o), columns(o, 3)], g_r.at[o, g, 0])
            half = weight.at[lo:hi, upper(o), columns(o, 3)]
            send(half, half, g_s, g_r.at[o, g, 2], first(o, 1))
            landed(weight.at[lo:hi, strip(o), columns(o, 1)], g_r.at[o, g, 1])
            half = weight.at[lo:hi, lower(o), columns(o, 1)]
            send(half, half, g_s, g_r.at[o, g, 2], first(o, 3))
        for o in (0, 1):
            spread(o, g, 3)
            spread(o, g, 1)

    def gather_far(g):
        lo, hi = GROUP[g]
        for o in (0, 1):
            landed(weight.at[lo:hi, strip(o), columns(o, 2)], g_r.at[o, g, 2])
            spread(o, g, 2)

    def gather_pass(g, ks):
        lo, hi = GROUP[g]
        late = (0, 1, 2, 1)[ks[0]]
        for o in (0, 1):
            landed(weight.at[lo:hi, strip(o), 0:128 * len(ks)], e_r.at[o, g, late, 0])
            for k in ks:
                half = weight.at[lo:hi, upper(o), columns(o, k, 3)]
                send(half, half, e_s, end_r.at[o, g], second(o, 1))
            landed(weight.at[lo:hi, strip(o), 0:128 * len(ks)], e_r.at[o, g, late, 1])
            for k in ks:
                half = weight.at[lo:hi, lower(o), columns(o, k, 1)]
                send(half, half, e_s, end_r.at[o, g], second(o, 3))

    def gather_end(g):
        lo, hi = GROUP[g]
        for o in (0, 1):
            landed(weight.at[lo:hi, strip(o), 0:512], end_r.at[o, g])

    OWN, SIDES, FAR = (0,), (3, 1), (2,)

    names = lax.broadcasted_iota(jnp.int32, (16, ROWS), 0)
    hit_0, hit_1 = names == ids[0:1, :], names == ids[1:2, :]
    hits = jnp.where(hit_0 | hit_1, 1.0, 0.0)
    before = lax.broadcasted_iota(jnp.int32, (ROWS, ROWS), 0) < lax.broadcasted_iota(jnp.int32, (ROWS, ROWS), 1)
    ranks = jnp.dot(hits.astype(bf16), jnp.where(before, 1.0, 0.0).astype(bf16), preferred_element_type=f32)
    slots = jnp.where(hits > 0.5, ranks, -1.0)
    values = jnp.where(hit_0, ways[0:1, :], 0.0) + jnp.where(hit_1, ways[1:2, :], 0.0)
    for e in range(16):
        table[e] = slots[e:e + 1, :]
        table[e + 16] = values[e:e + 1, :]
    for o in (0, 1):
        send(table, meta.at[o, 3], m_s, m_r.at[o, 0], first(o, 1))
        send(table, meta.at[o, 1], m_s, m_r.at[o, 1], first(o, 3))

    hopped(PLACE[7])
    hopped(PLACE[1])
    gather_start(0)
    hopped(PLACE[6])
    hop(PLACE[6], PLACE[5], 1)
    hop(PLACE[6], PLACE[4], 2)
    hopped(PLACE[2])
    hop(PLACE[2], PLACE[3], 7)
    gather_start(1)
    landed(halo, h_r.at[0])
    landed(halo_docs, h_r.at[1])
    inside = sp > 0
    gated[0:HALO, :] = jnp.where(inside, halo[...].astype(f32), 0.0)
    starts = []
    for i in range(3):
        extra = jnp.where(inside, halo_docs[i:i + 1, :], float(TAPS - 1)) - float(TAPS - 1)
        starts.append(local[i] + extra)

    CHUNK = 64

    def conv_block(dz):
        base = ((z + dz) % DEPTH) * 256

        def piece(i, _):
            row = pl.multiple_of(base + i * CHUNK, CHUNK)
            spot = lax.broadcasted_iota(jnp.int32, (CHUNK, 128), 0).astype(f32) + row.astype(f32)
            begun = jnp.full((CHUNK, 128), -1000.0, f32)
            for s in starts:
                begun = jnp.maximum(begun, jnp.where(s <= spot, s, -1000.0))
            age = spot - begun
            total = jnp.zeros((CHUNK, 128), f32)
            for j in range(TAPS):
                window = gated[pl.ds(row + (HALO - j), CHUNK), :]
                total = total + jnp.where(age >= float(j), window * tap32[j:j + 1, :], 0.0)
            conv[pl.ds(row, CHUNK), :] = total.astype(bf16)
            return 0

        lax.fori_loop(0, 256 // CHUNK, piece, 0)
        rows = pl.ds(pl.multiple_of(base, 256), 256)
        if dz == 0:
            conv_in[:, 7 * 128:] = conv[rows, :]

    def conv_send(*steps):
        for dz in steps:
            rows = pl.ds(pl.multiple_of(((z + dz) % DEPTH) * 256, 256), 256)
            there = PLACE[(DEPTH - dz) % DEPTH]
            push(
                conv.at[rows, :], conv_in.at[:, there * 128:(there + 1) * 128],
                a_s, a_r, sp, along(dz),
            )

    conv_block(1)
    conv_block(7)
    for o in (0, 1):
        landed(meta.at[o, 3], m_r.at[o, 0])
        send(meta.at[o, 3], meta.at[o, 2], m_s, m_r.at[o, 2], first(o, 1))
        landed(meta.at[o, 1], m_r.at[o, 1])
    gather_near(0)
    conv_block(2)
    gather_pass(0, OWN)
    hopped(PLACE[5])
    hopped(PLACE[3])
    hopped(PLACE[4])
    gather_start(2)
    conv_send(2, 1, 7)
    conv_block(6)
    conv_send(6)
    gather_near(1)
    gather_far(0)
    conv_block(3)
    conv_send(3)
    gather_pass(0, SIDES)
    gather_pass(1, OWN)
    conv_block(5)
    conv_send(5)
    gather_near(2)
    conv_block(4)
    conv_send(4)
    gather_far(1)
    conv_block(0)
    gather_pass(1, SIDES)
    gather_pass(0, FAR)
    gather_pass(2, OWN)
    gather_far(2)
    gather_pass(1, FAR)
    gather_pass(2, SIDES)

    landed(conv_in.at[:, 0:7 * 128], a_r)
    mean_part = jnp.zeros((256, 128), f32)
    square_part = jnp.zeros((256, 128), f32)
    for s in range(DEPTH):
        v = conv_in[:, s * 128:(s + 1) * 128].astype(f32)
        mean_part = mean_part + v
        square_part = square_part + v * v
    sums[0] = mean_part
    sums[1] = square_part
    push(sums, sums_in, st_s, st_r, sp, z * 2 + other)
    gather_pass(2, FAR)
    landed(sums_in, st_r)
    mean = jnp.sum(sums[0] + sums_in[0], 1, keepdims=True) * (1.0 / 2048.0)
    square = jnp.sum(sums[1] + sums_in[1], 1, keepdims=True) * (1.0 / 2048.0)
    scale = lax.rsqrt(square - mean * mean + EPSILON)
    for dz, s in PLACE.items():
        v = conv_in[:, s * 128:(s + 1) * 128].astype(f32)
        v = (v - mean) * scale * channel_gain[along(dz)]
        act[:, s * 128:(s + 1) * 128] = (v / (1.0 + jnp.exp(-v))).astype(bf16)

    for o in (0, 1):
        landed(meta.at[o, 2], m_r.at[o, 2])

    for g, (lo, hi) in enumerate(((0, 2), (2, 4), (4, 8))):
        gather_end(g)
        for n in range(4):
            w = weight[lo:hi, :, n * 512:(n + 1) * 512].reshape((hi - lo) * 128, 512)
            got = jnp.dot(act[:, lo * 128:hi * 128], w, preferred_element_type=f32).reshape(2, ROWS, 512)
            part[n] = got if g == 0 else part[n] + got
            if g == 2:
                push(part.at[n, other], part_in2.at[n], x_s, x_r.at[n], sp, z * 2 + other)
    own_loads[10].wait()
    for n in range(4):
        cols = slice(n * 512, (n + 1) * 512)
        landed(part_in2.at[n], x_r.at[n])
        kept[:, cols] = RESIDUAL_SCALE * residual[:, cols].astype(f32) + part[n, core] + part_in2[n]
    normed[...] = (normalize(kept[...]) * mix_gain[...]).astype(bf16)

    for o in (0, 1):
        mine = normed.at[:, o * HALF:(o + 1) * HALF]
        send(mine, near.at[o, 3], s1_s, s1_r.at[o, 0], first(o, 1))
        send(mine, near.at[o, 1], s1_s, s1_r.at[o, 1], first(o, 3))

    lanes = lax.broadcasted_iota(jnp.int32, (CAP, 128), 0).astype(f32)

    def expert_at(o, k):
        return second(o, k)

    def slot_row(o, k, e):
        return table[e] if k == 0 else meta[o, k, e]

    def weight_row(o, k, e):
        return table[e + 16] if k == 0 else meta[o, k, e + 16]

    def pack(o, k):
        rows = normed[:, o * HALF:(o + 1) * HALF] if k == 0 else near[o, k]
        for q in (2, 1, 3, 0):
            hit = jnp.where(lanes == slot_row(o, k, expert_at(o, q)), 1.0, 0.0).astype(bf16)
            block = jnp.dot(hit, rows, preferred_element_type=f32).astype(bf16)
            if q == 0:
                arrived[o, 0, k] = block
            else:
                packed[o, q - 1, k] = block
            if q == 2:
                way = 1 if k < 2 else 3
                send(packed.at[o, 1, k], relay.at[o, k], rl_s, rl_r.at[o, k], second(o, way))
        if k != 2:
            pack_send(o, k)

    def pack_send(o, k):
        send(packed.at[o, 0, k], arrived.at[o, 3, k], d_s, d_r.at[o, k], second(o, 1))
        send(packed.at[o, 2, k], arrived.at[o, 1, k], d_s, d_r.at[o, k], second(o, 3))

    def pass_on(o, k):
        landed(relay.at[o, k], rl_r.at[o, k])
        way = 1 if k < 2 else 3
        send(relay.at[o, k], arrived.at[o, 2, k], fw_s, d_r.at[o, k], second(o, way))

    for o in (0, 1):
        pack(o, 0)
    gone(weight.at[0:7, :, 0:128], z_s)
    gone(tail, h_s.at[0])
    gone(tail_docs, h_s.at[1])
    gone(conv_in.at[:, 0:7 * 128], a_s)
    gone(weight.at[0:7, :, 0:384], g_s)
    gone(weight.at[0:7, :, 0:1536], e_s)
    gone(sums, st_s)
    gone(part_in2, x_s)
    for o in (0, 1):
        landed(near.at[o, 3], s1_r.at[o, 0])
        send(near.at[o, 3, 0:64], near.at[o, 2, 0:64], s1_s, s1_r.at[o, 2], first(o, 1))
    for o in (0, 1):
        landed(near.at[o, 1], s1_r.at[o, 1])
        send(near.at[o, 1, 64:128], near.at[o, 2, 64:128], s1_s, s1_r.at[o, 2], first(o, 3))
    for k in (3, 1):
        for o in (0, 1):
            pack(o, k)
    for o in (0, 1):
        pass_on(o, 0)
    for o in (0, 1):
        landed(near.at[o, 2], s1_r.at[o, 2])
        pack(o, 2)

    acc_g[...] = jnp.zeros_like(acc_g)
    acc_u[...] = jnp.zeros_like(acc_u)
    for load in loads[:3]:
        load.wait()
    act = jnp.dot(normed[...], sg[...], preferred_element_type=f32)
    lin = jnp.dot(normed[...], su[...], preferred_element_type=f32)
    common = (act / (1.0 + jnp.exp(-act)) * lin).astype(bf16)
    shared[...] = jnp.dot(common, sd[...], preferred_element_type=f32)
    for k in (3, 1):
        for o in (0, 1):
            pass_on(o, k)
    for o in (0, 1):
        pack_send(o, 2)
    for o in (0, 1):
        pass_on(o, 2)
    for load in loads[3:]:
        load.wait()

    def product(o, k):
        landed(arrived.at[o, 1:4, k], d_r.at[o, k])
        rows = arrived[o, :, k].reshape(SIDE * CAP, HALF)
        for acc, w in ((acc_g, wg), (acc_u, wu)):
            got = jnp.dot(rows, w[o * HALF:(o + 1) * HALF, :], preferred_element_type=f32)
            got = got.reshape(SIDE, CAP, 512)
            if o == 0:
                acc[:, k] = acc[:, k] + got
            else:
                acc[k] = acc[k] + got

    for k in (0, 3, 1, 2):
        for o in (0, 1):
            product(o, k)

    def relayed(k):
        for o in (0, 1):
            way = 1 if k < 2 else 3
            send(answers.at[o, 1, k], relay_back.at[o, k], bl_s, bl_r.at[o, k], second(o, way))

    def direct(k):
        for o in (0, 1):
            for q in (1, 3):
                send(answers.at[o, q - 1, k], back.at[o, k, SIDE - q], b_s, b_r.at[o, k], second(o, q))

    def pass_back(o, k):
        landed(relay_back.at[o, k], bl_r.at[o, k])
        way = 1 if k < 2 else 3
        send(relay_back.at[o, k], back.at[o, k, 2], bf_s, b_r.at[o, k], second(o, way))

    ready = set()

    def hide(dy, dx):
        if (dy, dx) not in ready:
            ready.add((dy, dx))
            g = acc_g[dy, dx]
            hidden[dy, dx] = (g / (1.0 + jnp.exp(-g)) * acc_u[dy, dx]).astype(bf16)

    def answer(k):
        for o in (0, 1):
            for q in range(SIDE):
                hide(*((q, k) if o == 0 else (k, q)))
            rows = (hidden[:, k] if o == 0 else hidden[k]).reshape(SIDE * CAP, 512)
            ans = jnp.dot(rows, wd[:, o * HALF:(o + 1) * HALF], preferred_element_type=f32).astype(bf16)
            back[o, k, 0] = ans[0:CAP]
            for q in (1, 2, 3):
                answers[o, q - 1, k] = ans[q * CAP:(q + 1) * CAP]

    answer(2)
    relayed(2)
    direct(2)
    answer(1)
    relayed(1)
    answer(3)
    relayed(3)
    answer(0)

    def choose(o, k, part):
        rows = []
        for j in range(SIDE):
            e = expert_at(o, j)
            w = weight_row(o, k, e)
            high = w.astype(bf16).astype(f32)
            value = high if part == 0 else w - high
            rows.append(jnp.where(lanes == slot_row(o, k, e), value, 0.0).astype(bf16))
        return jnp.concatenate(rows, 0)

    def combine(o, k):
        landed(back.at[o, k, 1:4], b_r.at[o, k])
        rows = back[o, k].reshape(SIDE * CAP, HALF)
        dims = (((0,), (0,)), ((), ()))
        total = lax.dot_general(choose(o, k, 0), rows, dims, preferred_element_type=f32)
        return total + lax.dot_general(choose(o, k, 1), rows, dims, preferred_element_type=f32)

    def pass_sum(o, k):
        total = combine(o, k)
        mine = partial.at[o, k - 1]
        if k == 2:
            partial[o, k - 1] = total.astype(bf16)
            send(mine.at[0:64], relay_part.at[o, 0], p_s, p_r.at[o, 0], first(o, 1))
            send(mine.at[64:128], relay_part.at[o, 1], p_s, p_r.at[o, 1], first(o, 3))
        elif k == 1:
            landed(relay_part.at[o, 0], p_r.at[o, 0])
            partial[o, k - 1, 0:64] = (total[0:64] + relay_part[o, 0].astype(f32)).astype(bf16)
            partial[o, k - 1, 64:128] = total[64:128].astype(bf16)
            send(mine, part_in.at[o, 0], p_s, p_r.at[o, 2], first(o, 1))
        else:
            landed(relay_part.at[o, 1], p_r.at[o, 1])
            partial[o, k - 1, 0:64] = total[0:64].astype(bf16)
            partial[o, k - 1, 64:128] = (total[64:128] + relay_part[o, 1].astype(f32)).astype(bf16)
            send(mine, part_in.at[o, 1], p_s, p_r.at[o, 2], first(o, 3))

    def both(step, k):
        for o in (0, 1):
            step(o, k)

    both(pass_back, 2)
    direct(1)
    both(pass_back, 1)
    direct(3)
    both(pass_back, 3)
    relayed(0)
    gone(meta.at[:, 0:3], m_s)
    gone(near.at[:, 0:3], s1_s)
    gone(arrived.at[0], d_s)
    gone(relay, rl_s)
    gone(relay, fw_s)
    both(pass_sum, 2)
    direct(0)
    both(pass_back, 0)
    both(pass_sum, 1)
    both(pass_sum, 3)
    for o in (0, 1):
        kept[:, o * HALF:(o + 1) * HALF] = combine(o, 0)
    gone(back.at[0], b_s)
    gone(relay_back, bl_s)
    gone(relay_back, bf_s)
    for o in (0, 1):
        landed(part_in.at[o], p_r.at[o, 2])
        here = slice(o * HALF, (o + 1) * HALF)
        kept[:, here] = kept[:, here] + part_in[o, 0].astype(f32) + part_in[o, 1].astype(f32)
    values = RESIDUAL_SCALE * normed[...].astype(f32) + kept[...] + shared[...]
    out[...] = (normalize(values) * gain[...]).astype(bf16)
    gone(near.at[:, 0:3], p_s)


def shards(
    linear_part, gate_part, kernel_taps, channel_gain, output_weight, residual, mix_gain, documents,
    expert_ids, route_weights, expert_gate, expert_up, expert_down, shared_gate, shared_up, shared_down,
    final_gain,
):
    bf16, f32 = jnp.bfloat16, jnp.float32
    dma = pltpu.SemaphoreType.DMA
    vmem = pl.BlockSpec(memory_space=pltpu.VMEM)
    hbm = pl.BlockSpec(memory_space=pltpu.MemorySpace.HBM)
    block = (CAP, HALF)
    w_gate, w_up, w_down = expert_gate[0], expert_up[0], expert_down[0]
    args = (
        (linear_part, hbm), (gate_part, hbm), (kernel_taps, hbm), (channel_gain.reshape(16, 1, 128), hbm),
        (output_weight, hbm), (residual, hbm), (mix_gain[None, :], hbm), (documents.reshape(16, 128), hbm),
        (expert_ids.T, hbm), (route_weights.T, hbm), (final_gain[None, :], hbm),
        (w_gate, hbm), (w_up, hbm), (w_down, hbm), (shared_gate, hbm), (shared_up, hbm), (shared_down, hbm),
    )
    return pl.pallas_call(
        layer_kernel,
        out_shape=pltpu.MemorySpace.VMEM(residual.shape, bf16),
        in_specs=[spec for _, spec in args],
        out_specs=vmem,
        scratch_shapes=[
            pltpu.VMEM((TAPS, 128), bf16),
            pltpu.VMEM((16, 1, 128), f32),
            pltpu.VMEM((1, 2048), f32),
            pltpu.VMEM((16, 128), jnp.int32),
            pltpu.VMEM((2, ROWS), jnp.int32),
            pltpu.VMEM((2, ROWS), f32),
            pltpu.VMEM((1, 2048), f32),
            pltpu.VMEM((2048, 128), bf16),
            pltpu.VMEM((2048, 128), bf16),
            pltpu.VMEM((ROWS, 2048), bf16),
            pltpu.VMEM((DEPTH, 128, 2048), bf16),
            pltpu.VMEM((2048 + HALO, 128), f32),
            pltpu.VMEM((HALO, 128), bf16),
            pltpu.VMEM((8, 128), f32),
            pltpu.VMEM((HALO, 128), bf16),
            pltpu.VMEM((8, 128), f32),
            pltpu.VMEM((32, 128), f32),
            pltpu.VMEM((2048, 128), bf16),
            pltpu.VMEM((256, HALF), bf16),
            pltpu.VMEM((256, HALF), bf16),
            pltpu.VMEM((2, 256, 128), f32),
            pltpu.VMEM((2, 256, 128), f32),
            pltpu.VMEM((4, 2, ROWS, 512), f32),
            pltpu.VMEM((4, ROWS, 512), f32),
            pltpu.VMEM((ROWS, 2048), bf16),
            pltpu.VMEM((32, 1, 128), f32),
            pltpu.VMEM(w_gate.shape, bf16),
            pltpu.VMEM(w_up.shape, bf16),
            pltpu.VMEM(w_down.shape, bf16),
            pltpu.VMEM(shared_gate.shape, bf16),
            pltpu.VMEM(shared_up.shape, bf16),
            pltpu.VMEM(shared_down.shape, bf16),
            pltpu.VMEM((2, 4, ROWS, HALF), bf16),
            pltpu.VMEM((2, 4, 32, 1, 128), f32),
            pltpu.VMEM((2, 3, 4) + block, bf16),
            pltpu.VMEM((2, 4) + block, bf16),
            pltpu.VMEM((2, 4, 4) + block, bf16),
            pltpu.VMEM((4, 4, CAP, 512), f32),
            pltpu.VMEM((4, 4, CAP, 512), f32),
            pltpu.VMEM((4, 4, CAP, 512), bf16),
            pltpu.VMEM((2, 3, 4) + block, bf16),
            pltpu.VMEM((2, 4) + block, bf16),
            pltpu.VMEM((2, 4, 4) + block, bf16),
            pltpu.VMEM((2, 3, ROWS, HALF), bf16),
            pltpu.VMEM((2, 2) + block, bf16),
            pltpu.VMEM((2, 2, ROWS, HALF), bf16),
            pltpu.VMEM((ROWS, 2048), f32),
            pltpu.VMEM((ROWS, 2048), f32),
            dma((11,)), dma((6,)), dma((7,)), dma((2,)), dma, dma((2, 3, 3)), dma((2, 3, 3, 2)), dma((2, 3)),
            dma, dma((4,)), dma((2, 3)), dma((2, 3)), dma((2, 4)), dma((2, 4)), dma((2, 4)), dma((2, 4)),
            dma((2, 3)),
            dma, dma((2,)), dma, dma, dma, dma, dma, dma, dma, dma, dma, dma, dma, dma, dma, dma,
        ],
        compiler_params=pltpu.CompilerParams(
            collective_id=0, has_side_effects=True, vmem_limit_bytes=54 * 1024 * 1024
        ),
    )(*[a for a, _ in args])


def solution(mesh):
    both = P(("sp", "tp"), None)
    placed = (
        P("sp", "tp"), P("sp", "tp"), P(None, "tp"), P(), P("tp", None), both, P(), P("sp"), both, both,
        P("sp", None, None), P("sp", None, None), P("sp", None, None), P(), P(), P(), P(),
    )
    return jax.shard_map(shards, mesh=mesh, in_specs=placed, out_specs=both, check_vma=False)
```

```python
import jax
import jax.numpy as jnp
from jax import lax
from jax.experimental import pallas as pl
from jax.experimental.pallas import tpu as pltpu
from jax.sharding import PartitionSpec as P

EPSILON = 1e-05
RESIDUAL_SCALE = 8.0**0.25
MESH_ID = pl.DeviceIdType.MESH
HALF = 1024
SIDE = 4
DEPTH = 8
CAP = 64
ROWS = 128
HALO = 32
TAPS = 31
PLACE = {1: 0, 7: 1, 2: 2, 6: 3, 3: 4, 5: 5, 4: 6, 0: 7}
GROUP = ((0, 2), (2, 4), (4, 7))


def normalize(values):
    mean = jnp.mean(values, -1, keepdims=True)
    square = jnp.mean(values * values, -1, keepdims=True)
    return (values - mean) * lax.rsqrt(square - mean * mean + EPSILON)


def layer_kernel(
    linear_h, gate_h, taps_h, channel_gain_h, w_h, residual_h, mix_gain_h, docs_h, ids_h, ways_h, gain_h,
    w_gate, w_up, w_down, s_gate, s_up, s_down, out,
    taps, channel_gain, mix_gain, docs, ids, ways, gain,
    linear, gate, residual, weight, gated, tail, tail_docs, halo, halo_docs, tap32, conv, conv_in, act,
    sums, sums_in, part, part_in2, normed, table,
    wg, wu, wd, sg, su, sd,
    near, meta, packed, relay, arrived, acc_g, acc_u, hidden, answers, relay_back, back, partial, relay_part,
    part_in, kept, shared,
    l_sem, w_sem, z_r, h_r, a_r, g_r, e_r, end_r, st_r, x_r, s1_r, m_r, d_r, rl_r, b_r, bl_r, p_r,
    z_s, h_s, a_s, g_s, e_s, st_s, x_s, s1_s, m_s, d_s, rl_s, fw_s, b_s, bl_s, bf_s, p_s,
):
    f32, bf16 = jnp.float32, jnp.bfloat16
    sp, tp = lax.axis_index("sp"), lax.axis_index("tp")
    y, x = sp // SIDE, sp % SIDE
    z, core = tp // 2, tp % 2
    other = 1 - core

    def at(dy, dx):
        return ((y + dy) % SIDE) * SIDE + (x + dx) % SIDE

    def first(o, k):
        return at(0, k) if o == 0 else at(k, 0)

    def second(o, k):
        return at(k, 0) if o == 0 else at(0, k)

    def along(dz):
        return ((z + dz) % DEPTH) * 2 + core

    def push(src, dst, ss, rs, to_sp, to_tp):
        pltpu.make_async_remote_copy(
            src_ref=src, dst_ref=dst, send_sem=ss, recv_sem=rs,
            device_id=(to_sp, to_tp), device_id_type=MESH_ID,
        ).start()

    def send(src, dst, ss, rs, to):
        push(src, dst, ss, rs, to, tp)

    def landed(dst, rs):
        pltpu.make_async_remote_copy(
            src_ref=dst, dst_ref=dst, send_sem=rs, recv_sem=rs,
            device_id=(first(0, 1), tp), device_id_type=MESH_ID,
        ).wait_recv()

    def gone(src, ss):
        pltpu.make_async_remote_copy(
            src_ref=src, dst_ref=src, send_sem=ss, recv_sem=ss,
            device_id=(first(0, 1), tp), device_id_type=MESH_ID,
        ).wait_send()

    own_loads = [
        pltpu.make_async_copy(a, b, l_sem.at[i])
        for i, (a, b) in enumerate(
            [
                (w_h, weight.at[7]), (linear_h, linear), (gate_h, gate), (docs_h, docs), (ids_h, ids),
                (ways_h, ways), (taps_h, taps), (channel_gain_h, channel_gain), (mix_gain_h, mix_gain),
                (gain_h, gain), (residual_h, residual),
            ]
        )
    ]
    for load in own_loads:
        load.start()
    loads = [
        pltpu.make_async_copy(a, b, w_sem.at[i])
        for i, (a, b) in enumerate(
            [(s_gate, sg), (s_up, su), (s_down, sd), (w_gate, wg), (w_up, wu), (w_down, wd)]
        )
    ]

    after, ahead = (sp + 1) % 16, (sp + 15) % 16
    barrier = pltpu.get_barrier_semaphore()

    def greet(to_sp, to_tp):
        pl.semaphore_signal(barrier, inc=1, device_id=(to_sp, to_tp), device_id_type=MESH_ID)

    for dz in (1, 7, 2, 6):
        greet(sp, along(dz))
    for to in (at(0, 1), at(0, 3), at(1, 0), at(3, 0), after, ahead):
        greet(to, tp)
    greet(sp, z * 2 + other)
    pl.semaphore_wait(barrier, 11)

    def columns(o, k, ks=0):
        fast, slow = (x, y) if o == 0 else (y, x)
        block = ((slow + ks) % SIDE) * SIDE + (fast + k) % SIDE
        return pl.ds(pl.multiple_of(block * 128, 128), 128)

    def strip(o):
        return slice(o * 64, o * 64 + 64)

    def upper(o):
        return slice(o * 64, o * 64 + 32)

    def lower(o):
        return slice(o * 64 + 32, o * 64 + 64)

    def hop(here, there, dz):
        for o in (0, 1):
            push(
                weight.at[here, strip(o), columns(o, 0)], weight.at[there, strip(o), columns(o, 0)],
                z_s, z_r.at[there], sp, along(dz),
            )

    def hopped(there):
        landed(weight.at[there, :, 0:128], z_r.at[there])

    own_loads[0].wait()
    hop(7, PLACE[7], 1)
    hop(7, PLACE[1], 7)
    hop(7, PLACE[6], 2)
    hop(7, PLACE[2], 6)

    for load in own_loads[1:4]:
        load.wait()

    def gate_rows(a, b):
        a, b = a.astype(f32), b.astype(f32)
        return (a * (1.0 / (1.0 + jnp.exp(-b)))).astype(bf16)

    tail[...] = gate_rows(linear[2048 - HALO:, :], gate[2048 - HALO:, :])
    doc = docs[...]
    spot = lax.broadcasted_iota(jnp.int32, (16, 128), 0) * 128 + lax.broadcasted_iota(jnp.int32, (16, 128), 1)
    local, last = [], []
    for d in (1, 2, 3):
        below = jnp.where(doc < d, 1.0, 0.0)
        local.append(jnp.sum(jnp.sum(below, 1, keepdims=True), 0, keepdims=True))
        below = jnp.where(spot >= 2048 - (TAPS - 1), below, 0.0)
        last.append(jnp.sum(jnp.sum(below, 1, keepdims=True), 0, keepdims=True))
    for i in range(3):
        tail_docs[i:i + 1, :] = jnp.broadcast_to(last[i], (1, 128))
    tail_docs[3:8, :] = jnp.zeros((5, 128), f32)
    push(tail, halo, h_s.at[0], h_r.at[0], after, tp)
    push(tail_docs, halo_docs, h_s.at[1], h_r.at[1], after, tp)
    for load in loads:
        load.start()

    def gate_block(i, _):
        rows = pl.ds(pl.multiple_of(i * 128, 128), 128)
        there = pl.ds(pl.multiple_of(i * 128 + HALO, 32), 128)
        gated[there, :] = gate_rows(linear[rows, :], gate[rows, :]).astype(f32)
        return 0

    lax.fori_loop(0, 16, gate_block, 0)
    for load in own_loads[4:10]:
        load.wait()
    tap32[0:TAPS, :] = taps[...].astype(f32)

    def spread(o, g, k):
        lo, hi = GROUP[g]
        mine = weight.at[lo:hi, strip(o), columns(o, k)]
        late = (0, 1, 2, 1)[k]
        send(mine, mine, e_s, e_r.at[o, g, late, 0], second(o, 1))
        send(mine, mine, e_s, e_r.at[o, g, late, 1], second(o, 3))

    def gather_start(g):
        lo, hi = GROUP[g]
        for o in (0, 1):
            mine = weight.at[lo:hi, strip(o), columns(o, 0)]
            send(mine, mine, g_s, g_r.at[o, g, 0], first(o, 1))
            send(mine, mine, g_s, g_r.at[o, g, 1], first(o, 3))
        for o in (0, 1):
            spread(o, g, 0)

    def gather_near(g):
        lo, hi = GROUP[g]
        for o in (0, 1):
            landed(weight.at[lo:hi, strip(o), columns(o, 3)], g_r.at[o, g, 0])
            half = weight.at[lo:hi, upper(o), columns(o, 3)]
            send(half, half, g_s, g_r.at[o, g, 2], first(o, 1))
            landed(weight.at[lo:hi, strip(o), columns(o, 1)], g_r.at[o, g, 1])
            half = weight.at[lo:hi, lower(o), columns(o, 1)]
            send(half, half, g_s, g_r.at[o, g, 2], first(o, 3))
        for o in (0, 1):
            spread(o, g, 3)
            spread(o, g, 1)

    def gather_far(g):
        lo, hi = GROUP[g]
        for o in (0, 1):
            landed(weight.at[lo:hi, strip(o), columns(o, 2)], g_r.at[o, g, 2])
            spread(o, g, 2)

    def gather_pass(g, ks):
        lo, hi = GROUP[g]
        late = (0, 1, 2, 1)[ks[0]]
        for o in (0, 1):
            landed(weight.at[lo:hi, strip(o), 0:128 * len(ks)], e_r.at[o, g, late, 0])
            for k in ks:
                half = weight.at[lo:hi, upper(o), columns(o, k, 3)]
                send(half, half, e_s, end_r.at[o, g], second(o, 1))
            landed(weight.at[lo:hi, strip(o), 0:128 * len(ks)], e_r.at[o, g, late, 1])
            for k in ks:
                half = weight.at[lo:hi, lower(o), columns(o, k, 1)]
                send(half, half, e_s, end_r.at[o, g], second(o, 3))

    def gather_end(g):
        lo, hi = GROUP[g]
        for o in (0, 1):
            landed(weight.at[lo:hi, strip(o), 0:512], end_r.at[o, g])

    OWN, SIDES, FAR = (0,), (3, 1), (2,)

    names = lax.broadcasted_iota(jnp.int32, (16, ROWS), 0)
    hit_0, hit_1 = names == ids[0:1, :], names == ids[1:2, :]
    hits = jnp.where(hit_0 | hit_1, 1.0, 0.0)
    before = lax.broadcasted_iota(jnp.int32, (ROWS, ROWS), 0) < lax.broadcasted_iota(jnp.int32, (ROWS, ROWS), 1)
    ranks = jnp.dot(hits.astype(bf16), jnp.where(before, 1.0, 0.0).astype(bf16), preferred_element_type=f32)
    slots = jnp.where(hits > 0.5, ranks, -1.0)
    values = jnp.where(hit_0, ways[0:1, :], 0.0) + jnp.where(hit_1, ways[1:2, :], 0.0)
    for e in range(16):
        table[e] = slots[e:e + 1, :]
        table[e + 16] = values[e:e + 1, :]
    for o in (0, 1):
        send(table, meta.at[o, 3], m_s, m_r.at[o, 0], first(o, 1))
        send(table, meta.at[o, 1], m_s, m_r.at[o, 1], first(o, 3))

    hopped(PLACE[7])
    hopped(PLACE[1])
    gather_start(0)
    hopped(PLACE[6])
    hop(PLACE[6], PLACE[5], 1)
    hop(PLACE[6], PLACE[4], 2)
    hopped(PLACE[2])
    hop(PLACE[2], PLACE[3], 7)
    gather_start(1)
    landed(halo, h_r.at[0])
    landed(halo_docs, h_r.at[1])
    inside = sp > 0
    gated[0:HALO, :] = jnp.where(inside, halo[...].astype(f32), 0.0)
    starts = []
    for i in range(3):
        extra = jnp.where(inside, halo_docs[i:i + 1, :], float(TAPS - 1)) - float(TAPS - 1)
        starts.append(local[i] + extra)

    CHUNK = 64

    def conv_block(dz):
        base = ((z + dz) % DEPTH) * 256

        def piece(i, _):
            row = pl.multiple_of(base + i * CHUNK, CHUNK)
            spot = lax.broadcasted_iota(jnp.int32, (CHUNK, 128), 0).astype(f32) + row.astype(f32)
            begun = jnp.full((CHUNK, 128), -1000.0, f32)
            for s in starts:
                begun = jnp.maximum(begun, jnp.where(s <= spot, s, -1000.0))
            age = spot - begun
            total = jnp.zeros((CHUNK, 128), f32)
            for j in range(TAPS):
                window = gated[pl.ds(row + (HALO - j), CHUNK), :]
                total = total + jnp.where(age >= float(j), window * tap32[j:j + 1, :], 0.0)
            conv[pl.ds(row, CHUNK), :] = total.astype(bf16)
            return 0

        lax.fori_loop(0, 256 // CHUNK, piece, 0)
        rows = pl.ds(pl.multiple_of(base, 256), 256)
        if dz == 0:
            conv_in[:, 7 * 128:] = conv[rows, :]

    def conv_send(*steps):
        for dz in steps:
            rows = pl.ds(pl.multiple_of(((z + dz) % DEPTH) * 256, 256), 256)
            there = PLACE[(DEPTH - dz) % DEPTH]
            push(
                conv.at[rows, :], conv_in.at[:, there * 128:(there + 1) * 128],
                a_s, a_r, sp, along(dz),
            )

    conv_block(1)
    conv_block(7)
    for o in (0, 1):
        landed(meta.at[o, 3], m_r.at[o, 0])
        send(meta.at[o, 3], meta.at[o, 2], m_s, m_r.at[o, 2], first(o, 1))
        landed(meta.at[o, 1], m_r.at[o, 1])
    gather_near(0)
    conv_block(2)
    gather_pass(0, OWN)
    hopped(PLACE[5])
    hopped(PLACE[3])
    hopped(PLACE[4])
    gather_start(2)
    conv_send(2, 1, 7)
    conv_block(6)
    conv_send(6)
    gather_near(1)
    gather_far(0)
    conv_block(3)
    conv_send(3)
    gather_near(2)
    gather_pass(0, SIDES)
    conv_block(5)
    conv_send(5)
    gather_far(1)
    gather_pass(1, OWN)
    conv_block(4)
    conv_send(4)
    gather_far(2)
    gather_pass(1, SIDES)
    gather_pass(0, FAR)
    conv_block(0)
    gather_pass(2, OWN)
    gather_pass(2, SIDES)
    gather_pass(1, FAR)

    landed(conv_in.at[:, 0:7 * 128], a_r)
    mean_part = jnp.zeros((256, 128), f32)
    square_part = jnp.zeros((256, 128), f32)
    for s in range(DEPTH):
        v = conv_in[:, s * 128:(s + 1) * 128].astype(f32)
        mean_part = mean_part + v
        square_part = square_part + v * v
    sums[0] = mean_part
    sums[1] = square_part
    push(sums, sums_in, st_s, st_r, sp, z * 2 + other)
    gather_pass(2, FAR)
    landed(sums_in, st_r)
    mean = jnp.sum(sums[0] + sums_in[0], 1, keepdims=True) * (1.0 / 2048.0)
    square = jnp.sum(sums[1] + sums_in[1], 1, keepdims=True) * (1.0 / 2048.0)
    scale = lax.rsqrt(square - mean * mean + EPSILON)
    for dz, s in PLACE.items():
        v = conv_in[:, s * 128:(s + 1) * 128].astype(f32)
        v = (v - mean) * scale * channel_gain[along(dz)]
        act[:, s * 128:(s + 1) * 128] = (v / (1.0 + jnp.exp(-v))).astype(bf16)

    for o in (0, 1):
        landed(meta.at[o, 2], m_r.at[o, 2])

    for g, (lo, hi) in enumerate(((0, 2), (2, 4), (4, 8))):
        gather_end(g)
        for n in range(4):
            w = weight[lo:hi, :, n * 512:(n + 1) * 512].reshape((hi - lo) * 128, 512)
            got = jnp.dot(act[:, lo * 128:hi * 128], w, preferred_element_type=f32).reshape(2, ROWS, 512)
            part[n] = got if g == 0 else part[n] + got
            if g == 2:
                push(part.at[n, other], part_in2.at[n], x_s, x_r.at[n], sp, z * 2 + other)
    own_loads[10].wait()
    for n in range(4):
        cols = slice(n * 512, (n + 1) * 512)
        landed(part_in2.at[n], x_r.at[n])
        kept[:, cols] = RESIDUAL_SCALE * residual[:, cols].astype(f32) + part[n, core] + part_in2[n]
    normed[...] = (normalize(kept[...]) * mix_gain[...]).astype(bf16)

    for o in (0, 1):
        mine = normed.at[:, o * HALF:(o + 1) * HALF]
        send(mine, near.at[o, 3], s1_s, s1_r.at[o, 0], first(o, 1))
        send(mine, near.at[o, 1], s1_s, s1_r.at[o, 1], first(o, 3))

    lanes = lax.broadcasted_iota(jnp.int32, (CAP, 128), 0).astype(f32)

    def expert_at(o, k):
        return second(o, k)

    def slot_row(o, k, e):
        return table[e] if k == 0 else meta[o, k, e]

    def weight_row(o, k, e):
        return table[e + 16] if k == 0 else meta[o, k, e + 16]

    def pack(o, k):
        rows = normed[:, o * HALF:(o + 1) * HALF] if k == 0 else near[o, k]
        for q in (2, 1, 3, 0):
            hit = jnp.where(lanes == slot_row(o, k, expert_at(o, q)), 1.0, 0.0).astype(bf16)
            block = jnp.dot(hit, rows, preferred_element_type=f32).astype(bf16)
            if q == 0:
                arrived[o, 0, k] = block
            else:
                packed[o, q - 1, k] = block
            if q == 2:
                way = 1 if k < 2 else 3
                send(packed.at[o, 1, k], relay.at[o, k], rl_s, rl_r.at[o, k], second(o, way))
        if k != 2:
            pack_send(o, k)

    def pack_send(o, k):
        send(packed.at[o, 0, k], arrived.at[o, 3, k], d_s, d_r.at[o, k], second(o, 1))
        send(packed.at[o, 2, k], arrived.at[o, 1, k], d_s, d_r.at[o, k], second(o, 3))

    def pass_on(o, k):
        landed(relay.at[o, k], rl_r.at[o, k])
        way = 1 if k < 2 else 3
        send(relay.at[o, k], arrived.at[o, 2, k], fw_s, d_r.at[o, k], second(o, way))

    for o in (0, 1):
        pack(o, 0)
    gone(weight.at[0:7, :, 0:128], z_s)
    gone(tail, h_s.at[0])
    gone(tail_docs, h_s.at[1])
    gone(conv_in.at[:, 0:7 * 128], a_s)
    gone(weight.at[0:7, :, 0:384], g_s)
    gone(weight.at[0:7, :, 0:1536], e_s)
    gone(sums, st_s)
    gone(part_in2, x_s)
    for o in (0, 1):
        landed(near.at[o, 3], s1_r.at[o, 0])
        send(near.at[o, 3, 0:64], near.at[o, 2, 0:64], s1_s, s1_r.at[o, 2], first(o, 1))
    for o in (0, 1):
        landed(near.at[o, 1], s1_r.at[o, 1])
        send(near.at[o, 1, 64:128], near.at[o, 2, 64:128], s1_s, s1_r.at[o, 2], first(o, 3))
    for k in (3, 1):
        for o in (0, 1):
            pack(o, k)
    for o in (0, 1):
        pass_on(o, 0)
    for o in (0, 1):
        landed(near.at[o, 2], s1_r.at[o, 2])
        pack(o, 2)

    acc_g[...] = jnp.zeros_like(acc_g)
    acc_u[...] = jnp.zeros_like(acc_u)
    for load in loads[:3]:
        load.wait()
    act = jnp.dot(normed[...], sg[...], preferred_element_type=f32)
    lin = jnp.dot(normed[...], su[...], preferred_element_type=f32)
    common = (act / (1.0 + jnp.exp(-act)) * lin).astype(bf16)
    shared[...] = jnp.dot(common, sd[...], preferred_element_type=f32)
    for k in (3, 1):
        for o in (0, 1):
            pass_on(o, k)
    for o in (0, 1):
        pack_send(o, 2)
    for o in (0, 1):
        pass_on(o, 2)
    for load in loads[3:]:
        load.wait()

    def product(o, k):
        landed(arrived.at[o, 1:4, k], d_r.at[o, k])
        rows = arrived[o, :, k].reshape(SIDE * CAP, HALF)
        for acc, w in ((acc_g, wg), (acc_u, wu)):
            got = jnp.dot(rows, w[o * HALF:(o + 1) * HALF, :], preferred_element_type=f32)
            got = got.reshape(SIDE, CAP, 512)
            if o == 0:
                acc[:, k] = acc[:, k] + got
            else:
                acc[k] = acc[k] + got

    for k in (0, 3, 1):
        for o in (0, 1):
            product(o, k)

    def relayed(k):
        for o in (0, 1):
            way = 1 if k < 2 else 3
            send(answers.at[o, 1, k], relay_back.at[o, k], bl_s, bl_r.at[o, k], second(o, way))

    def direct(k, ways=(1, 3)):
        for o in (0, 1):
            for q in ways:
                send(answers.at[o, q - 1, k], back.at[o, k, SIDE - q], b_s, b_r.at[o, k], second(o, q))

    def pass_back(o, k):
        landed(relay_back.at[o, k], bl_r.at[o, k])
        way = 1 if k < 2 else 3
        send(relay_back.at[o, k], back.at[o, k, 2], bf_s, b_r.at[o, k], second(o, way))

    ready = set()

    def hide(dy, dx):
        if (dy, dx) not in ready:
            ready.add((dy, dx))
            g = acc_g[dy, dx]
            hidden[dy, dx] = (g / (1.0 + jnp.exp(-g)) * acc_u[dy, dx]).astype(bf16)

    def answer(k, qs=(0, 1, 2, 3)):
        for o in (0, 1):
            rows = []
            for q in qs:
                at_q = (q, k) if o == 0 else (k, q)
                hide(*at_q)
                rows.append(hidden[at_q])
            rows = jnp.concatenate(rows, 0) if len(rows) > 1 else rows[0]
            ans = jnp.dot(rows, wd[:, o * HALF:(o + 1) * HALF], preferred_element_type=f32).astype(bf16)
            for i, q in enumerate(qs):
                if q == 0:
                    back[o, k, 0] = ans[i * CAP:(i + 1) * CAP]
                else:
                    answers[o, q - 1, k] = ans[i * CAP:(i + 1) * CAP]

    answer(1, (0, 1, 3))
    direct(1)
    for o in (0, 1):
        product(o, 2)
    answer(2)
    relayed(2)
    direct(2)
    answer(1, (2,))
    relayed(1)
    answer(3)
    relayed(3)
    direct(3, (1,))
    answer(0)

    def choose(o, k, part):
        rows = []
        for j in range(SIDE):
            e = expert_at(o, j)
            w = weight_row(o, k, e)
            high = w.astype(bf16).astype(f32)
            value = high if part == 0 else w - high
            rows.append(jnp.where(lanes == slot_row(o, k, e), value, 0.0).astype(bf16))
        return jnp.concatenate(rows, 0)

    def combine(o, k):
        landed(back.at[o, k, 1:4], b_r.at[o, k])
        rows = back[o, k].reshape(SIDE * CAP, HALF)
        dims = (((0,), (0,)), ((), ()))
        total = lax.dot_general(choose(o, k, 0), rows, dims, preferred_element_type=f32)
        return total + lax.dot_general(choose(o, k, 1), rows, dims, preferred_element_type=f32)

    def send_sum(o, k, rows):
        place = 0 if k == 1 else 1
        send(partial.at[o, k - 1, rows], part_in.at[o, place, rows], p_s, p_r.at[o, 2], first(o, k))

    top, bottom = slice(0, 64), slice(64, 128)

    def pass_sum(o, k):
        total = combine(o, k)
        if k == 2:
            partial[o, 1] = total.astype(bf16)
            send(partial.at[o, 1, top], relay_part.at[o, 0], p_s, p_r.at[o, 0], first(o, 1))
            send(partial.at[o, 1, bottom], relay_part.at[o, 1], p_s, p_r.at[o, 1], first(o, 3))
            return
        early, late = (bottom, top) if k == 1 else (top, bottom)
        partial[o, k - 1, early] = total[early].astype(bf16)
        send_sum(o, k, early)
        kept[late, o * HALF:(o + 1) * HALF] = total[late]

    def pass_rest(o, k):
        place, late = (0, top) if k == 1 else (1, bottom)
        landed(relay_part.at[o, place], p_r.at[o, place])
        total = kept[late, o * HALF:(o + 1) * HALF] + relay_part[o, place].astype(f32)
        partial[o, k - 1, late] = total.astype(bf16)
        send_sum(o, k, late)

    def both(step, k):
        for o in (0, 1):
            step(o, k)

    both(pass_back, 2)
    direct(3, (3,))
    both(pass_back, 1)
    relayed(0)
    both(pass_back, 3)
    gone(meta.at[:, 0:3], m_s)
    gone(near.at[:, 0:3], s1_s)
    gone(arrived.at[0], d_s)
    gone(relay, rl_s)
    gone(relay, fw_s)
    both(pass_sum, 2)
    direct(0)
    both(pass_sum, 1)
    both(pass_back, 0)
    both(pass_sum, 3)
    both(pass_rest, 1)
    both(pass_rest, 3)
    for o in (0, 1):
        kept[:, o * HALF:(o + 1) * HALF] = combine(o, 0)
    gone(back.at[0], b_s)
    gone(relay_back, bl_s)
    gone(relay_back, bf_s)
    for o in (0, 1):
        landed(part_in.at[o], p_r.at[o, 2])
        here = slice(o * HALF, (o + 1) * HALF)
        kept[:, here] = kept[:, here] + part_in[o, 0].astype(f32) + part_in[o, 1].astype(f32)
    values = RESIDUAL_SCALE * normed[...].astype(f32) + kept[...] + shared[...]
    out[...] = (normalize(values) * gain[...]).astype(bf16)
    gone(near.at[:, 0:3], p_s)


def shards(
    linear_part, gate_part, kernel_taps, channel_gain, output_weight, residual, mix_gain, documents,
    expert_ids, route_weights, expert_gate, expert_up, expert_down, shared_gate, shared_up, shared_down,
    final_gain,
):
    bf16, f32 = jnp.bfloat16, jnp.float32
    dma = pltpu.SemaphoreType.DMA
    vmem = pl.BlockSpec(memory_space=pltpu.VMEM)
    hbm = pl.BlockSpec(memory_space=pltpu.MemorySpace.HBM)
    block = (CAP, HALF)
    w_gate, w_up, w_down = expert_gate[0], expert_up[0], expert_down[0]
    args = (
        (linear_part, hbm), (gate_part, hbm), (kernel_taps, hbm), (channel_gain.reshape(16, 1, 128), hbm),
        (output_weight, hbm), (residual, hbm), (mix_gain[None, :], hbm), (documents.reshape(16, 128), hbm),
        (expert_ids.T, hbm), (route_weights.T, hbm), (final_gain[None, :], hbm),
        (w_gate, hbm), (w_up, hbm), (w_down, hbm), (shared_gate, hbm), (shared_up, hbm), (shared_down, hbm),
    )
    return pl.pallas_call(
        layer_kernel,
        out_shape=pltpu.MemorySpace.VMEM(residual.shape, bf16),
        in_specs=[spec for _, spec in args],
        out_specs=vmem,
        scratch_shapes=[
            pltpu.VMEM((TAPS, 128), bf16),
            pltpu.VMEM((16, 1, 128), f32),
            pltpu.VMEM((1, 2048), f32),
            pltpu.VMEM((16, 128), jnp.int32),
            pltpu.VMEM((2, ROWS), jnp.int32),
            pltpu.VMEM((2, ROWS), f32),
            pltpu.VMEM((1, 2048), f32),
            pltpu.VMEM((2048, 128), bf16),
            pltpu.VMEM((2048, 128), bf16),
            pltpu.VMEM((ROWS, 2048), bf16),
            pltpu.VMEM((DEPTH, 128, 2048), bf16),
            pltpu.VMEM((2048 + HALO, 128), f32),
            pltpu.VMEM((HALO, 128), bf16),
            pltpu.VMEM((8, 128), f32),
            pltpu.VMEM((HALO, 128), bf16),
            pltpu.VMEM((8, 128), f32),
            pltpu.VMEM((32, 128), f32),
            pltpu.VMEM((2048, 128), bf16),
            pltpu.VMEM((256, HALF), bf16),
            pltpu.VMEM((256, HALF), bf16),
            pltpu.VMEM((2, 256, 128), f32),
            pltpu.VMEM((2, 256, 128), f32),
            pltpu.VMEM((4, 2, ROWS, 512), f32),
            pltpu.VMEM((4, ROWS, 512), f32),
            pltpu.VMEM((ROWS, 2048), bf16),
            pltpu.VMEM((32, 1, 128), f32),
            pltpu.VMEM(w_gate.shape, bf16),
            pltpu.VMEM(w_up.shape, bf16),
            pltpu.VMEM(w_down.shape, bf16),
            pltpu.VMEM(shared_gate.shape, bf16),
            pltpu.VMEM(shared_up.shape, bf16),
            pltpu.VMEM(shared_down.shape, bf16),
            pltpu.VMEM((2, 4, ROWS, HALF), bf16),
            pltpu.VMEM((2, 4, 32, 1, 128), f32),
            pltpu.VMEM((2, 3, 4) + block, bf16),
            pltpu.VMEM((2, 4) + block, bf16),
            pltpu.VMEM((2, 4, 4) + block, bf16),
            pltpu.VMEM((4, 4, CAP, 512), f32),
            pltpu.VMEM((4, 4, CAP, 512), f32),
            pltpu.VMEM((4, 4, CAP, 512), bf16),
            pltpu.VMEM((2, 3, 4) + block, bf16),
            pltpu.VMEM((2, 4) + block, bf16),
            pltpu.VMEM((2, 4, 4) + block, bf16),
            pltpu.VMEM((2, 3, ROWS, HALF), bf16),
            pltpu.VMEM((2, 2) + block, bf16),
            pltpu.VMEM((2, 2, ROWS, HALF), bf16),
            pltpu.VMEM((ROWS, 2048), f32),
            pltpu.VMEM((ROWS, 2048), f32),
            dma((11,)), dma((6,)), dma((7,)), dma((2,)), dma, dma((2, 3, 3)), dma((2, 3, 3, 2)), dma((2, 3)),
            dma, dma((4,)), dma((2, 3)), dma((2, 3)), dma((2, 4)), dma((2, 4)), dma((2, 4)), dma((2, 4)),
            dma((2, 3)),
            dma, dma((2,)), dma, dma, dma, dma, dma, dma, dma, dma, dma, dma, dma, dma, dma, dma,
        ],
        compiler_params=pltpu.CompilerParams(
            collective_id=0, has_side_effects=True, vmem_limit_bytes=54 * 1024 * 1024
        ),
    )(*[a for a, _ in args])


def solution(mesh):
    both = P(("sp", "tp"), None)
    placed = (
        P("sp", "tp"), P("sp", "tp"), P(None, "tp"), P(), P("tp", None), both, P(), P("sp"), both, both,
        P("sp", None, None), P("sp", None, None), P("sp", None, None), P(), P(), P(), P(),
    )
    return jax.shard_map(shards, mesh=mesh, in_specs=placed, out_specs=both, check_vma=False)
```

```python
import jax
import jax.numpy as jnp
from jax import lax
from jax.experimental import pallas as pl
from jax.experimental.pallas import tpu as pltpu
from jax.sharding import PartitionSpec as P

EPSILON = 1e-05
RESIDUAL_SCALE = 8.0**0.25
MESH_ID = pl.DeviceIdType.MESH
HALF = 1024
SIDE = 4
DEPTH = 8
CAP = 64
ROWS = 128
HALO = 32
TAPS = 31
PLACE = {1: 0, 7: 1, 2: 2, 6: 3, 3: 4, 5: 5, 4: 6, 0: 7}
GROUP = ((0, 2), (2, 4), (4, 7))


def normalize(values):
    mean = jnp.mean(values, -1, keepdims=True)
    square = jnp.mean(values * values, -1, keepdims=True)
    return (values - mean) * lax.rsqrt(square - mean * mean + EPSILON)


def layer_kernel(
    linear_h, gate_h, taps_h, channel_gain_h, w_h, residual_h, mix_gain_h, docs_h, ids_h, ways_h, gain_h,
    w_gate, w_up, w_down, s_gate, s_up, s_down, out,
    taps, channel_gain, mix_gain, docs, ids, ways, gain,
    linear, gate, residual, weight, gated, tail, tail_docs, halo, halo_docs, tap32, conv, conv_in, act,
    sums, sums_in, part, part_in2, normed, table,
    wg, wu, wd, sg, su, sd,
    near, meta, packed, relay, arrived, acc_g, acc_u, hidden, answers, relay_back, back, partial, relay_part,
    part_in, kept, shared,
    l_sem, w_sem, z_r, h_r, a_r, g_r, e_r, end_r, st_r, x_r, s1_r, m_r, d_r, rl_r, b_r, bl_r, p_r,
    z_s, h_s, a_s, g_s, e_s, st_s, x_s, s1_s, m_s, d_s, rl_s, fw_s, b_s, bl_s, bf_s, p_s,
):
    f32, bf16 = jnp.float32, jnp.bfloat16
    sp, tp = lax.axis_index("sp"), lax.axis_index("tp")
    y, x = sp // SIDE, sp % SIDE
    z, core = tp // 2, tp % 2
    other = 1 - core

    def at(dy, dx):
        return ((y + dy) % SIDE) * SIDE + (x + dx) % SIDE

    def first(o, k):
        return at(0, k) if o == 0 else at(k, 0)

    def second(o, k):
        return at(k, 0) if o == 0 else at(0, k)

    def along(dz):
        return ((z + dz) % DEPTH) * 2 + core

    def push(src, dst, ss, rs, to_sp, to_tp):
        pltpu.make_async_remote_copy(
            src_ref=src, dst_ref=dst, send_sem=ss, recv_sem=rs,
            device_id=(to_sp, to_tp), device_id_type=MESH_ID,
        ).start()

    def send(src, dst, ss, rs, to):
        push(src, dst, ss, rs, to, tp)

    def landed(dst, rs):
        pltpu.make_async_remote_copy(
            src_ref=dst, dst_ref=dst, send_sem=rs, recv_sem=rs,
            device_id=(first(0, 1), tp), device_id_type=MESH_ID,
        ).wait_recv()

    def gone(src, ss):
        pltpu.make_async_remote_copy(
            src_ref=src, dst_ref=src, send_sem=ss, recv_sem=ss,
            device_id=(first(0, 1), tp), device_id_type=MESH_ID,
        ).wait_send()

    own_loads = [
        pltpu.make_async_copy(a, b, l_sem.at[i])
        for i, (a, b) in enumerate(
            [
                (w_h, weight.at[7]), (linear_h, linear), (gate_h, gate), (docs_h, docs), (ids_h, ids),
                (ways_h, ways), (taps_h, taps), (channel_gain_h, channel_gain), (mix_gain_h, mix_gain),
                (gain_h, gain), (residual_h, residual),
            ]
        )
    ]
    for load in own_loads:
        load.start()
    loads = [
        pltpu.make_async_copy(a, b, w_sem.at[i])
        for i, (a, b) in enumerate(
            [(s_gate, sg), (s_up, su), (s_down, sd), (w_gate, wg), (w_up, wu), (w_down, wd)]
        )
    ]

    after, ahead = (sp + 1) % 16, (sp + 15) % 16
    barrier = pltpu.get_barrier_semaphore()

    def greet(to_sp, to_tp):
        pl.semaphore_signal(barrier, inc=1, device_id=(to_sp, to_tp), device_id_type=MESH_ID)

    for dz in (1, 7, 2, 6):
        greet(sp, along(dz))
    for to in (at(0, 1), at(0, 3), at(1, 0), at(3, 0), after, ahead):
        greet(to, tp)
    greet(sp, z * 2 + other)
    pl.semaphore_wait(barrier, 11)

    def columns(o, k, ks=0):
        fast, slow = (x, y) if o == 0 else (y, x)
        block = ((slow + ks) % SIDE) * SIDE + (fast + k) % SIDE
        return pl.ds(pl.multiple_of(block * 128, 128), 128)

    def strip(o):
        return slice(o * 64, o * 64 + 64)

    def upper(o):
        return slice(o * 64, o * 64 + 32)

    def lower(o):
        return slice(o * 64 + 32, o * 64 + 64)

    def hop(here, there, dz):
        for o in (0, 1):
            push(
                weight.at[here, strip(o), columns(o, 0)], weight.at[there, strip(o), columns(o, 0)],
                z_s, z_r.at[there], sp, along(dz),
            )

    def hopped(there):
        landed(weight.at[there, :, 0:128], z_r.at[there])

    own_loads[0].wait()
    hop(7, PLACE[7], 1)
    hop(7, PLACE[1], 7)
    hop(7, PLACE[6], 2)
    hop(7, PLACE[2], 6)

    for load in own_loads[1:4]:
        load.wait()

    def gate_rows(a, b):
        a, b = a.astype(f32), b.astype(f32)
        return (a * (1.0 / (1.0 + jnp.exp(-b)))).astype(bf16)

    tail[...] = gate_rows(linear[2048 - HALO:, :], gate[2048 - HALO:, :])
    doc = docs[...]
    spot = lax.broadcasted_iota(jnp.int32, (16, 128), 0) * 128 + lax.broadcasted_iota(jnp.int32, (16, 128), 1)
    local, last = [], []
    for d in (1, 2, 3):
        below = jnp.where(doc < d, 1.0, 0.0)
        local.append(jnp.sum(jnp.sum(below, 1, keepdims=True), 0, keepdims=True))
        below = jnp.where(spot >= 2048 - (TAPS - 1), below, 0.0)
        last.append(jnp.sum(jnp.sum(below, 1, keepdims=True), 0, keepdims=True))
    for i in range(3):
        tail_docs[i:i + 1, :] = jnp.broadcast_to(last[i], (1, 128))
    tail_docs[3:8, :] = jnp.zeros((5, 128), f32)
    push(tail, halo, h_s.at[0], h_r.at[0], after, tp)
    push(tail_docs, halo_docs, h_s.at[1], h_r.at[1], after, tp)
    for load in loads:
        load.start()

    def gate_block(i, _):
        rows = pl.ds(pl.multiple_of(i * 128, 128), 128)
        there = pl.ds(pl.multiple_of(i * 128 + HALO, 32), 128)
        gated[there, :] = gate_rows(linear[rows, :], gate[rows, :]).astype(f32)
        return 0

    lax.fori_loop(0, 16, gate_block, 0)
    for load in own_loads[4:10]:
        load.wait()
    tap32[0:TAPS, :] = taps[...].astype(f32)

    def spread(o, g, k):
        lo, hi = GROUP[g]
        mine = weight.at[lo:hi, strip(o), columns(o, k)]
        late = (0, 1, 2, 1)[k]
        send(mine, mine, e_s, e_r.at[o, g, late, 0], second(o, 1))
        send(mine, mine, e_s, e_r.at[o, g, late, 1], second(o, 3))

    def gather_start(g):
        lo, hi = GROUP[g]
        for o in (0, 1):
            mine = weight.at[lo:hi, strip(o), columns(o, 0)]
            send(mine, mine, g_s, g_r.at[o, g, 0], first(o, 1))
            send(mine, mine, g_s, g_r.at[o, g, 1], first(o, 3))
        for o in (0, 1):
            spread(o, g, 0)

    def gather_near(g):
        lo, hi = GROUP[g]
        for o in (0, 1):
            landed(weight.at[lo:hi, strip(o), columns(o, 3)], g_r.at[o, g, 0])
            half = weight.at[lo:hi, upper(o), columns(o, 3)]
            send(half, half, g_s, g_r.at[o, g, 2], first(o, 1))
            landed(weight.at[lo:hi, strip(o), columns(o, 1)], g_r.at[o, g, 1])
            half = weight.at[lo:hi, lower(o), columns(o, 1)]
            send(half, half, g_s, g_r.at[o, g, 2], first(o, 3))
        for o in (0, 1):
            spread(o, g, 3)
            spread(o, g, 1)

    def gather_far(g):
        lo, hi = GROUP[g]
        for o in (0, 1):
            landed(weight.at[lo:hi, strip(o), columns(o, 2)], g_r.at[o, g, 2])
            spread(o, g, 2)

    def gather_pass(g, ks):
        lo, hi = GROUP[g]
        late = (0, 1, 2, 1)[ks[0]]
        for o in (0, 1):
            landed(weight.at[lo:hi, strip(o), 0:128 * len(ks)], e_r.at[o, g, late, 0])
            for k in ks:
                half = weight.at[lo:hi, upper(o), columns(o, k, 3)]
                send(half, half, e_s, end_r.at[o, g], second(o, 1))
            landed(weight.at[lo:hi, strip(o), 0:128 * len(ks)], e_r.at[o, g, late, 1])
            for k in ks:
                half = weight.at[lo:hi, lower(o), columns(o, k, 1)]
                send(half, half, e_s, end_r.at[o, g], second(o, 3))

    def gather_end(g):
        lo, hi = GROUP[g]
        for o in (0, 1):
            landed(weight.at[lo:hi, strip(o), 0:512], end_r.at[o, g])

    OWN, SIDES, FAR = (0,), (3, 1), (2,)

    names = lax.broadcasted_iota(jnp.int32, (16, ROWS), 0)
    hit_0, hit_1 = names == ids[0:1, :], names == ids[1:2, :]
    hits = jnp.where(hit_0 | hit_1, 1.0, 0.0)
    before = lax.broadcasted_iota(jnp.int32, (ROWS, ROWS), 0) < lax.broadcasted_iota(jnp.int32, (ROWS, ROWS), 1)
    ranks = jnp.dot(hits.astype(bf16), jnp.where(before, 1.0, 0.0).astype(bf16), preferred_element_type=f32)
    slots = jnp.where(hits > 0.5, ranks, -1.0)
    values = jnp.where(hit_0, ways[0:1, :], 0.0) + jnp.where(hit_1, ways[1:2, :], 0.0)
    for e in range(16):
        table[e] = slots[e:e + 1, :]
        table[e + 16] = values[e:e + 1, :]
    for o in (0, 1):
        send(table, meta.at[o, 3], m_s, m_r.at[o, 0], first(o, 1))
        send(table, meta.at[o, 1], m_s, m_r.at[o, 1], first(o, 3))

    hopped(PLACE[7])
    hopped(PLACE[1])
    gather_start(0)
    hopped(PLACE[6])
    hop(PLACE[6], PLACE[5], 1)
    hop(PLACE[6], PLACE[4], 2)
    hopped(PLACE[2])
    hop(PLACE[2], PLACE[3], 7)
    gather_start(1)
    landed(halo, h_r.at[0])
    landed(halo_docs, h_r.at[1])
    inside = sp > 0
    gated[0:HALO, :] = jnp.where(inside, halo[...].astype(f32), 0.0)
    starts = []
    for i in range(3):
        extra = jnp.where(inside, halo_docs[i:i + 1, :], float(TAPS - 1)) - float(TAPS - 1)
        starts.append(local[i] + extra)

    CHUNK = 64

    def conv_block(dz):
        base = ((z + dz) % DEPTH) * 256

        def piece(i, _):
            row = pl.multiple_of(base + i * CHUNK, CHUNK)
            spot = lax.broadcasted_iota(jnp.int32, (CHUNK, 128), 0).astype(f32) + row.astype(f32)
            begun = jnp.full((CHUNK, 128), -1000.0, f32)
            for s in starts:
                begun = jnp.maximum(begun, jnp.where(s <= spot, s, -1000.0))
            age = spot - begun
            total = jnp.zeros((CHUNK, 128), f32)
            for j in range(TAPS):
                window = gated[pl.ds(row + (HALO - j), CHUNK), :]
                total = total + jnp.where(age >= float(j), window * tap32[j:j + 1, :], 0.0)
            conv[pl.ds(row, CHUNK), :] = total.astype(bf16)
            return 0

        lax.fori_loop(0, 256 // CHUNK, piece, 0)
        rows = pl.ds(pl.multiple_of(base, 256), 256)
        if dz == 0:
            conv_in[:, 7 * 128:] = conv[rows, :]

    def conv_send(*steps):
        for dz in steps:
            rows = pl.ds(pl.multiple_of(((z + dz) % DEPTH) * 256, 256), 256)
            there = PLACE[(DEPTH - dz) % DEPTH]
            push(
                conv.at[rows, :], conv_in.at[:, there * 128:(there + 1) * 128],
                a_s, a_r, sp, along(dz),
            )

    conv_block(1)
    conv_block(7)
    for o in (0, 1):
        landed(meta.at[o, 3], m_r.at[o, 0])
        send(meta.at[o, 3], meta.at[o, 2], m_s, m_r.at[o, 2], first(o, 1))
        landed(meta.at[o, 1], m_r.at[o, 1])
    gather_near(0)
    conv_block(2)
    gather_pass(0, OWN)
    hopped(PLACE[5])
    hopped(PLACE[3])
    hopped(PLACE[4])
    gather_start(2)
    conv_send(2, 1, 7)
    conv_block(6)
    conv_send(6)
    gather_near(1)
    gather_far(0)
    conv_block(3)
    conv_send(3)
    gather_near(2)
    gather_pass(0, SIDES)
    conv_block(5)
    conv_send(5)
    gather_far(1)
    gather_pass(1, OWN)
    conv_block(4)
    conv_send(4)
    gather_far(2)
    gather_pass(1, SIDES)
    gather_pass(0, FAR)
    conv_block(0)
    gather_pass(2, OWN)
    gather_pass(2, SIDES)
    gather_pass(1, FAR)
    gather_pass(2, FAR)

    landed(conv_in.at[:, 0:7 * 128], a_r)
    mean_part = jnp.zeros((256, 128), f32)
    square_part = jnp.zeros((256, 128), f32)
    for s in range(DEPTH):
        v = conv_in[:, s * 128:(s + 1) * 128].astype(f32)
        mean_part = mean_part + v
        square_part = square_part + v * v
    sums[0] = mean_part
    sums[1] = square_part
    push(sums, sums_in, st_s, st_r, sp, z * 2 + other)
    landed(sums_in, st_r)
    mean = jnp.sum(sums[0] + sums_in[0], 1, keepdims=True) * (1.0 / 2048.0)
    square = jnp.sum(sums[1] + sums_in[1], 1, keepdims=True) * (1.0 / 2048.0)
    scale = lax.rsqrt(square - mean * mean + EPSILON)
    for dz, s in PLACE.items():
        v = conv_in[:, s * 128:(s + 1) * 128].astype(f32)
        v = (v - mean) * scale * channel_gain[along(dz)]
        act[:, s * 128:(s + 1) * 128] = (v / (1.0 + jnp.exp(-v))).astype(bf16)

    for o in (0, 1):
        landed(meta.at[o, 2], m_r.at[o, 2])

    for g, (lo, hi) in enumerate(((0, 2), (2, 4), (4, 8))):
        gather_end(g)
        for n in range(4):
            w = weight[lo:hi, :, n * 512:(n + 1) * 512].reshape((hi - lo) * 128, 512)
            got = jnp.dot(act[:, lo * 128:hi * 128], w, preferred_element_type=f32).reshape(2, ROWS, 512)
            part[n] = got if g == 0 else part[n] + got
            if g == 2:
                push(part.at[n, other], part_in2.at[n], x_s, x_r.at[n], sp, z * 2 + other)
    own_loads[10].wait()
    for n in range(4):
        cols = slice(n * 512, (n + 1) * 512)
        landed(part_in2.at[n], x_r.at[n])
        kept[:, cols] = RESIDUAL_SCALE * residual[:, cols].astype(f32) + part[n, core] + part_in2[n]
    normed[...] = (normalize(kept[...]) * mix_gain[...]).astype(bf16)

    for o in (0, 1):
        mine = normed.at[:, o * HALF:(o + 1) * HALF]
        send(mine, near.at[o, 3], s1_s, s1_r.at[o, 0], first(o, 1))
        send(mine, near.at[o, 1], s1_s, s1_r.at[o, 1], first(o, 3))

    lanes = lax.broadcasted_iota(jnp.int32, (CAP, 128), 0).astype(f32)

    def expert_at(o, k):
        return second(o, k)

    def slot_row(o, k, e):
        return table[e] if k == 0 else meta[o, k, e]

    def weight_row(o, k, e):
        return table[e + 16] if k == 0 else meta[o, k, e + 16]

    def pack(o, k):
        rows = normed[:, o * HALF:(o + 1) * HALF] if k == 0 else near[o, k]
        for q in (2, 1, 3, 0):
            hit = jnp.where(lanes == slot_row(o, k, expert_at(o, q)), 1.0, 0.0).astype(bf16)
            block = jnp.dot(hit, rows, preferred_element_type=f32).astype(bf16)
            if q == 0:
                arrived[o, 0, k] = block
            else:
                packed[o, q - 1, k] = block
            if q == 2:
                way = 1 if k < 2 else 3
                send(packed.at[o, 1, k], relay.at[o, k], rl_s, rl_r.at[o, k], second(o, way))
        if k != 2:
            pack_send(o, k)

    def pack_send(o, k):
        send(packed.at[o, 0, k], arrived.at[o, 3, k], d_s, d_r.at[o, k], second(o, 1))
        send(packed.at[o, 2, k], arrived.at[o, 1, k], d_s, d_r.at[o, k], second(o, 3))

    def pass_on(o, k):
        landed(relay.at[o, k], rl_r.at[o, k])
        way = 1 if k < 2 else 3
        send(relay.at[o, k], arrived.at[o, 2, k], fw_s, d_r.at[o, k], second(o, way))

    for o in (0, 1):
        pack(o, 0)
    gone(weight.at[0:7, :, 0:128], z_s)
    gone(tail, h_s.at[0])
    gone(tail_docs, h_s.at[1])
    gone(conv_in.at[:, 0:7 * 128], a_s)
    gone(weight.at[0:7, :, 0:384], g_s)
    gone(weight.at[0:7, :, 0:1536], e_s)
    gone(sums, st_s)
    gone(part_in2, x_s)
    for o in (0, 1):
        landed(near.at[o, 3], s1_r.at[o, 0])
        send(near.at[o, 3, 0:64], near.at[o, 2, 0:64], s1_s, s1_r.at[o, 2], first(o, 1))
    for o in (0, 1):
        landed(near.at[o, 1], s1_r.at[o, 1])
        send(near.at[o, 1, 64:128], near.at[o, 2, 64:128], s1_s, s1_r.at[o, 2], first(o, 3))
    for k in (3, 1):
        for o in (0, 1):
            pack(o, k)
    for o in (0, 1):
        pass_on(o, 0)
    for o in (0, 1):
        landed(near.at[o, 2], s1_r.at[o, 2])
        pack(o, 2)

    acc_g[...] = jnp.zeros_like(acc_g)
    acc_u[...] = jnp.zeros_like(acc_u)
    for load in loads[:3]:
        load.wait()
    act = jnp.dot(normed[...], sg[...], preferred_element_type=f32)
    lin = jnp.dot(normed[...], su[...], preferred_element_type=f32)
    common = (act / (1.0 + jnp.exp(-act)) * lin).astype(bf16)
    shared[...] = jnp.dot(common, sd[...], preferred_element_type=f32)
    for k in (3, 1):
        for o in (0, 1):
            pass_on(o, k)
    for o in (0, 1):
        pack_send(o, 2)
    for o in (0, 1):
        pass_on(o, 2)
    for load in loads[3:]:
        load.wait()

    def product(o, k):
        landed(arrived.at[o, 1:4, k], d_r.at[o, k])
        rows = arrived[o, :, k].reshape(SIDE * CAP, HALF)
        for acc, w in ((acc_g, wg), (acc_u, wu)):
            got = jnp.dot(rows, w[o * HALF:(o + 1) * HALF, :], preferred_element_type=f32)
            got = got.reshape(SIDE, CAP, 512)
            if o == 0:
                acc[:, k] = acc[:, k] + got
            else:
                acc[k] = acc[k] + got

    for k in (0, 3, 1):
        for o in (0, 1):
            product(o, k)

    def relayed(k):
        for o in (0, 1):
            way = 1 if k < 2 else 3
            send(answers.at[o, 1, k], relay_back.at[o, k], bl_s, bl_r.at[o, k], second(o, way))

    def direct(k, ways=(1, 3)):
        for o in (0, 1):
            for q in ways:
                send(answers.at[o, q - 1, k], back.at[o, k, SIDE - q], b_s, b_r.at[o, k], second(o, q))

    def pass_back(o, k):
        landed(relay_back.at[o, k], bl_r.at[o, k])
        way = 1 if k < 2 else 3
        send(relay_back.at[o, k], back.at[o, k, 2], bf_s, b_r.at[o, k], second(o, way))

    ready = set()

    def hide(dy, dx):
        if (dy, dx) not in ready:
            ready.add((dy, dx))
            g = acc_g[dy, dx]
            hidden[dy, dx] = (g / (1.0 + jnp.exp(-g)) * acc_u[dy, dx]).astype(bf16)

    def answer(k, qs=(0, 1, 2, 3)):
        for o in (0, 1):
            rows = []
            for q in qs:
                at_q = (q, k) if o == 0 else (k, q)
                hide(*at_q)
                rows.append(hidden[at_q])
            rows = jnp.concatenate(rows, 0) if len(rows) > 1 else rows[0]
            ans = jnp.dot(rows, wd[:, o * HALF:(o + 1) * HALF], preferred_element_type=f32).astype(bf16)
            for i, q in enumerate(qs):
                if q == 0:
                    back[o, k, 0] = ans[i * CAP:(i + 1) * CAP]
                else:
                    answers[o, q - 1, k] = ans[i * CAP:(i + 1) * CAP]

    answer(1, (0, 1, 3))
    direct(1)
    for o in (0, 1):
        product(o, 2)
    answer(2)
    relayed(2)
    direct(2)
    answer(1, (2,))
    relayed(1)
    answer(3)
    relayed(3)
    direct(3, (1,))
    answer(0)

    def choose(o, k, part):
        rows = []
        for j in range(SIDE):
            e = expert_at(o, j)
            w = weight_row(o, k, e)
            high = w.astype(bf16).astype(f32)
            value = high if part == 0 else w - high
            rows.append(jnp.where(lanes == slot_row(o, k, e), value, 0.0).astype(bf16))
        return jnp.concatenate(rows, 0)

    def combine(o, k):
        landed(back.at[o, k, 1:4], b_r.at[o, k])
        rows = back[o, k].reshape(SIDE * CAP, HALF)
        dims = (((0,), (0,)), ((), ()))
        total = lax.dot_general(choose(o, k, 0), rows, dims, preferred_element_type=f32)
        return total + lax.dot_general(choose(o, k, 1), rows, dims, preferred_element_type=f32)

    def send_sum(o, k, rows):
        place = 0 if k == 1 else 1
        send(partial.at[o, k - 1, rows], part_in.at[o, place, rows], p_s, p_r.at[o, 2], first(o, k))

    top, bottom = slice(0, 64), slice(64, 128)

    def pass_sum(o, k):
        total = combine(o, k)
        if k == 2:
            partial[o, 1] = total.astype(bf16)
            send(partial.at[o, 1, top], relay_part.at[o, 0], p_s, p_r.at[o, 0], first(o, 1))
            send(partial.at[o, 1, bottom], relay_part.at[o, 1], p_s, p_r.at[o, 1], first(o, 3))
            return
        early, late = (bottom, top) if k == 1 else (top, bottom)
        partial[o, k - 1, early] = total[early].astype(bf16)
        send_sum(o, k, early)
        kept[late, o * HALF:(o + 1) * HALF] = total[late]

    def pass_rest(o, k):
        place, late = (0, top) if k == 1 else (1, bottom)
        landed(relay_part.at[o, place], p_r.at[o, place])
        total = kept[late, o * HALF:(o + 1) * HALF] + relay_part[o, place].astype(f32)
        partial[o, k - 1, late] = total.astype(bf16)
        send_sum(o, k, late)

    def both(step, k):
        for o in (0, 1):
            step(o, k)

    both(pass_back, 2)
    direct(3, (3,))
    both(pass_back, 1)
    relayed(0)
    both(pass_back, 3)
    gone(meta.at[:, 0:3], m_s)
    gone(near.at[:, 0:3], s1_s)
    gone(arrived.at[0], d_s)
    gone(relay, rl_s)
    gone(relay, fw_s)
    both(pass_sum, 2)
    direct(0)
    both(pass_sum, 1)
    both(pass_back, 0)
    both(pass_sum, 3)
    both(pass_rest, 1)
    both(pass_rest, 3)
    for o in (0, 1):
        kept[:, o * HALF:(o + 1) * HALF] = combine(o, 0)
    gone(back.at[0], b_s)
    gone(relay_back, bl_s)
    gone(relay_back, bf_s)
    for o in (0, 1):
        landed(part_in.at[o], p_r.at[o, 2])
        here = slice(o * HALF, (o + 1) * HALF)
        kept[:, here] = kept[:, here] + part_in[o, 0].astype(f32) + part_in[o, 1].astype(f32)
    values = RESIDUAL_SCALE * normed[...].astype(f32) + kept[...] + shared[...]
    out[...] = (normalize(values) * gain[...]).astype(bf16)
    gone(near.at[:, 0:3], p_s)


def shards(
    linear_part, gate_part, kernel_taps, channel_gain, output_weight, residual, mix_gain, documents,
    expert_ids, route_weights, expert_gate, expert_up, expert_down, shared_gate, shared_up, shared_down,
    final_gain,
):
    bf16, f32 = jnp.bfloat16, jnp.float32
    dma = pltpu.SemaphoreType.DMA
    vmem = pl.BlockSpec(memory_space=pltpu.VMEM)
    hbm = pl.BlockSpec(memory_space=pltpu.MemorySpace.HBM)
    block = (CAP, HALF)
    w_gate, w_up, w_down = expert_gate[0], expert_up[0], expert_down[0]
    args = (
        (linear_part, hbm), (gate_part, hbm), (kernel_taps, hbm), (channel_gain.reshape(16, 1, 128), hbm),
        (output_weight, hbm), (residual, hbm), (mix_gain[None, :], hbm), (documents.reshape(16, 128), hbm),
        (expert_ids.T, hbm), (route_weights.T, hbm), (final_gain[None, :], hbm),
        (w_gate, hbm), (w_up, hbm), (w_down, hbm), (shared_gate, hbm), (shared_up, hbm), (shared_down, hbm),
    )
    return pl.pallas_call(
        layer_kernel,
        out_shape=pltpu.MemorySpace.VMEM(residual.shape, bf16),
        in_specs=[spec for _, spec in args],
        out_specs=vmem,
        scratch_shapes=[
            pltpu.VMEM((TAPS, 128), bf16),
            pltpu.VMEM((16, 1, 128), f32),
            pltpu.VMEM((1, 2048), f32),
            pltpu.VMEM((16, 128), jnp.int32),
            pltpu.VMEM((2, ROWS), jnp.int32),
            pltpu.VMEM((2, ROWS), f32),
            pltpu.VMEM((1, 2048), f32),
            pltpu.VMEM((2048, 128), bf16),
            pltpu.VMEM((2048, 128), bf16),
            pltpu.VMEM((ROWS, 2048), bf16),
            pltpu.VMEM((DEPTH, 128, 2048), bf16),
            pltpu.VMEM((2048 + HALO, 128), f32),
            pltpu.VMEM((HALO, 128), bf16),
            pltpu.VMEM((8, 128), f32),
            pltpu.VMEM((HALO, 128), bf16),
            pltpu.VMEM((8, 128), f32),
            pltpu.VMEM((32, 128), f32),
            pltpu.VMEM((2048, 128), bf16),
            pltpu.VMEM((256, HALF), bf16),
            pltpu.VMEM((256, HALF), bf16),
            pltpu.VMEM((2, 256, 128), f32),
            pltpu.VMEM((2, 256, 128), f32),
            pltpu.VMEM((4, 2, ROWS, 512), f32),
            pltpu.VMEM((4, ROWS, 512), f32),
            pltpu.VMEM((ROWS, 2048), bf16),
            pltpu.VMEM((32, 1, 128), f32),
            pltpu.VMEM(w_gate.shape, bf16),
            pltpu.VMEM(w_up.shape, bf16),
            pltpu.VMEM(w_down.shape, bf16),
            pltpu.VMEM(shared_gate.shape, bf16),
            pltpu.VMEM(shared_up.shape, bf16),
            pltpu.VMEM(shared_down.shape, bf16),
            pltpu.VMEM((2, 4, ROWS, HALF), bf16),
            pltpu.VMEM((2, 4, 32, 1, 128), f32),
            pltpu.VMEM((2, 3, 4) + block, bf16),
            pltpu.VMEM((2, 4) + block, bf16),
            pltpu.VMEM((2, 4, 4) + block, bf16),
            pltpu.VMEM((4, 4, CAP, 512), f32),
            pltpu.VMEM((4, 4, CAP, 512), f32),
            pltpu.VMEM((4, 4, CAP, 512), bf16),
            pltpu.VMEM((2, 3, 4) + block, bf16),
            pltpu.VMEM((2, 4) + block, bf16),
            pltpu.VMEM((2, 4, 4) + block, bf16),
            pltpu.VMEM((2, 3, ROWS, HALF), bf16),
            pltpu.VMEM((2, 2) + block, bf16),
            pltpu.VMEM((2, 2, ROWS, HALF), bf16),
            pltpu.VMEM((ROWS, 2048), f32),
            pltpu.VMEM((ROWS, 2048), f32),
            dma((11,)), dma((6,)), dma((7,)), dma((2,)), dma, dma((2, 3, 3)), dma((2, 3, 3, 2)), dma((2, 3)),
            dma, dma((4,)), dma((2, 3)), dma((2, 3)), dma((2, 4)), dma((2, 4)), dma((2, 4)), dma((2, 4)),
            dma((2, 3)),
            dma, dma((2,)), dma, dma, dma, dma, dma, dma, dma, dma, dma, dma, dma, dma, dma, dma,
        ],
        compiler_params=pltpu.CompilerParams(
            collective_id=0, has_side_effects=True, vmem_limit_bytes=54 * 1024 * 1024
        ),
    )(*[a for a, _ in args])


def solution(mesh):
    both = P(("sp", "tp"), None)
    placed = (
        P("sp", "tp"), P("sp", "tp"), P(None, "tp"), P(), P("tp", None), both, P(), P("sp"), both, both,
        P("sp", None, None), P("sp", None, None), P("sp", None, None), P(), P(), P(), P(),
    )
    return jax.shard_map(shards, mesh=mesh, in_specs=placed, out_specs=both, check_vma=False)
```

```python
import jax
import jax.numpy as jnp
from jax import lax
from jax.experimental import pallas as pl
from jax.experimental.pallas import tpu as pltpu
from jax.sharding import PartitionSpec as P

EPSILON = 1e-05
RESIDUAL_SCALE = 8.0**0.25
MESH_ID = pl.DeviceIdType.MESH
HALF = 1024
SIDE = 4
DEPTH = 8
CAP = 64
ROWS = 128
HALO = 32
TAPS = 31
PLACE = {1: 0, 7: 1, 2: 2, 6: 3, 3: 4, 5: 5, 4: 6, 0: 7}
GROUP = ((0, 2), (2, 4), (4, 7))


def normalize(values):
    mean = jnp.mean(values, -1, keepdims=True)
    square = jnp.mean(values * values, -1, keepdims=True)
    return (values - mean) * lax.rsqrt(square - mean * mean + EPSILON)


def layer_kernel(
    linear_h, gate_h, taps_h, channel_gain_h, w_h, residual_h, mix_gain_h, docs_h, ids_h, ways_h, gain_h,
    w_gate, w_up, w_down, s_gate, s_up, s_down, out,
    taps, channel_gain, mix_gain, docs, ids, ways, gain,
    linear, gate, residual, weight, gated, tail, tail_docs, halo, halo_docs, tap32, conv, conv_in, act,
    sums, sums_in, part, part_in2, normed, table,
    wg, wu, wd, sg, su, sd,
    near, meta, packed, relay, arrived, acc_g, acc_u, hidden, answers, relay_back, back, partial, relay_part,
    part_in, kept, shared,
    l_sem, w_sem, z_r, h_r, a_r, g_r, e_r, end_r, st_r, x_r, s1_r, m_r, d_r, rl_r, b_r, bl_r, p_r,
    z_s, h_s, a_s, g_s, e_s, st_s, x_s, s1_s, m_s, d_s, rl_s, fw_s, b_s, bl_s, bf_s, p_s,
):
    f32, bf16 = jnp.float32, jnp.bfloat16
    sp, tp = lax.axis_index("sp"), lax.axis_index("tp")
    y, x = sp // SIDE, sp % SIDE
    z, core = tp // 2, tp % 2
    other = 1 - core

    def at(dy, dx):
        return ((y + dy) % SIDE) * SIDE + (x + dx) % SIDE

    def first(o, k):
        return at(0, k) if o == 0 else at(k, 0)

    def second(o, k):
        return at(k, 0) if o == 0 else at(0, k)

    def along(dz):
        return ((z + dz) % DEPTH) * 2 + core

    def push(src, dst, ss, rs, to_sp, to_tp):
        pltpu.make_async_remote_copy(
            src_ref=src, dst_ref=dst, send_sem=ss, recv_sem=rs,
            device_id=(to_sp, to_tp), device_id_type=MESH_ID,
        ).start()

    def send(src, dst, ss, rs, to):
        push(src, dst, ss, rs, to, tp)

    def landed(dst, rs):
        pltpu.make_async_remote_copy(
            src_ref=dst, dst_ref=dst, send_sem=rs, recv_sem=rs,
            device_id=(first(0, 1), tp), device_id_type=MESH_ID,
        ).wait_recv()

    def gone(src, ss):
        pltpu.make_async_remote_copy(
            src_ref=src, dst_ref=src, send_sem=ss, recv_sem=ss,
            device_id=(first(0, 1), tp), device_id_type=MESH_ID,
        ).wait_send()

    own_loads = [
        pltpu.make_async_copy(a, b, l_sem.at[i])
        for i, (a, b) in enumerate(
            [
                (w_h, weight.at[7]), (linear_h, linear), (gate_h, gate), (docs_h, docs), (ids_h, ids),
                (ways_h, ways), (taps_h, taps), (channel_gain_h, channel_gain), (mix_gain_h, mix_gain),
                (gain_h, gain), (residual_h, residual),
            ]
        )
    ]
    for load in own_loads:
        load.start()
    loads = [
        pltpu.make_async_copy(a, b, w_sem.at[i])
        for i, (a, b) in enumerate(
            [(s_gate, sg), (s_up, su), (s_down, sd), (w_gate, wg), (w_up, wu), (w_down, wd)]
        )
    ]

    after, ahead = (sp + 1) % 16, (sp + 15) % 16
    barrier = pltpu.get_barrier_semaphore()

    def greet(to_sp, to_tp):
        pl.semaphore_signal(barrier, inc=1, device_id=(to_sp, to_tp), device_id_type=MESH_ID)

    for dz in (1, 7, 2, 6):
        greet(sp, along(dz))
    for to in (at(0, 1), at(0, 3), at(1, 0), at(3, 0), after, ahead):
        greet(to, tp)
    greet(sp, z * 2 + other)
    pl.semaphore_wait(barrier, 11)

    def columns(o, k, ks=0):
        fast, slow = (x, y) if o == 0 else (y, x)
        block = ((slow + ks) % SIDE) * SIDE + (fast + k) % SIDE
        return pl.ds(pl.multiple_of(block * 128, 128), 128)

    def strip(o):
        return slice(o * 64, o * 64 + 64)

    def upper(o):
        return slice(o * 64, o * 64 + 32)

    def lower(o):
        return slice(o * 64 + 32, o * 64 + 64)

    def hop(here, there, dz):
        for o in (0, 1):
            push(
                weight.at[here, strip(o), columns(o, 0)], weight.at[there, strip(o), columns(o, 0)],
                z_s, z_r.at[there], sp, along(dz),
            )

    def hopped(there):
        landed(weight.at[there, :, 0:128], z_r.at[there])

    own_loads[0].wait()
    hop(7, PLACE[7], 1)
    hop(7, PLACE[1], 7)
    hop(7, PLACE[6], 2)
    hop(7, PLACE[2], 6)

    for load in own_loads[1:4]:
        load.wait()

    def gate_rows(a, b):
        a, b = a.astype(f32), b.astype(f32)
        return (a * (1.0 / (1.0 + jnp.exp(-b)))).astype(bf16)

    tail[...] = gate_rows(linear[2048 - HALO:, :], gate[2048 - HALO:, :])
    doc = docs[...]
    spot = lax.broadcasted_iota(jnp.int32, (16, 128), 0) * 128 + lax.broadcasted_iota(jnp.int32, (16, 128), 1)
    local, last = [], []
    for d in (1, 2, 3):
        below = jnp.where(doc < d, 1.0, 0.0)
        local.append(jnp.sum(jnp.sum(below, 1, keepdims=True), 0, keepdims=True))
        below = jnp.where(spot >= 2048 - (TAPS - 1), below, 0.0)
        last.append(jnp.sum(jnp.sum(below, 1, keepdims=True), 0, keepdims=True))
    for i in range(3):
        tail_docs[i:i + 1, :] = jnp.broadcast_to(last[i], (1, 128))
    tail_docs[3:8, :] = jnp.zeros((5, 128), f32)
    push(tail, halo, h_s.at[0], h_r.at[0], after, tp)
    push(tail_docs, halo_docs, h_s.at[1], h_r.at[1], after, tp)
    for load in loads:
        load.start()

    def gate_block(i, _):
        rows = pl.ds(pl.multiple_of(i * 128, 128), 128)
        there = pl.ds(pl.multiple_of(i * 128 + HALO, 32), 128)
        gated[there, :] = gate_rows(linear[rows, :], gate[rows, :]).astype(f32)
        return 0

    lax.fori_loop(0, 16, gate_block, 0)
    for load in own_loads[4:10]:
        load.wait()
    tap32[0:TAPS, :] = taps[...].astype(f32)

    def spread(o, g, k):
        lo, hi = GROUP[g]
        mine = weight.at[lo:hi, strip(o), columns(o, k)]
        late = (0, 1, 2, 1)[k]
        send(mine, mine, e_s, e_r.at[o, g, late, 0], second(o, 1))
        send(mine, mine, e_s, e_r.at[o, g, late, 1], second(o, 3))

    def gather_start(g):
        lo, hi = GROUP[g]
        for o in (0, 1):
            mine = weight.at[lo:hi, strip(o), columns(o, 0)]
            send(mine, mine, g_s, g_r.at[o, g, 0], first(o, 1))
            send(mine, mine, g_s, g_r.at[o, g, 1], first(o, 3))
        for o in (0, 1):
            spread(o, g, 0)

    def gather_near(g):
        lo, hi = GROUP[g]
        for o in (0, 1):
            landed(weight.at[lo:hi, strip(o), columns(o, 3)], g_r.at[o, g, 0])
            half = weight.at[lo:hi, upper(o), columns(o, 3)]
            send(half, half, g_s, g_r.at[o, g, 2], first(o, 1))
            landed(weight.at[lo:hi, strip(o), columns(o, 1)], g_r.at[o, g, 1])
            half = weight.at[lo:hi, lower(o), columns(o, 1)]
            send(half, half, g_s, g_r.at[o, g, 2], first(o, 3))
        for o in (0, 1):
            spread(o, g, 3)
            spread(o, g, 1)

    def gather_far(g):
        lo, hi = GROUP[g]
        for o in (0, 1):
            landed(weight.at[lo:hi, strip(o), columns(o, 2)], g_r.at[o, g, 2])
            spread(o, g, 2)

    def gather_pass(g, ks):
        lo, hi = GROUP[g]
        late = (0, 1, 2, 1)[ks[0]]
        for o in (0, 1):
            landed(weight.at[lo:hi, strip(o), 0:128 * len(ks)], e_r.at[o, g, late, 0])
            for k in ks:
                half = weight.at[lo:hi, upper(o), columns(o, k, 3)]
                send(half, half, e_s, end_r.at[o, g], second(o, 1))
            landed(weight.at[lo:hi, strip(o), 0:128 * len(ks)], e_r.at[o, g, late, 1])
            for k in ks:
                half = weight.at[lo:hi, lower(o), columns(o, k, 1)]
                send(half, half, e_s, end_r.at[o, g], second(o, 3))

    def gather_end(g):
        lo, hi = GROUP[g]
        for o in (0, 1):
            landed(weight.at[lo:hi, strip(o), 0:512], end_r.at[o, g])

    OWN, SIDES, FAR = (0,), (3, 1), (2,)

    names = lax.broadcasted_iota(jnp.int32, (16, ROWS), 0)
    hit_0, hit_1 = names == ids[0:1, :], names == ids[1:2, :]
    hits = jnp.where(hit_0 | hit_1, 1.0, 0.0)
    before = lax.broadcasted_iota(jnp.int32, (ROWS, ROWS), 0) < lax.broadcasted_iota(jnp.int32, (ROWS, ROWS), 1)
    ranks = jnp.dot(hits.astype(bf16), jnp.where(before, 1.0, 0.0).astype(bf16), preferred_element_type=f32)
    slots = jnp.where(hits > 0.5, ranks, -1.0)
    values = jnp.where(hit_0, ways[0:1, :], 0.0) + jnp.where(hit_1, ways[1:2, :], 0.0)
    for e in range(16):
        table[e] = slots[e:e + 1, :]
        table[e + 16] = values[e:e + 1, :]
    for o in (0, 1):
        send(table, meta.at[o, 3], m_s, m_r.at[o, 0], first(o, 1))
        send(table, meta.at[o, 1], m_s, m_r.at[o, 1], first(o, 3))

    hopped(PLACE[7])
    hopped(PLACE[1])
    gather_start(0)
    hopped(PLACE[6])
    hop(PLACE[6], PLACE[5], 1)
    hop(PLACE[6], PLACE[4], 2)
    hopped(PLACE[2])
    hop(PLACE[2], PLACE[3], 7)
    gather_start(1)
    landed(halo, h_r.at[0])
    landed(halo_docs, h_r.at[1])
    inside = sp > 0
    gated[0:HALO, :] = jnp.where(inside, halo[...].astype(f32), 0.0)
    starts = []
    for i in range(3):
        extra = jnp.where(inside, halo_docs[i:i + 1, :], float(TAPS - 1)) - float(TAPS - 1)
        starts.append(local[i] + extra)

    CHUNK = 64

    def conv_block(dz):
        base = ((z + dz) % DEPTH) * 256

        def piece(i, _):
            row = pl.multiple_of(base + i * CHUNK, CHUNK)
            spot = lax.broadcasted_iota(jnp.int32, (CHUNK, 128), 0).astype(f32) + row.astype(f32)
            begun = jnp.full((CHUNK, 128), -1000.0, f32)
            for s in starts:
                begun = jnp.maximum(begun, jnp.where(s <= spot, s, -1000.0))
            age = spot - begun
            total = jnp.zeros((CHUNK, 128), f32)
            for j in range(TAPS):
                window = gated[pl.ds(row + (HALO - j), CHUNK), :]
                total = total + jnp.where(age >= float(j), window * tap32[j:j + 1, :], 0.0)
            conv[pl.ds(row, CHUNK), :] = total.astype(bf16)
            return 0

        lax.fori_loop(0, 256 // CHUNK, piece, 0)
        rows = pl.ds(pl.multiple_of(base, 256), 256)
        if dz == 0:
            conv_in[:, 7 * 128:] = conv[rows, :]

    def conv_send(*steps):
        for dz in steps:
            rows = pl.ds(pl.multiple_of(((z + dz) % DEPTH) * 256, 256), 256)
            there = PLACE[(DEPTH - dz) % DEPTH]
            push(
                conv.at[rows, :], conv_in.at[:, there * 128:(there + 1) * 128],
                a_s, a_r, sp, along(dz),
            )

    conv_block(1)
    conv_block(7)
    for o in (0, 1):
        landed(meta.at[o, 3], m_r.at[o, 0])
        send(meta.at[o, 3], meta.at[o, 2], m_s, m_r.at[o, 2], first(o, 1))
        landed(meta.at[o, 1], m_r.at[o, 1])
    gather_near(0)
    conv_block(2)
    gather_pass(0, OWN)
    hopped(PLACE[5])
    hopped(PLACE[3])
    hopped(PLACE[4])
    gather_start(2)
    conv_send(2, 1, 7)
    conv_block(6)
    conv_send(6)
    gather_near(1)
    gather_far(0)
    conv_block(3)
    conv_send(3)
    gather_near(2)
    gather_pass(0, SIDES)
    conv_block(5)
    conv_send(5)
    gather_far(1)
    gather_pass(1, OWN)
    conv_block(4)
    conv_send(4)
    gather_far(2)
    gather_pass(1, SIDES)
    gather_pass(0, FAR)
    gather_pass(2, OWN)
    gather_pass(2, SIDES)
    gather_pass(1, FAR)
    gather_pass(2, FAR)
    conv_block(0)

    landed(conv_in.at[:, 0:7 * 128], a_r)
    mean_part = jnp.zeros((256, 128), f32)
    square_part = jnp.zeros((256, 128), f32)
    for s in range(DEPTH):
        v = conv_in[:, s * 128:(s + 1) * 128].astype(f32)
        mean_part = mean_part + v
        square_part = square_part + v * v
    sums[0] = mean_part
    sums[1] = square_part
    push(sums, sums_in, st_s, st_r, sp, z * 2 + other)
    landed(sums_in, st_r)
    mean = jnp.sum(sums[0] + sums_in[0], 1, keepdims=True) * (1.0 / 2048.0)
    square = jnp.sum(sums[1] + sums_in[1], 1, keepdims=True) * (1.0 / 2048.0)
    scale = lax.rsqrt(square - mean * mean + EPSILON)
    for dz, s in PLACE.items():
        v = conv_in[:, s * 128:(s + 1) * 128].astype(f32)
        v = (v - mean) * scale * channel_gain[along(dz)]
        act[:, s * 128:(s + 1) * 128] = (v / (1.0 + jnp.exp(-v))).astype(bf16)

    for o in (0, 1):
        landed(meta.at[o, 2], m_r.at[o, 2])

    for g, (lo, hi) in enumerate(((0, 2), (2, 4), (4, 8))):
        gather_end(g)
        for n in range(4):
            w = weight[lo:hi, :, n * 512:(n + 1) * 512].reshape((hi - lo) * 128, 512)
            got = jnp.dot(act[:, lo * 128:hi * 128], w, preferred_element_type=f32).reshape(2, ROWS, 512)
            part[n] = got if g == 0 else part[n] + got
            if g == 2:
                push(part.at[n, other], part_in2.at[n], x_s, x_r.at[n], sp, z * 2 + other)
    own_loads[10].wait()
    for n in range(4):
        cols = slice(n * 512, (n + 1) * 512)
        landed(part_in2.at[n], x_r.at[n])
        kept[:, cols] = RESIDUAL_SCALE * residual[:, cols].astype(f32) + part[n, core] + part_in2[n]
    normed[...] = (normalize(kept[...]) * mix_gain[...]).astype(bf16)

    for o in (0, 1):
        mine = normed.at[:, o * HALF:(o + 1) * HALF]
        send(mine, near.at[o, 3], s1_s, s1_r.at[o, 0], first(o, 1))
        send(mine, near.at[o, 1], s1_s, s1_r.at[o, 1], first(o, 3))

    lanes = lax.broadcasted_iota(jnp.int32, (CAP, 128), 0).astype(f32)

    def expert_at(o, k):
        return second(o, k)

    def slot_row(o, k, e):
        return table[e] if k == 0 else meta[o, k, e]

    def weight_row(o, k, e):
        return table[e + 16] if k == 0 else meta[o, k, e + 16]

    def pack(o, k):
        rows = normed[:, o * HALF:(o + 1) * HALF] if k == 0 else near[o, k]
        for q in (2, 1, 3, 0):
            hit = jnp.where(lanes == slot_row(o, k, expert_at(o, q)), 1.0, 0.0).astype(bf16)
            block = jnp.dot(hit, rows, preferred_element_type=f32).astype(bf16)
            if q == 0:
                arrived[o, 0, k] = block
            else:
                packed[o, q - 1, k] = block
            if q == 2:
                way = 1 if k < 2 else 3
                send(packed.at[o, 1, k], relay.at[o, k], rl_s, rl_r.at[o, k], second(o, way))
        if k != 2:
            pack_send(o, k)

    def pack_send(o, k):
        send(packed.at[o, 0, k], arrived.at[o, 3, k], d_s, d_r.at[o, k], second(o, 1))
        send(packed.at[o, 2, k], arrived.at[o, 1, k], d_s, d_r.at[o, k], second(o, 3))

    def pass_on(o, k):
        landed(relay.at[o, k], rl_r.at[o, k])
        way = 1 if k < 2 else 3
        send(relay.at[o, k], arrived.at[o, 2, k], fw_s, d_r.at[o, k], second(o, way))

    for o in (0, 1):
        pack(o, 0)
    gone(weight.at[0:7, :, 0:128], z_s)
    gone(tail, h_s.at[0])
    gone(tail_docs, h_s.at[1])
    gone(conv_in.at[:, 0:7 * 128], a_s)
    gone(weight.at[0:7, :, 0:384], g_s)
    gone(weight.at[0:7, :, 0:1536], e_s)
    gone(sums, st_s)
    gone(part_in2, x_s)
    for o in (0, 1):
        landed(near.at[o, 3], s1_r.at[o, 0])
        send(near.at[o, 3, 0:64], near.at[o, 2, 0:64], s1_s, s1_r.at[o, 2], first(o, 1))
    for o in (0, 1):
        landed(near.at[o, 1], s1_r.at[o, 1])
        send(near.at[o, 1, 64:128], near.at[o, 2, 64:128], s1_s, s1_r.at[o, 2], first(o, 3))
    for k in (3, 1):
        for o in (0, 1):
            pack(o, k)
    for o in (0, 1):
        pass_on(o, 0)
    for o in (0, 1):
        landed(near.at[o, 2], s1_r.at[o, 2])
        pack(o, 2)

    acc_g[...] = jnp.zeros_like(acc_g)
    acc_u[...] = jnp.zeros_like(acc_u)
    for load in loads[:3]:
        load.wait()
    act = jnp.dot(normed[...], sg[...], preferred_element_type=f32)
    lin = jnp.dot(normed[...], su[...], preferred_element_type=f32)
    common = (act / (1.0 + jnp.exp(-act)) * lin).astype(bf16)
    shared[...] = jnp.dot(common, sd[...], preferred_element_type=f32)
    for k in (3, 1):
        for o in (0, 1):
            pass_on(o, k)
    for o in (0, 1):
        pack_send(o, 2)
    for o in (0, 1):
        pass_on(o, 2)
    for load in loads[3:]:
        load.wait()

    def product(o, k):
        landed(arrived.at[o, 1:4, k], d_r.at[o, k])
        rows = arrived[o, :, k].reshape(SIDE * CAP, HALF)
        for acc, w in ((acc_g, wg), (acc_u, wu)):
            got = jnp.dot(rows, w[o * HALF:(o + 1) * HALF, :], preferred_element_type=f32)
            got = got.reshape(SIDE, CAP, 512)
            if o == 0:
                acc[:, k] = acc[:, k] + got
            else:
                acc[k] = acc[k] + got

    for k in (0, 3, 1):
        for o in (0, 1):
            product(o, k)

    def relayed(k):
        for o in (0, 1):
            way = 1 if k < 2 else 3
            send(answers.at[o, 1, k], relay_back.at[o, k], bl_s, bl_r.at[o, k], second(o, way))

    def direct(k, ways=(1, 3)):
        for o in (0, 1):
            for q in ways:
                send(answers.at[o, q - 1, k], back.at[o, k, SIDE - q], b_s, b_r.at[o, k], second(o, q))

    def pass_back(o, k):
        landed(relay_back.at[o, k], bl_r.at[o, k])
        way = 1 if k < 2 else 3
        send(relay_back.at[o, k], back.at[o, k, 2], bf_s, b_r.at[o, k], second(o, way))

    ready = set()

    def hide(dy, dx):
        if (dy, dx) not in ready:
            ready.add((dy, dx))
            g = acc_g[dy, dx]
            hidden[dy, dx] = (g / (1.0 + jnp.exp(-g)) * acc_u[dy, dx]).astype(bf16)

    def answer(k, qs=(0, 1, 2, 3)):
        for o in (0, 1):
            rows = []
            for q in qs:
                at_q = (q, k) if o == 0 else (k, q)
                hide(*at_q)
                rows.append(hidden[at_q])
            rows = jnp.concatenate(rows, 0) if len(rows) > 1 else rows[0]
            ans = jnp.dot(rows, wd[:, o * HALF:(o + 1) * HALF], preferred_element_type=f32).astype(bf16)
            for i, q in enumerate(qs):
                if q == 0:
                    back[o, k, 0] = ans[i * CAP:(i + 1) * CAP]
                else:
                    answers[o, q - 1, k] = ans[i * CAP:(i + 1) * CAP]

    answer(1, (0, 1, 3))
    direct(1)
    for o in (0, 1):
        product(o, 2)
    answer(2)
    relayed(2)
    direct(2)
    answer(1, (2,))
    relayed(1)
    answer(3)
    relayed(3)
    direct(3, (1,))
    answer(0)

    def choose(o, k, part):
        rows = []
        for j in range(SIDE):
            e = expert_at(o, j)
            w = weight_row(o, k, e)
            high = w.astype(bf16).astype(f32)
            value = high if part == 0 else w - high
            rows.append(jnp.where(lanes == slot_row(o, k, e), value, 0.0).astype(bf16))
        return jnp.concatenate(rows, 0)

    def combine(o, k):
        landed(back.at[o, k, 1:4], b_r.at[o, k])
        rows = back[o, k].reshape(SIDE * CAP, HALF)
        dims = (((0,), (0,)), ((), ()))
        total = lax.dot_general(choose(o, k, 0), rows, dims, preferred_element_type=f32)
        return total + lax.dot_general(choose(o, k, 1), rows, dims, preferred_element_type=f32)

    def send_sum(o, k, rows):
        place = 0 if k == 1 else 1
        send(partial.at[o, k - 1, rows], part_in.at[o, place, rows], p_s, p_r.at[o, 2], first(o, k))

    top, bottom = slice(0, 64), slice(64, 128)

    def pass_sum(o, k):
        total = combine(o, k)
        if k == 2:
            partial[o, 1] = total.astype(bf16)
            send(partial.at[o, 1, top], relay_part.at[o, 0], p_s, p_r.at[o, 0], first(o, 1))
            send(partial.at[o, 1, bottom], relay_part.at[o, 1], p_s, p_r.at[o, 1], first(o, 3))
            return
        early, late = (bottom, top) if k == 1 else (top, bottom)
        partial[o, k - 1, early] = total[early].astype(bf16)
        send_sum(o, k, early)
        kept[late, o * HALF:(o + 1) * HALF] = total[late]

    def pass_rest(o, k):
        place, late = (0, top) if k == 1 else (1, bottom)
        landed(relay_part.at[o, place], p_r.at[o, place])
        total = kept[late, o * HALF:(o + 1) * HALF] + relay_part[o, place].astype(f32)
        partial[o, k - 1, late] = total.astype(bf16)
        send_sum(o, k, late)

    def both(step, k):
        for o in (0, 1):
            step(o, k)

    both(pass_back, 2)
    direct(3, (3,))
    both(pass_back, 1)
    relayed(0)
    both(pass_back, 3)
    gone(meta.at[:, 0:3], m_s)
    gone(near.at[:, 0:3], s1_s)
    gone(arrived.at[0], d_s)
    gone(relay, rl_s)
    gone(relay, fw_s)
    both(pass_sum, 2)
    direct(0)
    both(pass_sum, 1)
    both(pass_back, 0)
    both(pass_sum, 3)
    both(pass_rest, 1)
    both(pass_rest, 3)
    for o in (0, 1):
        kept[:, o * HALF:(o + 1) * HALF] = combine(o, 0)
    gone(back.at[0], b_s)
    gone(relay_back, bl_s)
    gone(relay_back, bf_s)
    for o in (0, 1):
        landed(part_in.at[o], p_r.at[o, 2])
        here = slice(o * HALF, (o + 1) * HALF)
        kept[:, here] = kept[:, here] + part_in[o, 0].astype(f32) + part_in[o, 1].astype(f32)
    values = RESIDUAL_SCALE * normed[...].astype(f32) + kept[...] + shared[...]
    out[...] = (normalize(values) * gain[...]).astype(bf16)
    gone(near.at[:, 0:3], p_s)


def shards(
    linear_part, gate_part, kernel_taps, channel_gain, output_weight, residual, mix_gain, documents,
    expert_ids, route_weights, expert_gate, expert_up, expert_down, shared_gate, shared_up, shared_down,
    final_gain,
):
    bf16, f32 = jnp.bfloat16, jnp.float32
    dma = pltpu.SemaphoreType.DMA
    vmem = pl.BlockSpec(memory_space=pltpu.VMEM)
    hbm = pl.BlockSpec(memory_space=pltpu.MemorySpace.HBM)
    block = (CAP, HALF)
    w_gate, w_up, w_down = expert_gate[0], expert_up[0], expert_down[0]
    args = (
        (linear_part, hbm), (gate_part, hbm), (kernel_taps, hbm), (channel_gain.reshape(16, 1, 128), hbm),
        (output_weight, hbm), (residual, hbm), (mix_gain[None, :], hbm), (documents.reshape(16, 128), hbm),
        (expert_ids.T, hbm), (route_weights.T, hbm), (final_gain[None, :], hbm),
        (w_gate, hbm), (w_up, hbm), (w_down, hbm), (shared_gate, hbm), (shared_up, hbm), (shared_down, hbm),
    )
    return pl.pallas_call(
        layer_kernel,
        out_shape=pltpu.MemorySpace.VMEM(residual.shape, bf16),
        in_specs=[spec for _, spec in args],
        out_specs=vmem,
        scratch_shapes=[
            pltpu.VMEM((TAPS, 128), bf16),
            pltpu.VMEM((16, 1, 128), f32),
            pltpu.VMEM((1, 2048), f32),
            pltpu.VMEM((16, 128), jnp.int32),
            pltpu.VMEM((2, ROWS), jnp.int32),
            pltpu.VMEM((2, ROWS), f32),
            pltpu.VMEM((1, 2048), f32),
            pltpu.VMEM((2048, 128), bf16),
            pltpu.VMEM((2048, 128), bf16),
            pltpu.VMEM((ROWS, 2048), bf16),
            pltpu.VMEM((DEPTH, 128, 2048), bf16),
            pltpu.VMEM((2048 + HALO, 128), f32),
            pltpu.VMEM((HALO, 128), bf16),
            pltpu.VMEM((8, 128), f32),
            pltpu.VMEM((HALO, 128), bf16),
            pltpu.VMEM((8, 128), f32),
            pltpu.VMEM((32, 128), f32),
            pltpu.VMEM((2048, 128), bf16),
            pltpu.VMEM((256, HALF), bf16),
            pltpu.VMEM((256, HALF), bf16),
            pltpu.VMEM((2, 256, 128), f32),
            pltpu.VMEM((2, 256, 128), f32),
            pltpu.VMEM((4, 2, ROWS, 512), f32),
            pltpu.VMEM((4, ROWS, 512), f32),
            pltpu.VMEM((ROWS, 2048), bf16),
            pltpu.VMEM((32, 1, 128), f32),
            pltpu.VMEM(w_gate.shape, bf16),
            pltpu.VMEM(w_up.shape, bf16),
            pltpu.VMEM(w_down.shape, bf16),
            pltpu.VMEM(shared_gate.shape, bf16),
            pltpu.VMEM(shared_up.shape, bf16),
            pltpu.VMEM(shared_down.shape, bf16),
            pltpu.VMEM((2, 4, ROWS, HALF), bf16),
            pltpu.VMEM((2, 4, 32, 1, 128), f32),
            pltpu.VMEM((2, 3, 4) + block, bf16),
            pltpu.VMEM((2, 4) + block, bf16),
            pltpu.VMEM((2, 4, 4) + block, bf16),
            pltpu.VMEM((4, 4, CAP, 512), f32),
            pltpu.VMEM((4, 4, CAP, 512), f32),
            pltpu.VMEM((4, 4, CAP, 512), bf16),
            pltpu.VMEM((2, 3, 4) + block, bf16),
            pltpu.VMEM((2, 4) + block, bf16),
            pltpu.VMEM((2, 4, 4) + block, bf16),
            pltpu.VMEM((2, 3, ROWS, HALF), bf16),
            pltpu.VMEM((2, 2) + block, bf16),
            pltpu.VMEM((2, 2, ROWS, HALF), bf16),
            pltpu.VMEM((ROWS, 2048), f32),
            pltpu.VMEM((ROWS, 2048), f32),
            dma((11,)), dma((6,)), dma((7,)), dma((2,)), dma, dma((2, 3, 3)), dma((2, 3, 3, 2)), dma((2, 3)),
            dma, dma((4,)), dma((2, 3)), dma((2, 3)), dma((2, 4)), dma((2, 4)), dma((2, 4)), dma((2, 4)),
            dma((2, 3)),
            dma, dma((2,)), dma, dma, dma, dma, dma, dma, dma, dma, dma, dma, dma, dma, dma, dma,
        ],
        compiler_params=pltpu.CompilerParams(
            collective_id=0, has_side_effects=True, vmem_limit_bytes=54 * 1024 * 1024
        ),
    )(*[a for a, _ in args])


def solution(mesh):
    both = P(("sp", "tp"), None)
    placed = (
        P("sp", "tp"), P("sp", "tp"), P(None, "tp"), P(), P("tp", None), both, P(), P("sp"), both, both,
        P("sp", None, None), P("sp", None, None), P("sp", None, None), P(), P(), P(), P(),
    )
    return jax.shard_map(shards, mesh=mesh, in_specs=placed, out_specs=both, check_vma=False)
```
